32 devices in a mesh: sp: 8 (over z, x), tp: 4 (over y, core).
Axes of the slice: x: 2, y: 2, z: 4, core: 2. Of those that a mesh axis runs over, the one named last changes fastest.
Arguments:
- latent: bfloat16 [8192, 2048], P(('sp', 'tp')), may hold values from -8 to 8
- context: bfloat16 [512, 2048], P('sp'), may hold values from -8 to 8
- latent_condition: bfloat16 [2048], replicated, may hold values from -4 to 4
- context_condition: bfloat16 [2048], replicated, may hold values from -4 to 4
- shift_weight: bfloat16 [2048, 2048], P('sp', 'tp'), may hold values from -0.125 to 0.125
- scale_weight: bfloat16 [2048, 2048], P('sp', 'tp'), may hold values from -0.125 to 0.125
- gate_weight: bfloat16 [2048, 2048], P('sp', 'tp'), may hold values from -0.125 to 0.125
- norm_gain: float32 [2048], replicated, may hold values from 0.1 to 1.9
- query_weight: bfloat16 [2048, 512], replicated, may hold values from -0.125 to 0.125
- key_weight: bfloat16 [2048, 512], replicated, may hold values from -0.125 to 0.125
- value_weight: bfloat16 [2048, 1024], replicated, may hold values from -0.125 to 0.125
- outgate_weight: bfloat16 [2048, 1024], replicated, may hold values from -0.125 to 0.125
- down_weight: bfloat16 [2048, 32], replicated, may hold values from -0.125 to 0.125
- up_weight: bfloat16 [32, 512], replicated, may hold values from -2 to 2
- decay_bias: float32 [512], replicated, as said below
- out_weight: bfloat16 [1024, 2048], replicated, may hold values from -0.1875 to 0.1875
- post_gain: float32 [2048], replicated, may hold values from 0.1 to 1.9
Outputs:
- updated: bfloat16 [8192, 2048], P(('sp', 'tp'))
The draws below stay inside these ranges and needn't reach their ends.
Inputs may be any that keep to these rules, and one draw needn't show every extreme that they name: decay_bias is at least 0; counting heads from 0, the channels of heads 1, 3, 5, … are at least log(512) + 2, those of heads 0, 2, 4, … at most 1.5.
All inputs are finite; a program needn't handle non-finite values.
Results may differ from the reference program's by a relative error of at most 0.0035.
The reference program's roundings to bfloat16 on the way count: a program that leaves them out, or rounds other values in their place, can miss the bound.
Values may be sent and summed in bfloat16 or wider, within the bound.
A program may use at most 192 MiB of HBM per device.

```python
import jax
import jax.numpy as jnp
from jax import lax

D = 2048
HEADS = 16
DK = 32
DV = 64
RANK = 32
BLOCK = 32
CTX = 512
KEYW = 512
VALW = 1024
LATENT = 8192


def draw_latent(key, part):
    noise_key, slow_key = jax.random.split(key)
    noise_part = jax.random.normal(noise_key, (LATENT, D), jnp.float32)
    slow_part = jax.random.normal(slow_key, (LATENT // 128, D), jnp.float32)
    values = noise_part + jnp.repeat(slow_part, 128, axis=0)
    return jnp.clip(values, -8.0, 8.0).astype(jnp.bfloat16)


def draw_context(key, part):
    noise_key, slow_key = jax.random.split(jax.random.fold_in(key, 7))
    noise_part = jax.random.normal(noise_key, (CTX, D), jnp.float32)
    slow_part = 1.5 * jax.random.normal(slow_key, (CTX // 4, D), jnp.float32)
    values = noise_part + jnp.repeat(slow_part, 4, axis=0)
    return jnp.clip(values, -8.0, 8.0).astype(jnp.bfloat16)


def draw_decay_bias(key, part):
    channel = jnp.arange(HEADS * DK)
    weak_head = channel // DK % 2 == 1
    unit_draw = jax.random.uniform(key, (HEADS * DK,), jnp.float32)
    strong_value = 1.5 * unit_draw
    weak_value = jnp.log(LATENT / 16.0) + 2.0 + 2.0 * unit_draw
    return jnp.where(weak_head, weak_value, strong_value).astype(jnp.float32)


def levels(key, shape, cuts, smallest, largest):
    level = 1.0
    for position, parts in cuts:
        steps = jax.random.uniform(jax.random.fold_in(jax.random.fold_in(key, 6), position), (parts,), jnp.float32, smallest / len(cuts), largest / len(cuts))
        level = level * jnp.repeat(jnp.exp(steps), shape[position] // parts).reshape((-1,) + (1,) * (len(shape) - 1 - position))
    return level


def normal_values(stream_key, shape, deviation, bound, pieces=(), dtype=jnp.bfloat16):
    array = jax.random.normal(stream_key, shape, jnp.float32) * deviation
    if len(pieces) > 0:
        array = levels(stream_key, shape, pieces, -0.22, 0.18) * array
    return jnp.clip(array, min=-bound, max=bound).astype(dtype)


def setup_inputs(seed: int = 0) -> dict:
    seeds = jax.random.split(jax.random.key(seed), 18)
    latent = draw_latent(jax.random.fold_in(seeds[17], 71), 0)
    context = draw_context(jax.random.fold_in(seeds[17], 71), 0)
    latent_condition = normal_values(seeds[2], (D,), 1.0, 4.0)
    context_condition = normal_values(seeds[3], (D,), 1.0, 4.0)
    shift_weight = normal_values(seeds[4], (D, D), D ** -0.5, 0.125, ((0, 8), (1, 4)))
    scale_weight = normal_values(seeds[5], (D, D), D ** -0.5, 0.125, ((0, 8), (1, 4)))
    gate_weight = normal_values(seeds[6], (D, D), D ** -0.5, 0.125, ((0, 8), (1, 4)))
    norm_gain = jnp.clip(1.0 + 0.18 * jax.random.normal(seeds[7], (D,), jnp.float32), 0.1, 1.9)
    query_weight = normal_values(seeds[8], (D, KEYW), D ** -0.5, 0.125)
    key_weight = normal_values(seeds[9], (D, KEYW), D ** -0.5, 0.125)
    value_weight = normal_values(seeds[10], (D, VALW), D ** -0.5, 0.125)
    outgate_weight = normal_values(seeds[11], (D, VALW), D ** -0.5, 0.125)
    down_weight = normal_values(seeds[12], (D, RANK), D ** -0.5, 0.125)
    up_weight = normal_values(seeds[13], (RANK, KEYW), (RANK // 4) ** -0.5, 2.0)
    decay_bias = draw_decay_bias(jax.random.fold_in(seeds[17], 71), 0)
    out_weight = normal_values(seeds[15], (VALW, D), VALW ** -0.5, 0.1875)
    post_gain = jnp.clip(1.0 + 0.18 * jax.random.normal(seeds[16], (D,), jnp.float32), 0.1, 1.9)
    return dict(latent=latent, context=context, latent_condition=latent_condition, context_condition=context_condition, shift_weight=shift_weight, scale_weight=scale_weight, gate_weight=gate_weight, norm_gain=norm_gain, query_weight=query_weight, key_weight=key_weight, value_weight=value_weight, outgate_weight=outgate_weight, down_weight=down_weight, up_weight=up_weight, decay_bias=decay_bias, out_weight=out_weight, post_gain=post_gain)


epsilon = 1e-06
decay_temper = 16.0
highest = lax.Precision.HIGHEST

def rms_factor(values):
    return lax.rsqrt(lax.optimization_barrier(jnp.mean(values * values, axis=-1, keepdims=True)) + epsilon)

def stored(values):
    return lax.optimization_barrier(values.astype(jnp.bfloat16))

def modulated(tokens, norm_gain, shift_row, scale_row):
    values = tokens.astype(jnp.float32)
    return (values * rms_factor(values) * norm_gain * (1.0 + scale_row) + shift_row).astype(jnp.bfloat16)

def project(normed, weight):
    return jnp.dot(normed, weight, preferred_element_type=jnp.float32)

def log_decays(normed, down_weight, up_weight, decay_bias):
    low_rank = project(normed, down_weight).astype(jnp.bfloat16)
    return jax.nn.log_sigmoid(project(low_rank, up_weight) + decay_bias) / decay_temper

def weighted_state(key_rows, value_rows, weights):
    row_count = key_rows.shape[0]
    scaled = (key_rows.astype(jnp.float32) * weights).reshape(row_count, HEADS, DK)
    value_heads = value_rows.astype(jnp.float32).reshape(row_count, HEADS, DV)
    return jnp.einsum('sha,she->hae', scaled, value_heads, precision=highest)

def segment_states(key_rows, value_rows, log_decay):
    inclusive = jnp.cumsum(log_decay, axis=0)
    total_log = inclusive[-1]
    after_log = total_log - inclusive
    before_log = inclusive - log_decay
    return (weighted_state(key_rows, value_rows, jnp.exp(after_log)), weighted_state(key_rows, value_rows, jnp.exp(before_log)), total_log)

def block_terms(query_heads, key_heads, value_heads, log_heads):
    block_count = query_heads.shape[0] // BLOCK
    q_blocks = query_heads.reshape(block_count, BLOCK, HEADS, DK)
    k_blocks = key_heads.reshape(block_count, BLOCK, HEADS, DK)
    v_blocks = value_heads.reshape(block_count, BLOCK, HEADS, DV)
    inside = jnp.cumsum(log_heads.reshape(block_count, BLOCK, HEADS, DK), axis=1)
    closing = inside[:, -1]
    q_decayed = q_blocks * jnp.exp(inside)
    k_decayed = k_blocks * jnp.exp(-inside)
    scores = jnp.einsum('ntha,nsha->nhts', q_decayed, k_decayed, precision=highest)
    lower_mask = jnp.tril(jnp.ones((BLOCK, BLOCK), bool))
    scores = jnp.where(lower_mask, scores, 0.0)
    within = jnp.einsum('nhts,nshe->nthe', scores, v_blocks, precision=highest)
    summary = jnp.einsum('nsha,nshe->nhae', k_blocks * jnp.exp(closing[:, None] - inside), v_blocks, precision=highest)
    return (q_decayed, within, closing, summary)

def direction(query_heads, key_heads, value_heads, log_heads, start_state):
    q_decayed, within, closing, summary = block_terms(query_heads, key_heads, value_heads, log_heads)

    def advance(carry_state, inputs):
        closing_one, summary_one = inputs
        return (jnp.exp(closing_one)[..., None] * carry_state + summary_one, carry_state)
    last_state, entering = lax.scan(advance, start_state, (closing, summary))
    across = jnp.einsum('ntha,nhae->nthe', q_decayed, entering, precision=highest)
    return (within + across).reshape(-1, HEADS, DV)

def reference(latent, context, latent_condition, context_condition, shift_weight, scale_weight, gate_weight, norm_gain, query_weight, key_weight, value_weight, outgate_weight, down_weight, up_weight, decay_bias, out_weight, post_gain):
    conditions = jnp.stack([latent_condition, context_condition])
    cond_act = jax.nn.silu(conditions.astype(jnp.float32)).astype(jnp.bfloat16)
    shifts = project(cond_act, shift_weight)
    scales = project(cond_act, scale_weight)
    gates = project(cond_act, gate_weight)
    ctx_normed = modulated(context, norm_gain, shifts[1], scales[1])
    ctx_keys = stored(project(ctx_normed, key_weight))
    ctx_values = stored(project(ctx_normed, value_weight))
    ctx_log = log_decays(ctx_normed, down_weight, up_weight, decay_bias)
    ctx_forward, ctx_backward, unused_total = segment_states(ctx_keys, ctx_values, ctx_log)
    normed = modulated(latent, norm_gain, shifts[0], scales[0])
    row_count = latent.shape[0]
    query_rows = stored(project(normed, query_weight))
    key_rows = stored(project(normed, key_weight))
    value_rows = stored(project(normed, value_weight))
    outgate_rows = stored(project(normed, outgate_weight))
    log_decay = log_decays(normed, down_weight, up_weight, decay_bias)
    query_heads = query_rows.astype(jnp.float32).reshape(row_count, HEADS, DK) * DK ** (-0.5)
    key_heads = key_rows.astype(jnp.float32).reshape(row_count, HEADS, DK)
    value_heads = value_rows.astype(jnp.float32).reshape(row_count, HEADS, DV)
    log_heads = log_decay.reshape(row_count, HEADS, DK)
    forward_out = direction(query_heads, key_heads, value_heads, log_heads, ctx_forward)
    backward_out = jnp.flip(direction(jnp.flip(query_heads, 0), jnp.flip(key_heads, 0), jnp.flip(value_heads, 0), jnp.flip(log_heads, 0), ctx_backward), 0)
    mixed_heads = forward_out + backward_out
    normalized = mixed_heads * rms_factor(mixed_heads)
    gate_heads = jax.nn.silu(outgate_rows.astype(jnp.float32).reshape(row_count, HEADS, DV))
    gated = (normalized * gate_heads).reshape(row_count, HEADS * DV).astype(jnp.bfloat16)
    branch = stored(project(gated, out_weight)).astype(jnp.float32)
    result = latent.astype(jnp.float32) + gates[0] * (branch * rms_factor(branch)) * post_gain
    return result.astype(jnp.bfloat16)
```

```python
import functools
from types import SimpleNamespace

import jax
import jax.numpy as jnp
from jax import lax
from jax.experimental import pallas as pl
from jax.experimental.pallas import tpu as pltpu
from jax.sharding import PartitionSpec as P

HEADS = 16
DK = 32
DV = 64
LANES = 128
SUB = 8
GROUP = LANES // DK
GV = GROUP * DV
GROUPS = HEADS // GROUP
CREW = DV // SUB
MESH = pl.DeviceIdType.MESH
TILE = 64
COLS = 256
STRIP = 16
VMEM_LIMIT = 60 * 1024 * 1024

NAMES = (
    "latent",
    "context",
    "latent_condition",
    "context_condition",
    "shift_weight",
    "scale_weight",
    "gate_weight",
    "norm_gain",
    "query_weight",
    "key_weight",
    "value_weight",
    "outgate_weight",
    "down_weight",
    "up_weight",
    "decay_bias",
    "out_weight",
    "post_gain",
)
MODULATION = ("shift_weight", "scale_weight", "gate_weight")
LATER = (
    "down_weight",
    "up_weight",
    "key_weight",
    "value_weight",
    "query_weight",
    "outgate_weight",
    "out_weight",
)

epsilon = 1e-06
decay_temper = 16.0
f32 = jnp.float32
bf16 = jnp.bfloat16


def dot(a, b):
    return jnp.dot(a, b, preferred_element_type=f32)


def dot_nt(a, b):
    return lax.dot_general(a, b, (((1,), (1,)), ((), ())), preferred_element_type=f32)


def dot_tn(a, b):
    return lax.dot_general(a, b, (((0,), (0,)), ((), ())), preferred_element_type=f32)


def iota(shape, axis):
    return lax.broadcasted_iota(jnp.int32, shape, axis)


def lower_ones(rows):
    return jnp.where(iota((rows, rows), 0) >= iota((rows, rows), 1), 1.0, 0.0).astype(bf16)


def running_sum(lower, log_rows):
    high = log_rows.astype(bf16)
    rest = log_rows - high.astype(f32)
    mid = rest.astype(bf16)
    low = (rest - mid.astype(f32)).astype(bf16)
    return dot(lower, high) + dot(lower, mid) + dot(lower, low)


def log_decays(values):
    return (jnp.minimum(values, 0.0) - jnp.log1p(jnp.exp(-jnp.abs(values)))) / decay_temper


def rms_factor(values):
    return lax.rsqrt(jnp.mean(values * values, axis=-1, keepdims=True) + epsilon)


def per_head(full, head):
    out = full[(GROUP - 1) * DV :]
    for h in range(GROUP - 2, -1, -1):
        out = jnp.where(head == h, full[h * DV : (h + 1) * DV], out)
    return out


def stacked(values, head):
    zero = jnp.zeros_like(values)
    return jnp.concatenate([jnp.where(head == h, values, zero) for h in range(GROUP)], axis=0)


def block_kernel(sp_count, tp_count, *refs):
    hbm = SimpleNamespace(**dict(zip((*NAMES, "out"), refs)))
    vm = SimpleNamespace(**refs[-2])
    sem = SimpleNamespace(**refs[-1])

    count = sp_count * tp_count
    crews = count // CREW
    sp, tp = lax.axis_index("sp"), lax.axis_index("tp")
    me = sp * tp_count + tp
    crew, post = me // CREW, lax.rem(me, CREW)
    rows, width = hbm.latent.shape
    blocks = rows // TILE
    chunks = hbm.shift_weight.shape[1] // LANES
    row_share = hbm.shift_weight.shape[0]
    ctx_rows = vm.context.shape[0]
    ctx_group = lax.rem(tp, GROUPS)

    def place(flat):
        return (flat // tp_count, lax.rem(flat, tp_count))

    def remote(src, dst, send, recv, flat):
        return pltpu.make_async_remote_copy(
            src_ref=src,
            dst_ref=dst,
            send_sem=send,
            recv_sem=recv,
            device_id=place(flat),
            device_id_type=MESH,
        )

    def others(body, total):
        def step(i, carry):
            body(i)
            return carry

        lax.fori_loop(1, total, step, 0)

    def load(slot, src, dst):
        return pltpu.make_async_copy(src, dst, sem.load.at[slot])

    ctx_at = (tp // GROUPS) * ctx_rows
    first = [
        load(0, hbm.shift_weight, vm.shift_weight),
        load(1, hbm.scale_weight, vm.scale_weight),
        load(2, hbm.gate_weight, vm.gate_weight),
        load(3, hbm.context.at[pl.ds(pl.multiple_of(ctx_at, 8), ctx_rows)], vm.context),
        load(4, hbm.latent, vm.latent),
    ]
    later = {
        name: load(5 + i, getattr(hbm, name), getattr(vm, name)) for i, name in enumerate(LATER)
    }
    for copy in first:
        copy.start()

    barrier = pltpu.get_barrier_semaphore()
    others(
        lambda i: pl.semaphore_signal(
            barrier, inc=1, device_id=place(lax.rem(me + i, count)), device_id_type=MESH
        ),
        count,
    )

    mine = pl.ds(pl.multiple_of(sp * row_share, LANES), row_share)
    pick = iota((STRIP, row_share), 0) == 0
    raw = jnp.where(
        pick, hbm.latent_condition[:, mine].astype(f32), hbm.context_condition[:, mine].astype(f32)
    )
    cond = (raw / (1.0 + jnp.exp(-raw))).astype(bf16)
    for copy in later.values():
        copy.start()
    for which in range(3):
        first[which].wait()
        weight = (vm.shift_weight, vm.scale_weight, vm.gate_weight)[which]
        part = dot(cond, weight[...])
        for c in range(chunks):
            at = slice(c * LANES, (c + 1) * LANES)
            vm.part[c, which : which + 1, :] = part[0:1, at]
            vm.part[c, 3 + which : 4 + which, :] = part[1:2, at]
    pl.semaphore_wait(barrier, count - 1)

    def to_reducer(c):
        return remote(
            vm.part.at[c], vm.parts.at[crew], sem.part_send.at[c], sem.part_recv.at[crew], c * CREW + post
        )

    for c in range(chunks):

        @pl.when(crew != c)
        def _():
            to_reducer(c).start()

    first[3].wait()
    xc = vm.context[...].astype(f32)
    vm.ctx_scaled[...] = xc * rms_factor(xc)
    first[4].wait()

    def scale_strip(i, carry):
        at = pl.ds(pl.multiple_of(i * STRIP, STRIP), STRIP)
        x = vm.latent[at, :].astype(f32)
        vm.scaled[at, :] = x * rms_factor(x)
        return carry

    lax.fori_loop(0, rows // STRIP, scale_strip, 0)

    def spread(flat, slot):
        return remote(
            vm.total, vm.totals.at[slot], sem.total_send.at[flat], sem.total_recv.at[slot], flat
        )

    @pl.when(crew < chunks)
    def _():
        vm.parts[crew] = vm.part[crew]

        def arrived(i):
            source = lax.rem(crew + i, crews)
            remote(
                vm.part.at[0],
                vm.parts.at[source],
                sem.part_send.at[0],
                sem.part_recv.at[source],
                source * CREW + post,
            ).wait_recv()

        others(arrived, crews)
        total = vm.parts[0]
        for i in range(1, crews):
            total = total + vm.parts[i]
        vm.total[...] = total
        vm.totals[me] = total
        others(lambda i: spread(lax.rem(me + i, count), me).start(), count)

    def total_in(f, carry):
        @pl.when(f != me)
        def _():
            spread(f, f).wait_recv()

        return carry

    lax.fori_loop(0, chunks * CREW, total_in, 0)
    for t in range(tp_count):
        for c in range(chunks):
            tile = vm.totals[c * CREW + t]
            for x in range(1, CREW // tp_count):
                tile = tile + vm.totals[c * CREW + x * tp_count + t]
            at = (t * chunks + c) * LANES
            vm.mods[:, at : at + LANES] = tile

    gain = hbm.norm_gain[...] * (1.0 + vm.mods[4:5, :])
    ctx_normed = (vm.ctx_scaled[...] * gain + vm.mods[3:4, :]).astype(bf16)
    later["down_weight"].wait()
    later["up_weight"].wait()
    later["key_weight"].wait()
    later["value_weight"].wait()
    head_k = iota((DV, 2 * LANES), 1) % LANES // DK
    key_at = pl.ds(pl.multiple_of(ctx_group * LANES, LANES), LANES)
    val_at = pl.ds(pl.multiple_of(ctx_group * GV, GV), GV)
    low = dot(ctx_normed, vm.down_weight[...]).astype(bf16)
    log_rows = log_decays(dot(low, vm.up_weight[:, key_at]) + hbm.decay_bias[:, key_at])
    keys = dot(ctx_normed, vm.key_weight[:, key_at]).astype(bf16).astype(f32)
    values = dot(ctx_normed, vm.value_weight[:, val_at]).astype(bf16)
    inclusive = running_sum(lower_ones(ctx_rows), log_rows)
    closing = inclusive[ctx_rows - 1 : ctx_rows, :]
    both = jnp.concatenate(
        [keys * jnp.exp(closing - inclusive), keys * jnp.exp(inclusive - log_rows)], axis=1
    ).astype(bf16)
    state = per_head(dot_tn(values, both), head_k)
    for j in range(CREW):
        at = slice(j * SUB, (j + 1) * SUB)
        vm.ctx_out[j] = jnp.concatenate([state[at, :LANES], state[at, LANES:]], axis=0).astype(bf16)
    vm.ctx_log[...] = closing

    def ctx_copies(flat, slot):
        return (
            remote(
                vm.ctx_out.at[lax.rem(flat, CREW)],
                vm.ctx_in.at[slot],
                sem.ctx_send.at[flat],
                sem.ctx_recv.at[slot],
                flat,
            ),
            remote(
                vm.ctx_log, vm.ctx_logs.at[slot], sem.ctx_log_send.at[flat], sem.ctx_log_recv.at[slot], flat
            ),
        )

    def ctx_start(i):
        for copy in ctx_copies(lax.rem(me + i, count), me):
            copy.start()

    others(ctx_start, count)
    vm.ctx_in[me] = vm.ctx_out[post]
    vm.ctx_logs[me] = closing

    gain = hbm.norm_gain[...] * (1.0 + vm.mods[1:2, :])
    shift = vm.mods[0:1, :]

    def norm_strip(i, carry):
        at = pl.ds(pl.multiple_of(i * STRIP, STRIP), STRIP)
        vm.normed[at, :] = (vm.scaled[at, :] * gain + shift).astype(bf16)
        return carry

    lax.fori_loop(0, rows // STRIP, norm_strip, 0)

    def project(weight, out):
        for n in range(0, weight.shape[1], COLS):
            at = slice(n, n + COLS)
            out[:, at] = dot(vm.normed[...], weight[:, at]).astype(bf16)

    low = dot(vm.normed[...], vm.down_weight[...]).astype(bf16)
    log_all = log_decays(dot(low, vm.up_weight[...]) + hbm.decay_bias[...])
    lower = lower_ones(TILE)
    ends = []
    for b in range(blocks):
        at = slice(b * TILE, (b + 1) * TILE)
        log_rows = log_all[at]
        inclusive = running_sum(lower, log_rows)
        vm.inclusive[at, :] = inclusive
        vm.before[at, :] = inclusive - log_rows
        ends.append(inclusive[TILE - 1 : TILE, :])
        vm.closing[b : b + 1, :] = ends[b]
    segment_log = functools.reduce(lambda a, b: a + b, ends)
    for g in range(GROUPS):
        vm.log_out[g : g + 1, :] = segment_log[:, g * LANES : (g + 1) * LANES]

    def mate(i):
        return lax.rem(post + i, CREW)

    def log_copy(p, slot):
        return remote(
            vm.log_out, vm.logs.at[slot], sem.log_send.at[p], sem.log_recv.at[slot], crew * CREW + p
        )

    others(lambda i: log_copy(mate(i), post).start(), CREW)
    vm.logs[post] = vm.log_out[...]
    project(vm.key_weight, vm.key)

    def seg_copy(p, slot, g):
        return remote(
            vm.seg_out.at[g, p],
            vm.seg_in.at[g, slot],
            sem.seg_send.at[g, p],
            sem.seg_recv.at[g, slot],
            crew * CREW + p,
        )

    for g in range(GROUPS):
        lanes = slice(g * LANES, (g + 1) * LANES)
        v_lanes = slice(g * GV, (g + 1) * GV)
        vm.value[:, v_lanes] = dot(vm.normed[...], vm.value_weight[:, v_lanes]).astype(bf16)
        decays = [jnp.exp(vm.closing[b : b + 1, lanes]) for b in range(blocks)]
        for b in range(blocks):
            at = slice(b * TILE, (b + 1) * TILE)
            keys = vm.key[at, lanes].astype(f32)
            both = jnp.concatenate(
                [
                    keys * jnp.exp(vm.closing[b : b + 1, lanes] - vm.inclusive[at, lanes]),
                    keys * jnp.exp(vm.before[at, lanes]),
                ],
                axis=1,
            ).astype(bf16)
            vm.summary[g, b] = per_head(dot_tn(vm.value[at, v_lanes], both), head_k)
        forward = vm.summary[g, 0, :, :LANES]
        for b in range(1, blocks):
            forward = decays[b] * forward + vm.summary[g, b, :, :LANES]
        backward = vm.summary[g, blocks - 1, :, LANES:]
        for b in range(blocks - 2, -1, -1):
            backward = decays[b] * backward + vm.summary[g, b, :, LANES:]
        for j in range(CREW):
            at = slice(j * SUB, (j + 1) * SUB)
            vm.seg_out[g, j] = jnp.concatenate([forward[at], backward[at]], axis=0).astype(bf16)
        others(lambda i: seg_copy(mate(i), post, g).start(), CREW)
        vm.seg_in[g, post] = vm.seg_out[g, post]

    head_k1 = iota((TILE, LANES), 1) // DK
    head_v = iota((TILE, GV), 1) // DV
    t_index = iota((TILE, GROUP * TILE), 0)
    s_index = iota((TILE, GROUP * TILE), 1) % TILE

    def inside(g):
        lanes = slice(g * LANES, (g + 1) * LANES)
        v_lanes = slice(g * GV, (g + 1) * GV)
        for b in range(blocks):
            at = slice(b * TILE, (b + 1) * TILE)
            inclusive, before = vm.inclusive[at, lanes], vm.before[at, lanes]
            closing = inclusive[TILE - 1 : TILE, :]
            middle = inclusive[TILE // 2 - 1 : TILE // 2, :]
            queries = vm.query[at, lanes].astype(f32) * DK ** (-0.5)
            keys = vm.key[at, lanes].astype(f32)
            scores = []
            for q_log, k_log in (
                (inclusive - middle, middle - inclusive),
                (middle - before, before - middle),
            ):
                k_stack = stacked((keys * jnp.exp(k_log)).astype(bf16), head_k1)
                scores.append(dot_nt((queries * jnp.exp(q_log)).astype(bf16), k_stack))
            both = jnp.where(t_index >= s_index, scores[0], 0.0) + jnp.where(
                t_index <= s_index, scores[1], 0.0
            )
            v_stack = stacked(vm.value[at, v_lanes], head_v)
            vm.within[at, v_lanes] = dot(both.astype(bf16), v_stack)
            vm.q_across[g, at, :] = jnp.concatenate(
                [queries * jnp.exp(inclusive), queries * jnp.exp(closing - before)], axis=1
            ).astype(bf16)

    later["query_weight"].wait()
    project(vm.query_weight, vm.query)
    inside(0)

    def log_in(i):
        log_copy(mate(i), mate(i)).wait_recv()

    others(log_in, CREW)
    decays = [[jnp.exp(vm.logs[p, g : g + 1, :]) for g in range(GROUPS)] for p in range(CREW)]
    crew_log = vm.logs[0]
    for p in range(1, CREW):
        crew_log = crew_log + vm.logs[p]
    side = GROUPS * SUB
    vm.crew_out[side : side + SUB, :] = crew_log
    for g in range(GROUPS):
        others(lambda i: seg_copy(mate(i), mate(i), g).wait_recv(), CREW)
        forward = vm.seg_in[g, 0].astype(f32)[:SUB]
        for p in range(1, CREW):
            forward = decays[p][g] * forward + vm.seg_in[g, p].astype(f32)[:SUB]
        backward = vm.seg_in[g, CREW - 1].astype(f32)[SUB:]
        for p in range(CREW - 2, -1, -1):
            backward = decays[p][g] * backward + vm.seg_in[g, p].astype(f32)[SUB:]
        vm.crew_out[g * SUB : (g + 1) * SUB, :] = forward
        at = side + SUB + g * SUB
        vm.crew_out[at : at + SUB, :] = backward

    def crew_copy(c, slot, ahead):
        part = pl.ds(0, side + SUB) if ahead else pl.ds(side, side + SUB)
        return remote(
            vm.crew_out.at[part],
            vm.crew_in.at[slot, part],
            sem.crew_send.at[c],
            sem.crew_recv.at[slot],
            c * CREW + post,
        )

    def crew_start(i):
        c = lax.rem(crew + i, crews)

        @pl.when(c > crew)
        def _():
            crew_copy(c, crew, True).start()

        @pl.when(c < crew)
        def _():
            crew_copy(c, crew, False).start()

    others(crew_start, crews)
    for g in range(1, GROUPS):
        inside(g)

    def ctx_arrived(i):
        flat = lax.rem(me + i, count)
        for copy in ctx_copies(flat, flat):
            copy.wait_recv()

    others(ctx_arrived, count)
    parts = count // GROUPS
    zero = jnp.zeros((SUB, LANES), f32)

    def ctx_chain(i, carry):
        out = []
        for g in range(GROUPS):
            a = i * GROUPS + g
            z = (parts - 1 - i) * GROUPS + g
            out.append(jnp.exp(vm.ctx_logs[a]) * carry[2 * g] + vm.ctx_in[a].astype(f32)[:SUB])
            out.append(jnp.exp(vm.ctx_logs[z]) * carry[2 * g + 1] + vm.ctx_in[z].astype(f32)[SUB:])
        return tuple(out)

    carry = lax.fori_loop(0, parts, ctx_chain, (zero,) * (2 * GROUPS))

    def from_before(c, states):
        crew_copy(c, c, True).wait_recv()
        return tuple(
            jnp.exp(vm.crew_in[c, side + g : side + g + 1, :]) * states[g]
            + vm.crew_in[c, g * SUB : (g + 1) * SUB, :]
            for g in range(GROUPS)
        )

    def from_after(i, states):
        c = crews - 1 - i
        crew_copy(c, c, False).wait_recv()
        at = side + SUB
        return tuple(
            jnp.exp(vm.crew_in[c, side + g : side + g + 1, :]) * states[g]
            + vm.crew_in[c, at + g * SUB : at + (g + 1) * SUB, :]
            for g in range(GROUPS)
        )

    forward = lax.fori_loop(0, crew, from_before, tuple(carry[0::2]))
    backward = lax.fori_loop(0, crews - 1 - crew, from_after, tuple(carry[1::2]))
    for g in range(GROUPS):
        state = forward[g]
        entering = []
        for p in range(CREW):
            entering.append(state)
            state = decays[p][g] * state + vm.seg_in[g, p].astype(f32)[:SUB]
        state = backward[g]
        for p in range(CREW - 1, -1, -1):
            vm.enter_out[p, g] = jnp.concatenate([entering[p], state], axis=0).astype(bf16)
            state = decays[p][g] * state + vm.seg_in[g, p].astype(f32)[SUB:]

    def enter_copy(p, slot):
        return remote(
            vm.enter_out.at[p],
            vm.enter_in.at[slot],
            sem.enter_send.at[p],
            sem.enter_recv.at[slot],
            crew * CREW + p,
        )

    others(lambda i: enter_copy(mate(i), post).start(), CREW)
    vm.enter_in[post] = vm.enter_out[post]

    later["outgate_weight"].wait()
    project(vm.outgate_weight, vm.outgate)
    head_mean = jnp.where(iota((GV, GV), 0) // DV == iota((GV, GV), 1) // DV, 1.0 / DV, 0.0).astype(bf16)

    others(lambda i: enter_copy(mate(i), mate(i)).wait_recv(), CREW)
    for g in range(GROUPS):
        lanes = slice(g * LANES, (g + 1) * LANES)
        v_lanes = slice(g * GV, (g + 1) * GV)
        units = [vm.enter_in[j, g].astype(f32) for j in range(CREW)]
        decays = [jnp.exp(vm.closing[b : b + 1, lanes]) for b in range(blocks)]
        forward = [jnp.concatenate([u[:SUB] for u in units], axis=0)]
        for b in range(blocks - 1):
            forward.append(decays[b] * forward[b] + vm.summary[g, b, :, :LANES])
        backward = [jnp.concatenate([u[SUB:] for u in units], axis=0)]
        for b in range(blocks - 1, 0, -1):
            backward.insert(0, decays[b] * backward[0] + vm.summary[g, b, :, LANES:])
        for b in range(blocks):
            at = slice(b * TILE, (b + 1) * TILE)
            entering = jnp.concatenate([forward[b], backward[b]], axis=1)
            across = dot_nt(vm.q_across[g, at, :], stacked(entering, head_k).astype(bf16))
            mixed = vm.within[at, v_lanes] + across
            square = mixed * mixed
            high = square.astype(bf16)
            rest = (square - high.astype(f32)).astype(bf16)
            mean = dot(high, head_mean) + dot(rest, head_mean)
            gate = vm.outgate[at, v_lanes].astype(f32)
            silu = gate / (1.0 + jnp.exp(-gate))
            vm.gated[at, v_lanes] = (mixed * lax.rsqrt(mean + epsilon) * silu).astype(bf16)

    later["out_weight"].wait()
    for n in range(0, width, COLS):
        at = slice(n, n + COLS)
        vm.branch[:, at] = dot(vm.gated[...], vm.out_weight[:, at]).astype(bf16)
    gain = vm.mods[2:3, :] * hbm.post_gain[...]

    def store(i):
        at = pl.ds(pl.multiple_of(i * TILE, TILE), TILE)
        return pltpu.make_async_copy(vm.updated.at[at], hbm.out.at[at], sem.store.at[i])

    def final_block(b, carry):
        for s in range(TILE // STRIP):
            at = pl.ds(pl.multiple_of(b * TILE + s * STRIP, STRIP), STRIP)
            branch = vm.branch[at, :].astype(f32)
            vm.updated[at, :] = (
                vm.latent[at, :].astype(f32) + gain * (branch * rms_factor(branch))
            ).astype(bf16)
        store(b).start()
        return carry

    lax.fori_loop(0, blocks, final_block, 0)

    for c in range(chunks):

        @pl.when(crew != c)
        def _():
            to_reducer(c).wait_send()

    @pl.when(crew < chunks)
    def _():
        others(lambda i: spread(lax.rem(me + i, count), me).wait_send(), count)

    def ctx_sent(i):
        for copy in ctx_copies(lax.rem(me + i, count), me):
            copy.wait_send()

    others(ctx_sent, count)

    def mate_sent(i):
        log_copy(mate(i), post).wait_send()
        enter_copy(mate(i), post).wait_send()
        for g in range(GROUPS):
            seg_copy(mate(i), post, g).wait_send()

    others(mate_sent, CREW)

    def crew_sent(i):
        crew_copy(lax.rem(crew + i, crews), crew, True).wait_send()

    others(crew_sent, crews)
    for b in range(blocks):
        store(b).wait()


def shards(*operands):
    values = dict(zip(NAMES, operands))
    latent, context = values["latent"], values["context"]
    sp_count, tp_count = lax.axis_size("sp"), lax.axis_size("tp")
    count = sp_count * tp_count
    crews = count // CREW
    rows, width = latent.shape
    args, specs = [], []
    for value in operands:
        vector = value.ndim == 1
        args.append(value.reshape(1, -1) if vector else value)
        specs.append(pl.BlockSpec(memory_space=pltpu.VMEM if vector else pl.ANY))
    ctx_rows = context.shape[0] * GROUPS // tp_count
    chunks = values["shift_weight"].shape[1] // LANES
    keyw, valw = values["key_weight"].shape[1], values["value_weight"].shape[1]
    blocks = rows // TILE
    side = GROUPS * SUB
    buffers = dict(
        latent=pltpu.VMEM((rows, width), bf16),
        context=pltpu.VMEM((ctx_rows, width), bf16),
        part=pltpu.VMEM((chunks, SUB, LANES), f32),
        parts=pltpu.VMEM((crews, SUB, LANES), f32),
        total=pltpu.VMEM((SUB, LANES), f32),
        totals=pltpu.VMEM((chunks * CREW, SUB, LANES), f32),
        mods=pltpu.VMEM((SUB, width), f32),
        scaled=pltpu.VMEM((rows, width), f32),
        ctx_scaled=pltpu.VMEM((ctx_rows, width), f32),
        normed=pltpu.VMEM((rows, width), bf16),
        ctx_out=pltpu.VMEM((CREW, 2 * SUB, LANES), bf16),
        ctx_in=pltpu.VMEM((count, 2 * SUB, LANES), bf16),
        ctx_log=pltpu.VMEM((1, LANES), f32),
        ctx_logs=pltpu.VMEM((count, 1, LANES), f32),
        key=pltpu.VMEM((rows, keyw), bf16),
        query=pltpu.VMEM((rows, keyw), bf16),
        value=pltpu.VMEM((rows, valw), bf16),
        outgate=pltpu.VMEM((rows, valw), bf16),
        gated=pltpu.VMEM((rows, valw), bf16),
        inclusive=pltpu.VMEM((rows, keyw), f32),
        before=pltpu.VMEM((rows, keyw), f32),
        closing=pltpu.VMEM((SUB, keyw), f32),
        log_out=pltpu.VMEM((SUB, LANES), f32),
        logs=pltpu.VMEM((CREW, SUB, LANES), f32),
        summary=pltpu.VMEM((GROUPS, blocks, DV, 2 * LANES), f32),
        seg_out=pltpu.VMEM((GROUPS, CREW, 2 * SUB, LANES), bf16),
        seg_in=pltpu.VMEM((GROUPS, CREW, 2 * SUB, LANES), bf16),
        crew_out=pltpu.VMEM((2 * side + SUB, LANES), f32),
        crew_in=pltpu.VMEM((crews, 2 * side + SUB, LANES), f32),
        enter_out=pltpu.VMEM((CREW, GROUPS, 2 * SUB, LANES), bf16),
        enter_in=pltpu.VMEM((CREW, GROUPS, 2 * SUB, LANES), bf16),
        q_across=pltpu.VMEM((GROUPS, rows, 2 * LANES), bf16),
        within=pltpu.VMEM((rows, valw), f32),
        branch=pltpu.VMEM((rows, width), bf16),
        updated=pltpu.VMEM((rows, width), bf16),
    )
    for name in MODULATION + LATER:
        buffers[name] = pltpu.VMEM(values[name].shape, bf16)
    dma = pltpu.SemaphoreType.DMA
    semaphores = dict(
        load=dma((12,)),
        store=dma((blocks,)),
        part_send=dma((chunks,)),
        part_recv=dma((crews,)),
        total_send=dma((count,)),
        total_recv=dma((chunks * CREW,)),
        ctx_send=dma((count,)),
        ctx_recv=dma((count,)),
        ctx_log_send=dma((count,)),
        ctx_log_recv=dma((count,)),
        log_send=dma((CREW,)),
        log_recv=dma((CREW,)),
        seg_send=dma((GROUPS, CREW)),
        seg_recv=dma((GROUPS, CREW)),
        crew_send=dma((crews,)),
        crew_recv=dma((crews,)),
        enter_send=dma((CREW,)),
        enter_recv=dma((CREW,)),
    )
    return pl.pallas_call(
        functools.partial(block_kernel, sp_count, tp_count),
        out_shape=jax.ShapeDtypeStruct((rows, width), bf16),
        in_specs=specs,
        out_specs=pl.BlockSpec(memory_space=pl.ANY),
        scratch_shapes=[buffers, semaphores],
        compiler_params=pltpu.CompilerParams(
            collective_id=0, has_side_effects=True, vmem_limit_bytes=VMEM_LIMIT
        ),
        name="block",
    )(*args)


def solution(mesh):
    placed = (
        P(("sp", "tp"), None),
        P("sp", None),
        P(),
        P(),
        P("sp", "tp"),
        P("sp", "tp"),
        P("sp", "tp"),
        P(),
        P(),
        P(),
        P(),
        P(),
        P(),
        P(),
        P(),
        P(),
        P(),
    )
    return jax.shard_map(
        shards, mesh=mesh, in_specs=placed, out_specs=P(("sp", "tp"), None), check_vma=False
    )
```

```python
import functools
from types import SimpleNamespace

import jax
import jax.numpy as jnp
from jax import lax
from jax.experimental import pallas as pl
from jax.experimental.pallas import tpu as pltpu
from jax.sharding import PartitionSpec as P

HEADS = 16
DK = 32
DV = 64
LANES = 128
SUB = 8
GROUP = LANES // DK
GV = GROUP * DV
GROUPS = HEADS // GROUP
CREW = DV // SUB
MESH = pl.DeviceIdType.MESH
TILE = 64
COLS = 256
STRIP = 16
VMEM_LIMIT = 60 * 1024 * 1024

NAMES = (
    "latent",
    "context",
    "latent_condition",
    "context_condition",
    "shift_weight",
    "scale_weight",
    "gate_weight",
    "norm_gain",
    "query_weight",
    "key_weight",
    "value_weight",
    "outgate_weight",
    "down_weight",
    "up_weight",
    "decay_bias",
    "out_weight",
    "post_gain",
)
FIRST = (
    "latent_condition",
    "context_condition",
    "shift_weight",
    "scale_weight",
    "gate_weight",
    "context",
    "latent",
)
LATER = (
    "norm_gain",
    "decay_bias",
    "post_gain",
    "down_weight",
    "up_weight",
    "key_weight",
    "value_weight",
    "query_weight",
    "outgate_weight",
    "out_weight",
)

epsilon = 1e-06
decay_temper = 16.0
f32 = jnp.float32
bf16 = jnp.bfloat16


def dot(a, b):
    return jnp.dot(a, b, preferred_element_type=f32)


def dot_nt(a, b):
    return lax.dot_general(a, b, (((1,), (1,)), ((), ())), preferred_element_type=f32)


def dot_tn(a, b):
    return lax.dot_general(a, b, (((0,), (0,)), ((), ())), preferred_element_type=f32)


def iota(shape, axis):
    return lax.broadcasted_iota(jnp.int32, shape, axis)


def lower_ones(rows):
    return jnp.where(iota((rows, rows), 0) >= iota((rows, rows), 1), 1.0, 0.0).astype(bf16)


def running_sum(lower, log_rows):
    high = log_rows.astype(bf16)
    rest = log_rows - high.astype(f32)
    mid = rest.astype(bf16)
    low = (rest - mid.astype(f32)).astype(bf16)
    return dot(lower, high) + dot(lower, mid) + dot(lower, low)


def log_decays(values):
    return (jnp.minimum(values, 0.0) - jnp.log1p(jnp.exp(-jnp.abs(values)))) / decay_temper


def rms_factor(values):
    return lax.rsqrt(jnp.mean(values * values, axis=-1, keepdims=True) + epsilon)


def per_head(full, head):
    out = full[(GROUP - 1) * DV :]
    for h in range(GROUP - 2, -1, -1):
        out = jnp.where(head == h, full[h * DV : (h + 1) * DV], out)
    return out


def stacked(values, head):
    zero = jnp.zeros_like(values)
    return jnp.concatenate([jnp.where(head == h, values, zero) for h in range(GROUP)], axis=0)


def reduction(chunks, crews):
    reducers = min(2, chunks, crews)
    return reducers, chunks // reducers


def block_kernel(sp_count, tp_count, *refs):
    hbm = SimpleNamespace(**dict(zip((*NAMES, "out"), refs)))
    vm = SimpleNamespace(**refs[-2])
    sem = SimpleNamespace(**refs[-1])

    count = sp_count * tp_count
    crews = count // CREW
    sp, tp = lax.axis_index("sp"), lax.axis_index("tp")
    me = sp * tp_count + tp
    crew, post = me // CREW, lax.rem(me, CREW)
    rows, width = hbm.latent.shape
    blocks = rows // TILE
    row_share = hbm.shift_weight.shape[0]
    chunks = hbm.shift_weight.shape[1] // LANES
    reducers, share = reduction(chunks, crews)
    first_reducer = (crews - reducers) // 2
    ctx_rows = vm.context.shape[0]
    ctx_group = lax.rem(tp, GROUPS)

    def place(flat):
        return (flat // tp_count, lax.rem(flat, tp_count))

    def remote(src, dst, send, recv, flat):
        return pltpu.make_async_remote_copy(
            src_ref=src,
            dst_ref=dst,
            send_sem=send,
            recv_sem=recv,
            device_id=place(flat),
            device_id_type=MESH,
        )

    def others(body, total):
        def step(i, carry):
            body(i)
            return carry

        lax.fori_loop(1, total, step, 0)

    def mate(i):
        return lax.rem(post + i, CREW)

    def mates(body):
        for i in range(1, CREW):
            body(mate(i))

    ctx_at = pl.multiple_of((tp // GROUPS) * ctx_rows, SUB)
    hbm.context = hbm.context.at[pl.ds(ctx_at, ctx_rows)]
    loads = {
        name: pltpu.make_async_copy(getattr(hbm, name), getattr(vm, name), sem.load.at[i])
        for i, name in enumerate(FIRST + LATER)
    }
    for name in FIRST:
        loads[name].start()

    barrier = pltpu.get_barrier_semaphore()
    others(
        lambda i: pl.semaphore_signal(
            barrier, inc=1, device_id=place(lax.rem(me + i, count)), device_id_type=MESH
        ),
        count,
    )

    loads["latent_condition"].wait()
    loads["context_condition"].wait()
    vm.cond[0:1, :] = vm.latent_condition[...].astype(f32).reshape(1, width)
    vm.cond[1:2, :] = vm.context_condition[...].astype(f32).reshape(1, width)
    mine = pl.ds(pl.multiple_of(sp * row_share, LANES), row_share)
    pick = iota((STRIP, row_share), 0) == 0
    raw = jnp.where(pick, vm.cond[0:1, mine], vm.cond[1:2, mine])
    cond = (raw / (1.0 + jnp.exp(-raw))).astype(bf16)
    for name in LATER:
        loads[name].start()
    for which, name in enumerate(("shift_weight", "scale_weight", "gate_weight")):
        loads[name].wait()
        part = dot(cond, getattr(vm, name)[...])
        for c in range(chunks):
            at = slice(c * LANES, (c + 1) * LANES)
            r, row = c // share, c % share
            if which == 2:
                vm.gate_part[r, row] = part[0:1, at]
            else:
                vm.part[r, row * 4 + which : row * 4 + which + 1, :] = part[0:1, at]
                vm.part[r, row * 4 + 2 + which : row * 4 + 3 + which, :] = part[1:2, at]
    pl.semaphore_wait(barrier, count - 1)

    def to_reducer(r, slot):
        flat = (first_reducer + r) * CREW + post
        return (
            remote(vm.part.at[r], vm.parts.at[slot], sem.part_send.at[r], sem.part_recv.at[slot], flat),
            remote(
                vm.gate_part.at[r],
                vm.gate_parts.at[slot],
                sem.gate_part_send.at[r],
                sem.gate_part_recv.at[slot],
                flat,
            ),
        )

    for which in range(2):
        for r in range(reducers):

            @pl.when(crew != first_reducer + r)
            def _():
                to_reducer(r, crew)[which].start()

    loads["context"].wait()
    xc = vm.context[...].astype(f32)
    vm.ctx_scaled[...] = xc * rms_factor(xc)
    loads["latent"].wait()

    def scale_strip(i, carry):
        at = pl.ds(pl.multiple_of(i * TILE, TILE), TILE)
        x = vm.latent[at, :].astype(f32)
        vm.scaled[at, :] = x * rms_factor(x)
        return carry

    lax.fori_loop(0, rows // TILE, scale_strip, 0)

    reduced = reducers * CREW

    def spread(flat, slot):
        return remote(
            vm.total, vm.totals.at[slot], sem.total_send.at[flat], sem.total_recv.at[slot], flat
        )

    def gate_spread(flat, slot):
        return remote(
            vm.gate_total,
            vm.gate_totals.at[slot],
            sem.gate_send.at[flat],
            sem.gate_recv.at[slot],
            flat,
        )

    def reduce_here(which, mine, held, total, totals, copy):
        for r in range(reducers):
            home = first_reducer + r

            @pl.when(crew == home)
            def _():
                slot = r * CREW + post
                out = mine[r]
                for c in range(crews):
                    if c != home:
                        to_reducer(r, c)[which].wait_recv()
                        out = out + held[c]
                total[...] = out
                totals[slot] = out
                for c in sorted(range(crews), key=lambda c: -abs(c - home)):

                    def send(i, carry):
                        flat = c * CREW + mate(i)
                        copy(flat, slot).start()
                        return carry

                    lax.fori_loop(0 if c != home else 1, CREW, send, 0)

    def arrivals(copy):
        def arrived(i, carry):
            @pl.when(first_reducer * CREW + i != me)
            def _():
                copy(me, i).wait_recv()

            return carry

        lax.fori_loop(0, reduced, arrived, 0)

    def sent(copy):
        @pl.when((crew >= first_reducer) & (crew < first_reducer + reducers))
        def _():
            others(lambda i: copy(lax.rem(me + i, count), 0).wait_send(), count)

    reduce_here(0, vm.part, vm.parts, vm.total, vm.totals, spread)
    loads_needed = ("norm_gain", "decay_bias", "post_gain", "down_weight", "up_weight", "key_weight")
    for name in loads_needed + ("value_weight",):
        loads[name].wait()
    arrivals(spread)
    for r in range(reducers):
        for t in range(tp_count):
            tile = vm.totals[r * CREW + t]
            for x in range(1, CREW // tp_count):
                tile = tile + vm.totals[r * CREW + x * tp_count + t]
            for s in range(share):
                at = (t * chunks + r * share + s) * LANES
                vm.mods[0:4, at : at + LANES] = tile[s * 4 : s * 4 + 4]

    gain = vm.norm_gain[...] * (1.0 + vm.mods[3:4, :])
    ctx_normed = (vm.ctx_scaled[...] * gain + vm.mods[2:3, :]).astype(bf16)
    head_k = iota((DV, 2 * LANES), 1) % LANES // DK
    key_at = pl.ds(pl.multiple_of(ctx_group * LANES, LANES), LANES)
    val_at = pl.ds(pl.multiple_of(ctx_group * GV, GV), GV)
    low = dot_nt(ctx_normed, vm.down_weight[...]).astype(bf16)
    log_rows = log_decays(dot(low, vm.up_weight[:, key_at]) + vm.decay_bias[:, key_at])
    keys = dot(ctx_normed, vm.key_weight[:, key_at]).astype(bf16).astype(f32)
    values = dot(ctx_normed, vm.value_weight[:, val_at]).astype(bf16)
    inclusive = running_sum(lower_ones(ctx_rows), log_rows)
    closing = inclusive[ctx_rows - 1 : ctx_rows, :]
    both = jnp.concatenate(
        [keys * jnp.exp(closing - inclusive), keys * jnp.exp(inclusive - log_rows)], axis=1
    ).astype(bf16)
    state = per_head(dot_tn(values, both), head_k)
    for j in range(CREW):
        at = slice(j * SUB, (j + 1) * SUB)
        vm.ctx_out[j] = jnp.concatenate([state[at, :LANES], state[at, LANES:]], axis=0).astype(bf16)
    vm.ctx_log[...] = closing

    def ctx_copies(p, slot):
        flat = crew * CREW + p
        return (
            remote(vm.ctx_out.at[p], vm.ctx_in.at[slot], sem.ctx_send.at[p], sem.ctx_recv.at[slot], flat),
            remote(
                vm.ctx_log, vm.ctx_logs.at[slot], sem.ctx_log_send.at[p], sem.ctx_log_recv.at[slot], flat
            ),
        )

    def ctx_start(p):
        for copy in ctx_copies(p, post):
            copy.start()

    mates(ctx_start)
    vm.ctx_in[post] = vm.ctx_out[post]
    vm.ctx_logs[post] = closing

    gain = vm.norm_gain[...] * (1.0 + vm.mods[1:2, :])
    shift = vm.mods[0:1, :]
    for i in range(rows // STRIP):
        at = slice(i * STRIP, (i + 1) * STRIP)
        vm.normed[at, :] = (vm.scaled[at, :] * gain + shift).astype(bf16)

    def project(weight, out):
        for n in range(0, weight.shape[1], COLS):
            at = slice(n, n + COLS)
            out[:, at] = dot(vm.normed[...], weight[:, at]).astype(bf16)

    low = dot_nt(vm.normed[...], vm.down_weight[...]).astype(bf16)
    log_all = log_decays(dot(low, vm.up_weight[...]) + vm.decay_bias[...])
    lower = lower_ones(TILE)
    offset = None
    for b in range(blocks):
        at = slice(b * TILE, (b + 1) * TILE)
        log_rows = log_all[at]
        inclusive = running_sum(lower, log_rows)
        end = inclusive[TILE - 1 : TILE, :]
        vm.inclusive[at, :] = inclusive
        vm.before[at, :] = inclusive - log_rows
        vm.closing[b : b + 1, :] = end
        vm.offset[b : b + 1, :] = jnp.zeros_like(end) if offset is None else offset
        offset = end if offset is None else offset + end
    vm.offset[blocks : blocks + 1, :] = offset
    for g in range(GROUPS):
        vm.log_out[g : g + 1, :] = offset[:, g * LANES : (g + 1) * LANES]
    project(vm.key_weight, vm.key)
    project(vm.value_weight, vm.value)

    def log_copy(p, slot):
        return remote(
            vm.log_out, vm.logs.at[slot], sem.log_send.at[p], sem.log_recv.at[slot], crew * CREW + p
        )

    mates(lambda p: log_copy(p, post).start())
    vm.logs[post] = vm.log_out[...]

    def ctx_in(p):
        for copy in ctx_copies(p, p):
            copy.wait_recv()

    mates(ctx_in)
    for g in range(GROUPS):
        posts = list(range(g, CREW, GROUPS))
        logs = [vm.ctx_logs[p] for p in posts]
        tiles = [vm.ctx_in[p].astype(f32) for p in posts]
        forward, backward, log_sum = tiles[0][:SUB], tiles[-1][SUB:], logs[0]
        for i in range(1, len(posts)):
            forward = jnp.exp(logs[i]) * forward + tiles[i][:SUB]
            backward = jnp.exp(logs[-1 - i]) * backward + tiles[-1 - i][SUB:]
            log_sum = log_sum + logs[i]
        vm.ctx_crews_out[g] = jnp.concatenate([forward, backward], axis=0).astype(bf16)
        vm.ctx_crews_log[g : g + 1, :] = log_sum

    def ctx_crew_copies(c, slot):
        flat = c * CREW + post
        return (
            remote(
                vm.ctx_crews_out,
                vm.ctx_crews.at[slot],
                sem.ctx_crew_send.at[c],
                sem.ctx_crew_recv.at[slot],
                flat,
            ),
            remote(
                vm.ctx_crews_log,
                vm.ctx_crews_logs.at[slot],
                sem.ctx_crew_log_send.at[c],
                sem.ctx_crew_log_recv.at[slot],
                flat,
            ),
        )

    def ctx_crew_start(i):
        for copy in ctx_crew_copies(lax.rem(crew + i, crews), crew):
            copy.start()

    others(ctx_crew_start, crews)
    vm.ctx_crews[crew] = vm.ctx_crews_out[...]
    vm.ctx_crews_logs[crew] = vm.ctx_crews_log[...]

    def seg_copy(p, slot, g):
        return remote(
            vm.seg_out.at[g, p],
            vm.seg_in.at[g, slot],
            sem.seg_send.at[g, p],
            sem.seg_recv.at[g, slot],
            crew * CREW + p,
        )

    for g in range(GROUPS):
        lanes = slice(g * LANES, (g + 1) * LANES)
        v_lanes = slice(g * GV, (g + 1) * GV)
        whole = vm.offset[blocks : blocks + 1, lanes]
        both = []
        for b in range(blocks):
            at = slice(b * TILE, (b + 1) * TILE)
            keys = vm.key[at, lanes].astype(f32)
            start = vm.offset[b : b + 1, lanes]
            after = (whole - start) - vm.inclusive[at, lanes]
            both.append(
                jnp.concatenate(
                    [keys * jnp.exp(after), keys * jnp.exp(start + vm.before[at, lanes])], axis=1
                ).astype(bf16)
            )
        state = per_head(dot_tn(vm.value[:, v_lanes], jnp.concatenate(both, axis=0)), head_k)
        for j in range(CREW):
            at = slice(j * SUB, (j + 1) * SUB)
            vm.seg_out[g, j] = jnp.concatenate([state[at, :LANES], state[at, LANES:]], axis=0).astype(bf16)
        mates(lambda p: seg_copy(p, post, g).start())
        vm.seg_in[g, post] = vm.seg_out[g, post]

    mates(lambda p: log_copy(p, p).wait_recv())
    crew_log = vm.logs[0]
    for p in range(1, CREW):
        crew_log = crew_log + vm.logs[p]
    vm.crew_log[...] = crew_log

    def crew_log_copy(c, slot):
        return remote(
            vm.crew_log,
            vm.crew_logs.at[slot],
            sem.crew_log_send.at[c],
            sem.crew_log_recv.at[slot],
            c * CREW + post,
        )

    others(lambda i: crew_log_copy(lax.rem(crew + i, crews), crew).start(), crews)

    head_k1 = iota((TILE, LANES), 1) // DK
    head_v = iota((TILE, GV), 1) // DV
    t_index = iota((TILE, GROUP * TILE), 0)
    s_index = iota((TILE, GROUP * TILE), 1) % TILE

    def inside(g):
        lanes = slice(g * LANES, (g + 1) * LANES)
        v_lanes = slice(g * GV, (g + 1) * GV)
        whole = vm.offset[blocks : blocks + 1, lanes]
        for b in range(blocks):
            at = slice(b * TILE, (b + 1) * TILE)
            inclusive, before = vm.inclusive[at, lanes], vm.before[at, lanes]
            start = vm.offset[b : b + 1, lanes]
            closing = inclusive[TILE - 1 : TILE, :]
            middle = inclusive[TILE // 2 - 1 : TILE // 2, :]
            queries = vm.query[at, lanes].astype(f32) * DK ** (-0.5)
            keys = vm.key[at, lanes].astype(f32)
            scores = []
            for q_log, k_log in (
                (inclusive - middle, middle - inclusive),
                (middle - before, before - middle),
            ):
                k_stack = stacked((keys * jnp.exp(k_log)).astype(bf16), head_k1)
                scores.append(dot_nt((queries * jnp.exp(q_log)).astype(bf16), k_stack))
            both = jnp.where(t_index >= s_index, scores[0], 0.0) + jnp.where(
                t_index <= s_index, scores[1], 0.0
            )
            v_stack = stacked(vm.value[at, v_lanes], head_v)
            vm.within[at, v_lanes] = dot(both.astype(bf16), v_stack)
            vm.q_block[g, at, :] = jnp.concatenate(
                [queries * jnp.exp(inclusive), queries * jnp.exp(closing - before)], axis=1
            ).astype(bf16)
            vm.q_whole[g, at, :] = jnp.concatenate(
                [queries * jnp.exp(start + inclusive), queries * jnp.exp((whole - start) - before)], axis=1
            ).astype(bf16)

    def between(g):
        lanes = slice(g * LANES, (g + 1) * LANES)
        v_lanes = slice(g * GV, (g + 1) * GV)
        decays = [jnp.exp(vm.closing[b : b + 1, lanes]) for b in range(blocks)]
        left = []
        for b in range(blocks):
            at = slice(b * TILE, (b + 1) * TILE)
            keys = vm.key[at, lanes].astype(f32)
            both = jnp.concatenate(
                [
                    keys * jnp.exp(vm.closing[b : b + 1, lanes] - vm.inclusive[at, lanes]),
                    keys * jnp.exp(vm.before[at, lanes]),
                ],
                axis=1,
            ).astype(bf16)
            left.append(per_head(dot_tn(vm.value[at, v_lanes], both), head_k))
        forward = [jnp.zeros((DV, LANES), f32)]
        backward = [jnp.zeros((DV, LANES), f32)]
        for b in range(blocks - 1):
            forward.append(decays[b] * forward[b] + left[b][:, :LANES])
            back = blocks - 1 - b
            backward.insert(0, decays[back] * backward[0] + left[back][:, LANES:])
        for b in range(blocks):
            at = slice(b * TILE, (b + 1) * TILE)
            states = jnp.concatenate([forward[b], backward[b]], axis=1)
            across = dot_nt(vm.q_block[g, at, :], stacked(states, head_k).astype(bf16))
            vm.within[at, v_lanes] = vm.within[at, v_lanes] + across

    loads["query_weight"].wait()
    project(vm.query_weight, vm.query)
    inside(0)
    inside(1)

    decays = [[jnp.exp(vm.logs[p, g : g + 1, :]) for g in range(GROUPS)] for p in range(CREW)]
    for g in range(GROUPS):
        mates(lambda p: seg_copy(p, p, g).wait_recv())
    ends = []
    for g in range(GROUPS):
        forward = vm.seg_in[g, 0].astype(f32)[:SUB]
        for p in range(1, CREW):
            forward = decays[p][g] * forward + vm.seg_in[g, p].astype(f32)[:SUB]
        backward = vm.seg_in[g, CREW - 1].astype(f32)[SUB:]
        for p in range(CREW - 2, -1, -1):
            backward = decays[p][g] * backward + vm.seg_in[g, p].astype(f32)[SUB:]
        ends.append((forward, backward))
    for side in range(2):
        vm.crew_out[side] = jnp.concatenate([end[side] for end in ends], axis=0).astype(bf16)

    def crew_copy(c, slot, side):
        return remote(
            vm.crew_out.at[side],
            vm.crew_in.at[slot],
            sem.crew_send.at[c],
            sem.crew_recv.at[slot],
            c * CREW + post,
        )

    def crew_start(i):
        c = lax.rem(crew + i, crews)

        @pl.when(c > crew)
        def _():
            crew_copy(c, crew, 0).start()

        @pl.when(c < crew)
        def _():
            crew_copy(c, crew, 1).start()

    others(crew_start, crews)
    for g in range(2, GROUPS):
        inside(g)
    for g in range(GROUPS - 1):
        between(g)

    reduce_here(1, vm.gate_part, vm.gate_parts, vm.gate_total, vm.gate_totals, gate_spread)

    def ctx_arrived(i):
        c = lax.rem(crew + i, crews)
        for copy in ctx_crew_copies(c, c):
            copy.wait_recv()
        crew_log_copy(c, c).wait_recv()

    others(ctx_arrived, crews)
    zero = jnp.zeros((SUB, LANES), f32)
    forward, backward = [zero] * GROUPS, [zero] * GROUPS
    for a in range(crews):
        z = crews - 1 - a
        for g in range(GROUPS):
            forward[g] = (
                jnp.exp(vm.ctx_crews_logs[a, g : g + 1, :]) * forward[g]
                + vm.ctx_crews[a, g].astype(f32)[:SUB]
            )
            backward[g] = (
                jnp.exp(vm.ctx_crews_logs[z, g : g + 1, :]) * backward[g]
                + vm.ctx_crews[z, g].astype(f32)[SUB:]
            )

    def step_states(c, states):
        left = vm.crew_in[c].astype(f32)
        return tuple(
            jnp.exp(vm.crew_logs[c, g : g + 1, :]) * states[g] + left[g * SUB : (g + 1) * SUB]
            for g in range(GROUPS)
        )

    def from_before(c, states):
        crew_copy(c, c, 0).wait_recv()
        return step_states(c, states)

    def from_after(i, states):
        c = crews - 1 - i
        crew_copy(c, c, 1).wait_recv()
        return step_states(c, states)

    forward = lax.fori_loop(0, crew, from_before, tuple(forward))
    backward = lax.fori_loop(0, crews - 1 - crew, from_after, tuple(backward))

    def enter_copy(p, slot, g):
        return remote(
            vm.enter_out.at[g, p],
            vm.enter_in.at[g, slot],
            sem.enter_send.at[g, p],
            sem.enter_recv.at[g, slot],
            crew * CREW + p,
        )

    for g in range(GROUPS):
        state = forward[g]
        entering = []
        for p in range(CREW):
            entering.append(state)
            state = decays[p][g] * state + vm.seg_in[g, p].astype(f32)[:SUB]
        state = backward[g]
        for p in range(CREW - 1, -1, -1):
            vm.enter_out[g, p] = jnp.concatenate([entering[p], state], axis=0).astype(bf16)
            state = decays[p][g] * state + vm.seg_in[g, p].astype(f32)[SUB:]
        mates(lambda p: enter_copy(p, post, g).start())
        vm.enter_in[g, post] = vm.enter_out[g, post]

    loads["outgate_weight"].wait()
    for n in range(0, vm.outgate_weight.shape[1], COLS):
        at = slice(n, n + COLS)
        gate = dot(vm.normed[...], vm.outgate_weight[:, at]).astype(bf16).astype(f32)
        vm.silu[:, at] = gate / (1.0 + jnp.exp(-gate))
    between(GROUPS - 1)
    head_mean = jnp.where(iota((GV, GV), 0) // DV == iota((GV, GV), 1) // DV, 1.0 / DV, 0.0).astype(bf16)

    arrivals(gate_spread)
    for r in range(reducers):
        for t in range(tp_count):
            for s in range(share):
                row = vm.gate_totals[r * CREW + t, s]
                for x in range(1, CREW // tp_count):
                    row = row + vm.gate_totals[r * CREW + x * tp_count + t, s]
                at = (t * chunks + r * share + s) * LANES
                vm.mods[4:5, at : at + LANES] = row
    loads["out_weight"].wait()

    for r in range(reducers):

        @pl.when(crew != first_reducer + r)
        def _():
            for copy in to_reducer(r, crew):
                copy.wait_send()

    sent(spread)
    sent(gate_spread)

    def mate_sent(p):
        log_copy(p, post).wait_send()
        for copy in ctx_copies(p, post):
            copy.wait_send()
        for g in range(GROUPS):
            seg_copy(p, post, g).wait_send()

    mates(mate_sent)

    def crew_sent(i):
        c = lax.rem(crew + i, crews)
        for copy in ctx_crew_copies(c, crew):
            copy.wait_send()
        crew_log_copy(c, crew).wait_send()
        crew_copy(c, crew, 0).wait_send()

    others(crew_sent, crews)

    for g in range(GROUPS):
        v_lanes = slice(g * GV, (g + 1) * GV)
        mates(lambda p: enter_copy(p, p, g).wait_recv())
        units = [vm.enter_in[g, j].astype(f32) for j in range(CREW)]
        states = jnp.concatenate(
            [
                jnp.concatenate([u[:SUB] for u in units], axis=0),
                jnp.concatenate([u[SUB:] for u in units], axis=0),
            ],
            axis=1,
        )
        across = dot_nt(vm.q_whole[g], stacked(states, head_k).astype(bf16))
        mixed = vm.within[:, v_lanes] + across
        mean = dot((mixed * mixed).astype(bf16), head_mean)
        vm.gated[:, v_lanes] = (mixed * lax.rsqrt(mean + epsilon) * vm.silu[:, v_lanes]).astype(bf16)

    square = jnp.zeros((rows, LANES), f32)
    for n in range(0, width, COLS):
        at = slice(n, n + COLS)
        branch = dot(vm.gated[...], vm.out_weight[:, at]).astype(bf16)
        vm.branch[:, at] = branch
        branch = branch.astype(f32)
        branch = branch * branch
        for s in range(0, COLS, LANES):
            square = square + branch[:, s : s + LANES]
    factor = lax.rsqrt(jnp.sum(square, axis=1, keepdims=True) / width + epsilon)
    gain = vm.mods[4:5, :] * vm.post_gain[...]
    for i in range(rows // STRIP):
        at = slice(i * STRIP, (i + 1) * STRIP)
        hbm.out[at, :] = (
            vm.latent[at, :].astype(f32) + gain * (vm.branch[at, :].astype(f32) * factor[at])
        ).astype(bf16)

    for g in range(GROUPS):
        mates(lambda p: enter_copy(p, post, g).wait_send())


def shards(*operands):
    values = dict(zip(NAMES, operands))
    values["down_weight"] = values["down_weight"].T
    latent, context = values["latent"], values["context"]
    sp_count, tp_count = lax.axis_size("sp"), lax.axis_size("tp")
    count = sp_count * tp_count
    crews = count // CREW
    rows, width = latent.shape
    args, specs = [], []
    for name, value in values.items():
        vector = value.ndim == 1
        args.append(value.reshape(1, -1) if vector and value.dtype == f32 else value)
        specs.append(pl.BlockSpec(memory_space=pltpu.HBM))
    ctx_rows = context.shape[0] * GROUPS // tp_count
    chunks = values["shift_weight"].shape[1] // LANES
    reducers, share = reduction(chunks, crews)
    part_rows = -(-4 * share // SUB) * SUB
    keyw, valw = values["key_weight"].shape[1], values["value_weight"].shape[1]
    blocks = rows // TILE
    unit = (2 * SUB, LANES)
    buffers = dict(
        context=pltpu.VMEM((ctx_rows, width), bf16),
        cond=pltpu.VMEM((SUB, width), f32),
        part=pltpu.VMEM((reducers, part_rows, LANES), f32),
        parts=pltpu.VMEM((crews, part_rows, LANES), f32),
        total=pltpu.VMEM((part_rows, LANES), f32),
        totals=pltpu.VMEM((reducers * CREW, part_rows, LANES), f32),
        gate_part=pltpu.VMEM((reducers, share, 1, LANES), f32),
        gate_parts=pltpu.VMEM((crews, share, 1, LANES), f32),
        gate_total=pltpu.VMEM((share, 1, LANES), f32),
        gate_totals=pltpu.VMEM((reducers * CREW, share, 1, LANES), f32),
        mods=pltpu.VMEM((SUB, width), f32),
        scaled=pltpu.VMEM((rows, width), f32),
        ctx_scaled=pltpu.VMEM((ctx_rows, width), f32),
        normed=pltpu.VMEM((rows, width), bf16),
        ctx_out=pltpu.VMEM((CREW, *unit), bf16),
        ctx_in=pltpu.VMEM((CREW, *unit), bf16),
        ctx_log=pltpu.VMEM((1, LANES), f32),
        ctx_logs=pltpu.VMEM((CREW, 1, LANES), f32),
        ctx_crews_out=pltpu.VMEM((GROUPS, *unit), bf16),
        ctx_crews=pltpu.VMEM((crews, GROUPS, *unit), bf16),
        ctx_crews_log=pltpu.VMEM((SUB, LANES), f32),
        ctx_crews_logs=pltpu.VMEM((crews, SUB, LANES), f32),
        key=pltpu.VMEM((rows, keyw), bf16),
        query=pltpu.VMEM((rows, keyw), bf16),
        value=pltpu.VMEM((rows, valw), bf16),
        silu=pltpu.VMEM((rows, valw), f32),
        gated=pltpu.VMEM((rows, valw), bf16),
        inclusive=pltpu.VMEM((rows, keyw), f32),
        before=pltpu.VMEM((rows, keyw), f32),
        closing=pltpu.VMEM((blocks, keyw), f32),
        offset=pltpu.VMEM((blocks + 1, keyw), f32),
        log_out=pltpu.VMEM((SUB, LANES), f32),
        logs=pltpu.VMEM((CREW, SUB, LANES), f32),
        seg_out=pltpu.VMEM((GROUPS, CREW, *unit), bf16),
        seg_in=pltpu.VMEM((GROUPS, CREW, *unit), bf16),
        crew_out=pltpu.VMEM((2, GROUPS * SUB, LANES), bf16),
        crew_in=pltpu.VMEM((crews, GROUPS * SUB, LANES), bf16),
        crew_log=pltpu.VMEM((SUB, LANES), f32),
        crew_logs=pltpu.VMEM((crews, SUB, LANES), f32),
        enter_out=pltpu.VMEM((GROUPS, CREW, *unit), bf16),
        enter_in=pltpu.VMEM((GROUPS, CREW, *unit), bf16),
        q_block=pltpu.VMEM((GROUPS, rows, 2 * LANES), bf16),
        q_whole=pltpu.VMEM((GROUPS, rows, 2 * LANES), bf16),
        within=pltpu.VMEM((rows, valw), f32),
        branch=pltpu.VMEM((rows, width), bf16),
    )
    for name, value in zip(NAMES, args):
        if name not in buffers:
            buffers[name] = pltpu.VMEM(value.shape, value.dtype)
    dma = pltpu.SemaphoreType.DMA
    semaphores = dict(
        load=dma((len(NAMES),)),
        part_send=dma((reducers,)),
        part_recv=dma((crews,)),
        total_send=dma((count,)),
        total_recv=dma((reducers * CREW,)),
        gate_part_send=dma((reducers,)),
        gate_part_recv=dma((crews,)),
        gate_send=dma((count,)),
        gate_recv=dma((reducers * CREW,)),
        ctx_send=dma((CREW,)),
        ctx_recv=dma((CREW,)),
        ctx_log_send=dma((CREW,)),
        ctx_log_recv=dma((CREW,)),
        ctx_crew_send=dma((crews,)),
        ctx_crew_recv=dma((crews,)),
        ctx_crew_log_send=dma((crews,)),
        ctx_crew_log_recv=dma((crews,)),
        log_send=dma((CREW,)),
        log_recv=dma((CREW,)),
        seg_send=dma((GROUPS, CREW)),
        seg_recv=dma((GROUPS, CREW)),
        crew_send=dma((crews,)),
        crew_recv=dma((crews,)),
        crew_log_send=dma((crews,)),
        crew_log_recv=dma((crews,)),
        enter_send=dma((GROUPS, CREW)),
        enter_recv=dma((GROUPS, CREW)),
    )
    return pl.pallas_call(
        functools.partial(block_kernel, sp_count, tp_count),
        out_shape=pltpu.VMEM((rows, width), bf16),
        in_specs=specs,
        out_specs=pl.BlockSpec(memory_space=pltpu.VMEM),
        scratch_shapes=[buffers, semaphores],
        compiler_params=pltpu.CompilerParams(
            collective_id=0, has_side_effects=True, vmem_limit_bytes=VMEM_LIMIT
        ),
        name="block",
    )(*args)


def solution(mesh):
    placed = (
        P(("sp", "tp"), None),
        P("sp", None),
        P(),
        P(),
        P("sp", "tp"),
        P("sp", "tp"),
        P("sp", "tp"),
        P(),
        P(),
        P(),
        P(),
        P(),
        P(),
        P(),
        P(),
        P(),
        P(),
    )
    return jax.shard_map(
        shards, mesh=mesh, in_specs=placed, out_specs=P(("sp", "tp"), None), check_vma=False
    )
```

```python
import functools
from types import SimpleNamespace

import jax
import jax.numpy as jnp
from jax import lax
from jax.experimental import pallas as pl
from jax.experimental.pallas import tpu as pltpu
from jax.sharding import PartitionSpec as P

HEADS = 16
DK = 32
DV = 64
LANES = 128
SUB = 8
GROUP = LANES // DK
GV = GROUP * DV
GROUPS = HEADS // GROUP
CREW = DV // SUB
CORES = 2
OWNERS = CREW // CORES
UNIT = DV // OWNERS
MESH = pl.DeviceIdType.MESH
TILE = 64
COLS = 256
STRIP = 16
VMEM_LIMIT = 60 * 1024 * 1024

NAMES = (
    "latent",
    "context",
    "latent_condition",
    "context_condition",
    "shift_weight",
    "scale_weight",
    "gate_weight",
    "norm_gain",
    "query_weight",
    "key_weight",
    "value_weight",
    "outgate_weight",
    "down_weight",
    "up_weight",
    "decay_bias",
    "out_weight",
    "post_gain",
)
FIRST = (
    "latent_condition",
    "context_condition",
    "shift_weight",
    "scale_weight",
    "gate_weight",
    "context",
    "latent",
)
LATER = (
    "norm_gain",
    "decay_bias",
    "post_gain",
    "down_weight",
    "up_weight",
    "key_weight",
    "value_weight",
    "query_weight",
    "outgate_weight",
    "out_weight",
)

epsilon = 1e-06
decay_temper = 16.0
f32 = jnp.float32
bf16 = jnp.bfloat16


def dot(a, b):
    return jnp.dot(a, b, preferred_element_type=f32)


def dot_nt(a, b):
    return lax.dot_general(a, b, (((1,), (1,)), ((), ())), preferred_element_type=f32)


def dot_tn(a, b):
    return lax.dot_general(a, b, (((0,), (0,)), ((), ())), preferred_element_type=f32)


def iota(shape, axis):
    return lax.broadcasted_iota(jnp.int32, shape, axis)


def lower_ones(rows):
    return jnp.where(iota((rows, rows), 0) >= iota((rows, rows), 1), 1.0, 0.0).astype(bf16)


def running_sum(lower, log_rows):
    high = log_rows.astype(bf16)
    rest = log_rows - high.astype(f32)
    return dot(lower, high) + dot(lower, rest.astype(bf16))


def log_decays(values):
    return (jnp.minimum(values, 0.0) - jnp.log1p(jnp.exp(-jnp.abs(values)))) / decay_temper


def rms_factor(values):
    return lax.rsqrt(jnp.mean(values * values, axis=-1, keepdims=True) + epsilon)


def per_head(full, head):
    out = full[(GROUP - 1) * DV :]
    for h in range(GROUP - 2, -1, -1):
        out = jnp.where(head == h, full[h * DV : (h + 1) * DV], out)
    return out


def stacked(values, head):
    zero = jnp.zeros_like(values)
    return jnp.concatenate([jnp.where(head == h, values, zero) for h in range(GROUP)], axis=0)


def reduction(chunks, crews):
    reducers = min(2, chunks, crews)
    return reducers, chunks // reducers


def block_kernel(sp_count, tp_count, *refs):
    hbm = SimpleNamespace(**dict(zip((*NAMES, "out"), refs)))
    vm = SimpleNamespace(**refs[-2])
    sem = SimpleNamespace(**refs[-1])

    count = sp_count * tp_count
    crews = count // CREW
    sp, tp = lax.axis_index("sp"), lax.axis_index("tp")
    me = sp * tp_count + tp
    crew, post = me // CREW, lax.rem(me, CREW)
    chip, core = post // CORES, lax.rem(post, CORES)
    rows, width = hbm.latent.shape
    blocks = rows // TILE
    row_share = hbm.shift_weight.shape[0]
    chunks = hbm.shift_weight.shape[1] // LANES
    reducers, share = reduction(chunks, crews)
    first_reducer = (crews - reducers) // 2
    owner = core == CORES - 1
    middle_crew = (crew >= first_reducer) & (crew < first_reducer + reducers)
    reducer = owner & middle_crew
    ctx_rows = vm.context.shape[0]
    ctx_group = lax.rem(tp, GROUPS)

    def place(flat):
        return (flat // tp_count, lax.rem(flat, tp_count))

    def remote(src, dst, send, recv, flat):
        return pltpu.make_async_remote_copy(
            src_ref=src,
            dst_ref=dst,
            send_sem=send,
            recv_sem=recv,
            device_id=place(flat),
            device_id_type=MESH,
        )

    def others(body, total):
        def step(i, carry):
            body(i)
            return carry

        lax.fori_loop(1, total, step, 0)

    def mate(i):
        return lax.rem(post + i, CREW)

    def mates(body):
        for i in range(1, CREW):
            body(mate(i))

    def owners(body):
        for i in range(OWNERS):
            at = lax.rem(chip + i, OWNERS)
            if i == 0:
                pl.when(jnp.logical_not(owner))(functools.partial(body, at))
            else:
                body(at)

    def owner_of(at):
        return at * CORES + CORES - 1

    ctx_at = pl.multiple_of((tp // GROUPS) * ctx_rows, SUB)
    hbm.context = hbm.context.at[pl.ds(ctx_at, ctx_rows)]
    loads = {
        name: pltpu.make_async_copy(getattr(hbm, name), getattr(vm, name), sem.load.at[i])
        for i, name in enumerate(FIRST + LATER)
    }
    for name in FIRST:
        loads[name].start()

    barrier = pltpu.get_barrier_semaphore()

    def greet(flat):
        pl.semaphore_signal(barrier, inc=1, device_id=place(flat), device_id_type=MESH)

    for r in range(reducers):
        for q in range(OWNERS):
            flat = (first_reducer + r) * CREW + owner_of(q)

            @pl.when(flat != me)
            def _():
                greet(flat)

    @pl.when(reducer)
    def _():
        for c in range(crews):
            for k in range(CORES):
                if k < CORES - 1 or not first_reducer <= c < first_reducer + reducers:
                    greet(c * CREW + chip * CORES + k)

    loads["latent_condition"].wait()
    loads["context_condition"].wait()
    vm.cond[0:1, :] = vm.latent_condition[...].astype(f32).reshape(1, width)
    vm.cond[1:2, :] = vm.context_condition[...].astype(f32).reshape(1, width)
    mine = pl.ds(pl.multiple_of(sp * row_share, LANES), row_share)
    pick = iota((STRIP, row_share), 0) == 0
    raw = jnp.where(pick, vm.cond[0:1, mine], vm.cond[1:2, mine])
    cond = (raw / (1.0 + jnp.exp(-raw))).astype(bf16)
    for name in LATER:
        loads[name].start()
    for which, name in enumerate(("shift_weight", "scale_weight", "gate_weight")):
        loads[name].wait()
        part = dot(cond, getattr(vm, name)[...])
        for c in range(chunks):
            at = slice(c * LANES, (c + 1) * LANES)
            r, row = c // share, c % share
            if which == 2:
                vm.gate_part[r, row] = part[0:1, at]
            else:
                vm.part[r, row * 4 + which : row * 4 + which + 1, :] = part[0:1, at]
                vm.part[r, row * 4 + 2 + which : row * 4 + 3 + which, :] = part[1:2, at]
    @pl.when(reducer)
    def _():
        pl.semaphore_wait(barrier, count - 1)

    @pl.when(jnp.logical_not(reducer))
    def _():
        pl.semaphore_wait(barrier, reducers)

    def to_reducer(r, c, k, which):
        part, parts = ((vm.part, vm.parts), (vm.gate_part, vm.gate_parts))[which]
        return remote(
            part.at[r],
            parts.at[c, k],
            sem.part_send.at[which, r],
            sem.part_recv.at[which, c, k],
            (first_reducer + r) * CREW + owner_of(chip),
        )

    def elsewhere(r):
        return jnp.logical_not(owner & (crew == first_reducer + r))

    for which in range(2):
        for r in range(reducers):

            @pl.when(elsewhere(r))
            def _():
                to_reducer(r, crew, core, which).start()

    loads["context"].wait()
    xc = vm.context[...].astype(f32)
    vm.ctx_scaled[...] = xc * rms_factor(xc)
    loads["latent"].wait()

    def scale_strip(i, carry):
        at = pl.ds(pl.multiple_of(i * TILE, TILE), TILE)
        x = vm.latent[at, :].astype(f32)
        vm.scaled[at, :] = x * rms_factor(x)
        return carry

    lax.fori_loop(0, rows // TILE, scale_strip, 0)

    reduced = reducers * OWNERS

    def spread(flat, slot):
        return remote(
            vm.total, vm.totals.at[slot], sem.total_send.at[flat], sem.total_recv.at[slot], flat
        )

    def gate_spread(flat, slot):
        return remote(
            vm.gate_total,
            vm.gate_totals.at[slot],
            sem.gate_send.at[flat],
            sem.gate_recv.at[slot],
            flat,
        )

    def reduce_here(which, mine, held, total, totals, copy):
        for r in range(reducers):
            home = first_reducer + r

            @pl.when(owner & (crew == home))
            def _():
                slot = r * OWNERS + chip
                for k in range(CORES):
                    out = None
                    for c in range(crews):
                        if c == home and k == CORES - 1:
                            term = mine[r]
                        else:
                            to_reducer(r, c, k, which).wait_recv()
                            term = held[c, k]
                        out = term if out is None else out + term
                    total[k] = out
                    totals[slot, k] = out
                for c in sorted(range(crews), key=lambda c: -abs(c - home)):

                    def send(i, carry):
                        flat = c * CREW + mate(i)
                        copy(flat, slot).start()
                        return carry

                    lax.fori_loop(0 if c != home else 1, CREW, send, 0)

    def arrivals(copy):
        def arrived(i, carry):
            @pl.when((first_reducer + i // OWNERS) * CREW + owner_of(lax.rem(i, OWNERS)) != me)
            def _():
                copy(me, i).wait_recv()

            return carry

        lax.fori_loop(0, reduced, arrived, 0)

    def sent(copy):
        @pl.when(reducer)
        def _():
            others(lambda i: copy(lax.rem(me + i, count), 0).wait_send(), count)

    reduce_here(0, vm.part, vm.parts, vm.total, vm.totals, spread)
    loads_needed = ("norm_gain", "decay_bias", "post_gain", "down_weight", "up_weight", "key_weight")
    for name in loads_needed + ("value_weight",):
        loads[name].wait()
    arrivals(spread)
    def summed(totals, r, t):
        out = None
        for p in range(t, CREW, tp_count):
            term = totals[r * OWNERS + p // CORES, p % CORES]
            out = term if out is None else out + term
        return out

    for r in range(reducers):
        for t in range(tp_count):
            tile = summed(vm.totals, r, t)
            for s in range(share):
                at = (t * chunks + r * share + s) * LANES
                vm.mods[0:4, at : at + LANES] = tile[s * 4 : s * 4 + 4]

    gain = vm.norm_gain[...] * (1.0 + vm.mods[3:4, :])
    ctx_normed = (vm.ctx_scaled[...] * gain + vm.mods[2:3, :]).astype(bf16)
    head_k = iota((DV, 2 * LANES), 1) % LANES // DK
    key_at = pl.ds(pl.multiple_of(ctx_group * LANES, LANES), LANES)
    val_at = pl.ds(pl.multiple_of(ctx_group * GV, GV), GV)
    low = dot_nt(ctx_normed, vm.down_weight[...]).astype(bf16)
    log_rows = log_decays(dot(low, vm.up_weight[:, key_at]) + vm.decay_bias[:, key_at])
    keys = dot(ctx_normed, vm.key_weight[:, key_at]).astype(bf16).astype(f32)
    values = dot(ctx_normed, vm.value_weight[:, val_at]).astype(bf16)
    inclusive = running_sum(lower_ones(ctx_rows), log_rows)
    closing = inclusive[ctx_rows - 1 : ctx_rows, :]
    both = jnp.concatenate(
        [keys * jnp.exp(closing - inclusive), keys * jnp.exp(inclusive - log_rows)], axis=1
    ).astype(bf16)
    state = per_head(dot_tn(values, both), head_k)
    for j in range(OWNERS):
        at = slice(j * UNIT, (j + 1) * UNIT)
        vm.ctx_out[j] = jnp.concatenate([state[at, :LANES], state[at, LANES:]], axis=0).astype(bf16)
    vm.ctx_log[...] = closing

    gain = vm.norm_gain[...] * (1.0 + vm.mods[1:2, :])
    shift = vm.mods[0:1, :]
    for i in range(rows // STRIP):
        at = slice(i * STRIP, (i + 1) * STRIP)
        vm.normed[at, :] = (vm.scaled[at, :] * gain + shift).astype(bf16)

    def project(weight, out):
        for n in range(0, weight.shape[1], COLS):
            at = slice(n, n + COLS)
            out[:, at] = dot(vm.normed[...], weight[:, at]).astype(bf16)

    low = dot_nt(vm.normed[...], vm.down_weight[...]).astype(bf16)
    log_all = log_decays(dot(low, vm.up_weight[...]) + vm.decay_bias[...])
    lower = lower_ones(TILE)
    offset = None
    for b in range(blocks):
        at = slice(b * TILE, (b + 1) * TILE)
        log_rows = log_all[at]
        inclusive = running_sum(lower, log_rows)
        end = inclusive[TILE - 1 : TILE, :]
        vm.inclusive[at, :] = inclusive
        vm.before[at, :] = inclusive - log_rows
        vm.closing[b : b + 1, :] = end
        vm.offset[b : b + 1, :] = jnp.zeros_like(end) if offset is None else offset
        offset = end if offset is None else offset + end
    vm.offset[blocks : blocks + 1, :] = offset
    for g in range(GROUPS):
        vm.log_out[g : g + 1, :] = offset[:, g * LANES : (g + 1) * LANES]
    project(vm.key_weight, vm.key)
    project(vm.value_weight, vm.value)

    def log_copy(o, p):
        return remote(
            vm.log_out, vm.logs.at[p], sem.log_send.at[o], sem.log_recv.at[p], crew * CREW + owner_of(o)
        )

    def ctx_copies(o, p):
        flat = crew * CREW + owner_of(o)
        return (
            remote(vm.ctx_out.at[o], vm.ctx_in.at[p], sem.ctx_send.at[o], sem.ctx_recv.at[p], flat),
            remote(vm.ctx_log, vm.ctx_logs.at[p], sem.ctx_log_send.at[o], sem.ctx_log_recv.at[p], flat),
        )

    def early_copies(o, p):
        return (*ctx_copies(o, p), log_copy(o, p))

    def early_start(o):
        for copy in early_copies(o, post):
            copy.start()

    owners(early_start)

    @pl.when(owner)
    def _():
        vm.ctx_in[post] = vm.ctx_out[chip]
        vm.ctx_logs[post] = vm.ctx_log[...]
        vm.logs[post] = vm.log_out[...]

    def seg_copy(o, p, g):
        return remote(
            vm.seg_out.at[g, o],
            vm.seg_in.at[g, p],
            sem.seg_send.at[g, o],
            sem.seg_recv.at[g, p],
            crew * CREW + owner_of(o),
        )

    for g in range(GROUPS):
        lanes = slice(g * LANES, (g + 1) * LANES)
        v_lanes = slice(g * GV, (g + 1) * GV)
        whole = vm.offset[blocks : blocks + 1, lanes]
        both = []
        for b in range(blocks):
            at = slice(b * TILE, (b + 1) * TILE)
            keys = vm.key[at, lanes].astype(f32)
            start = vm.offset[b : b + 1, lanes]
            after = (whole - start) - vm.inclusive[at, lanes]
            both.append(
                jnp.concatenate(
                    [keys * jnp.exp(after), keys * jnp.exp(start + vm.before[at, lanes])], axis=1
                ).astype(bf16)
            )
        state = per_head(dot_tn(vm.value[:, v_lanes], jnp.concatenate(both, axis=0)), head_k)
        for j in range(OWNERS):
            at = slice(j * UNIT, (j + 1) * UNIT)
            vm.seg_out[g, j] = jnp.concatenate([state[at, :LANES], state[at, LANES:]], axis=0).astype(bf16)
        owners(lambda o: seg_copy(o, post, g).start())

    @pl.when(owner)
    def _():
        for g in range(GROUPS):
            vm.seg_in[g, post] = vm.seg_out[g, chip]

    reduce_here(1, vm.gate_part, vm.gate_parts, vm.gate_total, vm.gate_totals, gate_spread)


    head_k1 = iota((TILE, LANES), 1) // DK
    head_v = iota((TILE, GV), 1) // DV
    t_index = iota((TILE, GROUP * TILE), 0)
    s_index = iota((TILE, GROUP * TILE), 1) % TILE

    def inside(g):
        lanes = slice(g * LANES, (g + 1) * LANES)
        v_lanes = slice(g * GV, (g + 1) * GV)
        whole = vm.offset[blocks : blocks + 1, lanes]
        for b in range(blocks):
            at = slice(b * TILE, (b + 1) * TILE)
            inclusive, before = vm.inclusive[at, lanes], vm.before[at, lanes]
            start = vm.offset[b : b + 1, lanes]
            closing = inclusive[TILE - 1 : TILE, :]
            middle = inclusive[TILE // 2 - 1 : TILE // 2, :]
            queries = vm.query[at, lanes].astype(f32) * DK ** (-0.5)
            keys = vm.key[at, lanes].astype(f32)
            scores = []
            for q_log, k_log in (
                (inclusive - middle, middle - inclusive),
                (middle - before, before - middle),
            ):
                k_stack = stacked((keys * jnp.exp(k_log)).astype(bf16), head_k1)
                scores.append(dot_nt((queries * jnp.exp(q_log)).astype(bf16), k_stack))
            both = jnp.where(t_index >= s_index, scores[0], 0.0) + jnp.where(
                t_index <= s_index, scores[1], 0.0
            )
            v_stack = stacked(vm.value[at, v_lanes], head_v)
            vm.within[at, v_lanes] = dot(both.astype(bf16), v_stack)
            vm.q_block[g, at, :] = jnp.concatenate(
                [queries * jnp.exp(inclusive), queries * jnp.exp(closing - before)], axis=1
            ).astype(bf16)
            vm.q_whole[g, at, :] = jnp.concatenate(
                [queries * jnp.exp(start + inclusive), queries * jnp.exp((whole - start) - before)], axis=1
            ).astype(bf16)

    def between(g):
        lanes = slice(g * LANES, (g + 1) * LANES)
        v_lanes = slice(g * GV, (g + 1) * GV)
        decays = [jnp.exp(vm.closing[b : b + 1, lanes]) for b in range(blocks)]
        left = []
        for b in range(blocks):
            at = slice(b * TILE, (b + 1) * TILE)
            keys = vm.key[at, lanes].astype(f32)
            both = jnp.concatenate(
                [
                    keys * jnp.exp(vm.closing[b : b + 1, lanes] - vm.inclusive[at, lanes]),
                    keys * jnp.exp(vm.before[at, lanes]),
                ],
                axis=1,
            ).astype(bf16)
            left.append(per_head(dot_tn(vm.value[at, v_lanes], both), head_k))
        forward = [jnp.zeros((DV, LANES), f32)]
        backward = [jnp.zeros((DV, LANES), f32)]
        for b in range(blocks - 1):
            forward.append(decays[b] * forward[b] + left[b][:, :LANES])
            back = blocks - 1 - b
            backward.insert(0, decays[back] * backward[0] + left[back][:, LANES:])
        for b in range(blocks):
            at = slice(b * TILE, (b + 1) * TILE)
            states = jnp.concatenate([forward[b], backward[b]], axis=1)
            across = dot_nt(vm.q_block[g, at, :], stacked(states, head_k).astype(bf16))
            vm.within[at, v_lanes] = vm.within[at, v_lanes] + across

    loads["query_weight"].wait()
    project(vm.query_weight, vm.query)
    inside(0)

    def ctx_crew_copies(c, slot):
        flat = c * CREW + post
        return (
            remote(
                vm.ctx_crews_out,
                vm.ctx_crews.at[slot],
                sem.ctx_crew_send.at[c],
                sem.ctx_crew_recv.at[slot],
                flat,
            ),
            remote(
                vm.crew_log, vm.crew_logs.at[slot], sem.crew_log_send.at[c], sem.crew_log_recv.at[slot], flat
            ),
        )

    @pl.when(owner)
    def _():
        def early_in(p):
            for copy in early_copies(0, p):
                copy.wait_recv()

        mates(early_in)
        crew_log = vm.logs[0]
        for p in range(1, CREW):
            crew_log = crew_log + vm.logs[p]
        vm.crew_log[0] = crew_log
        for g in range(GROUPS):
            posts = list(range(g, CREW, GROUPS))
            logs = [vm.ctx_logs[p] for p in posts]
            tiles = [vm.ctx_in[p].astype(f32) for p in posts]
            forward, backward, log_sum = tiles[0][:UNIT], tiles[-1][UNIT:], logs[0]
            for i in range(1, len(posts)):
                forward = jnp.exp(logs[i]) * forward + tiles[i][:UNIT]
                backward = jnp.exp(logs[-1 - i]) * backward + tiles[-1 - i][UNIT:]
                log_sum = log_sum + logs[i]
            vm.ctx_crews_out[g] = jnp.concatenate([forward, backward], axis=0).astype(bf16)
            vm.crew_log[1, g : g + 1, :] = log_sum

        def ctx_crew_start(i):
            for copy in ctx_crew_copies(lax.rem(crew + i, crews), crew):
                copy.start()

        others(ctx_crew_start, crews)
        vm.ctx_crews[crew] = vm.ctx_crews_out[...]
        vm.crew_logs[crew] = vm.crew_log[...]

    inside(1)

    def crew_copy(c, slot, side):
        return remote(
            vm.crew_out.at[side],
            vm.crew_in.at[slot],
            sem.crew_send.at[c],
            sem.crew_recv.at[slot],
            c * CREW + post,
        )

    def post_decay(p, g):
        return jnp.exp(vm.logs[p, g : g + 1, :])

    @pl.when(owner)
    def _():
        for g in range(GROUPS):
            mates(lambda p: seg_copy(0, p, g).wait_recv())
        at = slice(0, UNIT)
        for g in range(GROUPS):
            at = slice(g * UNIT, (g + 1) * UNIT)
            forward = vm.seg_in[g, 0, :UNIT].astype(f32)
            for p in range(1, CREW):
                forward = post_decay(p, g) * forward + vm.seg_in[g, p, :UNIT].astype(f32)
            backward = vm.seg_in[g, CREW - 1, UNIT:].astype(f32)
            for p in range(CREW - 2, -1, -1):
                backward = post_decay(p, g) * backward + vm.seg_in[g, p, UNIT:].astype(f32)
            vm.crew_out[0, at, :] = forward.astype(bf16)
            vm.crew_out[1, at, :] = backward.astype(bf16)

        def crew_start(i):
            c = lax.rem(crew + i, crews)

            @pl.when(c > crew)
            def _():
                crew_copy(c, crew, 0).start()

            @pl.when(c < crew)
            def _():
                crew_copy(c, crew, 1).start()

        others(crew_start, crews)

    for g in range(2, GROUPS):
        inside(g)
    for g in range(GROUPS - 2):
        between(g)

    def enter_copy(p, o, g):
        return remote(
            vm.enter_out.at[g, p],
            vm.enter_in.at[g, o],
            sem.enter_send.at[g, p],
            sem.enter_recv.at[g, o],
            crew * CREW + p,
        )

    @pl.when(owner)
    def _():
        def ctx_arrived(i):
            c = lax.rem(crew + i, crews)
            for copy in ctx_crew_copies(c, c):
                copy.wait_recv()

        others(ctx_arrived, crews)
        zero = jnp.zeros((UNIT, LANES), f32)
        forward, backward = [zero] * GROUPS, [zero] * GROUPS
        for a in range(crews):
            z = crews - 1 - a
            for g in range(GROUPS):
                forward[g] = (
                    jnp.exp(vm.crew_logs[a, 1, g : g + 1, :]) * forward[g]
                    + vm.ctx_crews[a, g, :UNIT].astype(f32)
                )
                backward[g] = (
                    jnp.exp(vm.crew_logs[z, 1, g : g + 1, :]) * backward[g]
                    + vm.ctx_crews[z, g, UNIT:].astype(f32)
                )

        def step_states(c, states):
            left = vm.crew_in[c].astype(f32)
            return tuple(
                jnp.exp(vm.crew_logs[c, 0, g : g + 1, :]) * states[g] + left[g * UNIT : (g + 1) * UNIT]
                for g in range(GROUPS)
            )

        def from_before(c, states):
            crew_copy(c, c, 0).wait_recv()
            return step_states(c, states)

        def from_after(i, states):
            c = crews - 1 - i
            crew_copy(c, c, 1).wait_recv()
            return step_states(c, states)

        forward = lax.fori_loop(0, crew, from_before, tuple(forward))
        backward = lax.fori_loop(0, crews - 1 - crew, from_after, tuple(backward))
        for g in range(GROUPS):
            state = forward[g]
            for p in range(CREW):
                vm.enter_out[g, p, :UNIT] = state.astype(bf16)
                if p < CREW - 1:
                    state = post_decay(p, g) * state + vm.seg_in[g, p, :UNIT].astype(f32)
            state = backward[g]
            for p in range(CREW - 1, -1, -1):
                vm.enter_out[g, p, UNIT:] = state.astype(bf16)
                if p > 0:
                    state = post_decay(p, g) * state + vm.seg_in[g, p, UNIT:].astype(f32)
            mates(lambda p: enter_copy(p, chip, g).start())
        for g in range(GROUPS):
            vm.enter_in[g, chip] = vm.enter_out[g, post]

    loads["outgate_weight"].wait()
    for n in range(0, vm.outgate_weight.shape[1], COLS):
        at = slice(n, n + COLS)
        gate = dot(vm.normed[...], vm.outgate_weight[:, at]).astype(bf16).astype(f32)
        vm.silu[:, at] = gate / (1.0 + jnp.exp(-gate))
    for g in range(GROUPS - 2, GROUPS):
        between(g)
    head_mean = jnp.where(iota((GV, GV), 0) // DV == iota((GV, GV), 1) // DV, 1.0 / DV, 0.0).astype(bf16)

    arrivals(gate_spread)
    for r in range(reducers):
        for t in range(tp_count):
            tile = summed(vm.gate_totals, r, t)
            for s in range(share):
                at = (t * chunks + r * share + s) * LANES
                vm.mods[4:5, at : at + LANES] = tile[s]
    loads["out_weight"].wait()

    for which in range(2):
        for r in range(reducers):

            @pl.when(elsewhere(r))
            def _():
                to_reducer(r, crew, core, which).wait_send()

    sent(spread)
    sent(gate_spread)

    def to_owner_sent(o):
        for copy in early_copies(o, post):
            copy.wait_send()
        for g in range(GROUPS):
            seg_copy(o, post, g).wait_send()

    owners(to_owner_sent)

    @pl.when(owner)
    def _():
        def crew_sent(i):
            c = lax.rem(crew + i, crews)
            for copy in ctx_crew_copies(c, crew):
                copy.wait_send()
            crew_copy(c, crew, 0).wait_send()

        others(crew_sent, crews)

    def finish(g):
        v_lanes = slice(g * GV, (g + 1) * GV)
        states = jnp.concatenate(
            [
                jnp.concatenate([vm.enter_in[g, o, :UNIT] for o in range(OWNERS)], axis=0),
                jnp.concatenate([vm.enter_in[g, o, UNIT:] for o in range(OWNERS)], axis=0),
            ],
            axis=1,
        )
        across = dot_nt(vm.q_whole[g], stacked(states, head_k))
        mixed = vm.within[:, v_lanes] + across
        mean = dot((mixed * mixed).astype(bf16), head_mean)
        vm.gated[:, v_lanes] = (mixed * lax.rsqrt(mean + epsilon) * vm.silu[:, v_lanes]).astype(bf16)

    for half in range(0, GROUPS, 2):
        for g in range(half, half + 2):
            owners(lambda o: enter_copy(post, o, g).wait_recv())
        for g in range(half, half + 2):
            finish(g)

    square = jnp.zeros((rows, LANES), f32)
    for n in range(0, width, COLS):
        at = slice(n, n + COLS)
        branch = dot(vm.gated[...], vm.out_weight[:, at]).astype(bf16)
        vm.branch[:, at] = branch
        branch = branch.astype(f32)
        branch = branch * branch
        for s in range(0, COLS, LANES):
            square = square + branch[:, s : s + LANES]
    factor = lax.rsqrt(jnp.sum(square, axis=1, keepdims=True) / width + epsilon)
    gain = vm.mods[4:5, :] * vm.post_gain[...]
    for i in range(rows // STRIP):
        at = slice(i * STRIP, (i + 1) * STRIP)
        hbm.out[at, :] = (
            vm.latent[at, :].astype(f32) + gain * (vm.branch[at, :].astype(f32) * factor[at])
        ).astype(bf16)

    @pl.when(owner)
    def _():
        for g in range(GROUPS):
            mates(lambda p: enter_copy(p, chip, g).wait_send())


def shards(*operands):
    values = dict(zip(NAMES, operands))
    values["down_weight"] = values["down_weight"].T
    latent, context = values["latent"], values["context"]
    sp_count, tp_count = lax.axis_size("sp"), lax.axis_size("tp")
    count = sp_count * tp_count
    crews = count // CREW
    rows, width = latent.shape
    args, specs = [], []
    for name, value in values.items():
        vector = value.ndim == 1
        args.append(value.reshape(1, -1) if vector and value.dtype == f32 else value)
        specs.append(pl.BlockSpec(memory_space=pltpu.HBM))
    ctx_rows = context.shape[0] * GROUPS // tp_count
    chunks = values["shift_weight"].shape[1] // LANES
    reducers, share = reduction(chunks, crews)
    part_rows = -(-4 * share // SUB) * SUB
    keyw, valw = values["key_weight"].shape[1], values["value_weight"].shape[1]
    blocks = rows // TILE
    unit = (2 * UNIT, LANES)
    buffers = dict(
        context=pltpu.VMEM((ctx_rows, width), bf16),
        cond=pltpu.VMEM((SUB, width), f32),
        part=pltpu.VMEM((reducers, part_rows, LANES), f32),
        parts=pltpu.VMEM((crews, CORES, part_rows, LANES), f32),
        total=pltpu.VMEM((CORES, part_rows, LANES), f32),
        totals=pltpu.VMEM((reducers * OWNERS, CORES, part_rows, LANES), f32),
        gate_part=pltpu.VMEM((reducers, share, 1, LANES), f32),
        gate_parts=pltpu.VMEM((crews, CORES, share, 1, LANES), f32),
        gate_total=pltpu.VMEM((CORES, share, 1, LANES), f32),
        gate_totals=pltpu.VMEM((reducers * OWNERS, CORES, share, 1, LANES), f32),
        mods=pltpu.VMEM((SUB, width), f32),
        scaled=pltpu.VMEM((rows, width), f32),
        ctx_scaled=pltpu.VMEM((ctx_rows, width), f32),
        normed=pltpu.VMEM((rows, width), bf16),
        ctx_out=pltpu.VMEM((OWNERS, *unit), bf16),
        ctx_in=pltpu.VMEM((CREW, *unit), bf16),
        ctx_log=pltpu.VMEM((1, LANES), f32),
        ctx_logs=pltpu.VMEM((CREW, 1, LANES), f32),
        ctx_crews_out=pltpu.VMEM((GROUPS, *unit), bf16),
        ctx_crews=pltpu.VMEM((crews, GROUPS, *unit), bf16),
        key=pltpu.VMEM((rows, keyw), bf16),
        query=pltpu.VMEM((rows, keyw), bf16),
        value=pltpu.VMEM((rows, valw), bf16),
        silu=pltpu.VMEM((rows, valw), f32),
        gated=pltpu.VMEM((rows, valw), bf16),
        inclusive=pltpu.VMEM((rows, keyw), f32),
        before=pltpu.VMEM((rows, keyw), f32),
        closing=pltpu.VMEM((blocks, keyw), f32),
        offset=pltpu.VMEM((blocks + 1, keyw), f32),
        log_out=pltpu.VMEM((SUB, LANES), f32),
        logs=pltpu.VMEM((CREW, SUB, LANES), f32),
        seg_out=pltpu.VMEM((GROUPS, OWNERS, *unit), bf16),
        seg_in=pltpu.VMEM((GROUPS, CREW, *unit), bf16),
        crew_out=pltpu.VMEM((2, GROUPS * UNIT, LANES), bf16),
        crew_in=pltpu.VMEM((crews, GROUPS * UNIT, LANES), bf16),
        crew_log=pltpu.VMEM((2, SUB, LANES), f32),
        crew_logs=pltpu.VMEM((crews, 2, SUB, LANES), f32),
        enter_out=pltpu.VMEM((GROUPS, CREW, *unit), bf16),
        enter_in=pltpu.VMEM((GROUPS, OWNERS, *unit), bf16),
        q_block=pltpu.VMEM((GROUPS, rows, 2 * LANES), bf16),
        q_whole=pltpu.VMEM((GROUPS, rows, 2 * LANES), bf16),
        within=pltpu.VMEM((rows, valw), f32),
        branch=pltpu.VMEM((rows, width), bf16),
    )
    for name, value in zip(NAMES, args):
        if name not in buffers:
            buffers[name] = pltpu.VMEM(value.shape, value.dtype)
    dma = pltpu.SemaphoreType.DMA
    semaphores = dict(
        load=dma((len(NAMES),)),
        part_send=dma((2, reducers)),
        part_recv=dma((2, crews, CORES)),
        total_send=dma((count,)),
        total_recv=dma((reducers * OWNERS,)),
        gate_send=dma((count,)),
        gate_recv=dma((reducers * OWNERS,)),
        ctx_send=dma((OWNERS,)),
        ctx_recv=dma((CREW,)),
        ctx_log_send=dma((OWNERS,)),
        ctx_log_recv=dma((CREW,)),
        log_send=dma((OWNERS,)),
        log_recv=dma((CREW,)),
        seg_send=dma((GROUPS, OWNERS)),
        seg_recv=dma((GROUPS, CREW)),
        ctx_crew_send=dma((crews,)),
        ctx_crew_recv=dma((crews,)),
        crew_log_send=dma((crews,)),
        crew_log_recv=dma((crews,)),
        crew_send=dma((crews,)),
        crew_recv=dma((crews,)),
        enter_send=dma((GROUPS, CREW)),
        enter_recv=dma((GROUPS, OWNERS)),
    )
    return pl.pallas_call(
        functools.partial(block_kernel, sp_count, tp_count),
        out_shape=pltpu.VMEM((rows, width), bf16),
        in_specs=specs,
        out_specs=pl.BlockSpec(memory_space=pltpu.VMEM),
        scratch_shapes=[buffers, semaphores],
        compiler_params=pltpu.CompilerParams(
            collective_id=0, has_side_effects=True, vmem_limit_bytes=VMEM_LIMIT
        ),
        name="block",
    )(*args)


def solution(mesh):
    placed = (
        P(("sp", "tp"), None),
        P("sp", None),
        P(),
        P(),
        P("sp", "tp"),
        P("sp", "tp"),
        P("sp", "tp"),
        P(),
        P(),
        P(),
        P(),
        P(),
        P(),
        P(),
        P(),
        P(),
        P(),
    )
    return jax.shard_map(
        shards, mesh=mesh, in_specs=placed, out_specs=P(("sp", "tp"), None), check_vma=False
    )
```

```python
import functools
from types import SimpleNamespace

import jax
import jax.numpy as jnp
from jax import lax
from jax.experimental import pallas as pl
from jax.experimental.pallas import tpu as pltpu
from jax.sharding import PartitionSpec as P

HEADS = 16
DK = 32
DV = 64
LANES = 128
SUB = 8
GROUP = LANES // DK
GV = GROUP * DV
GROUPS = HEADS // GROUP
CREW = DV // SUB
CORES = 2
OWNERS = CREW // CORES
UNIT = DV // OWNERS
MESH = pl.DeviceIdType.MESH
TILE = 64
COLS = 256
STRIP = 16
VMEM_LIMIT = 60 * 1024 * 1024

NAMES = (
    "latent",
    "context",
    "latent_condition",
    "context_condition",
    "shift_weight",
    "scale_weight",
    "gate_weight",
    "norm_gain",
    "query_weight",
    "key_weight",
    "value_weight",
    "outgate_weight",
    "down_weight",
    "up_weight",
    "decay_bias",
    "out_weight",
    "post_gain",
)
FIRST = (
    "latent_condition",
    "context_condition",
    "shift_weight",
    "scale_weight",
    "gate_weight",
)
LATER = (
    "context",
    "latent",
    "down_weight",
    "norm_gain",
    "decay_bias",
    "post_gain",
    "up_weight",
    "key_weight",
    "value_weight",
    "query_weight",
    "outgate_weight",
    "out_weight",
)

epsilon = 1e-06
decay_temper = 16.0
f32 = jnp.float32
bf16 = jnp.bfloat16


def dot(a, b):
    return jnp.dot(a, b, preferred_element_type=f32)


def dot_nt(a, b):
    return lax.dot_general(a, b, (((1,), (1,)), ((), ())), preferred_element_type=f32)


def dot_tn(a, b):
    return lax.dot_general(a, b, (((0,), (0,)), ((), ())), preferred_element_type=f32)


def iota(shape, axis):
    return lax.broadcasted_iota(jnp.int32, shape, axis)


def lower_ones(rows):
    return jnp.where(iota((rows, rows), 0) >= iota((rows, rows), 1), 1.0, 0.0).astype(bf16)


def running_sum(lower, log_rows):
    high = log_rows.astype(bf16)
    rest = log_rows - high.astype(f32)
    return dot(lower, high) + dot(lower, rest.astype(bf16))


def log_decays(values):
    return (jnp.minimum(values, 0.0) - jnp.log(1.0 + jnp.exp(-jnp.abs(values)))) * (1.0 / decay_temper)


def rms_factor(values):
    return lax.rsqrt(jnp.mean(values * values, axis=-1, keepdims=True) + epsilon)


def per_head(full, head):
    out = full[(GROUP - 1) * DV :]
    for h in range(GROUP - 2, -1, -1):
        out = jnp.where(head == h, full[h * DV : (h + 1) * DV], out)
    return out


def stacked(values, head):
    zero = jnp.zeros_like(values)
    return jnp.concatenate([jnp.where(head == h, values, zero) for h in range(GROUP)], axis=0)


def reduction(chunks, crews):
    reducers = min(2, chunks, crews)
    return reducers, chunks // reducers


def block_kernel(sp_count, tp_count, *refs):
    hbm = SimpleNamespace(**dict(zip((*NAMES, "out"), refs)))
    vm = SimpleNamespace(**refs[-2])
    sem = SimpleNamespace(**refs[-1])

    count = sp_count * tp_count
    crews = count // CREW
    sp, tp = lax.axis_index("sp"), lax.axis_index("tp")
    me = sp * tp_count + tp
    crew, post = lax.div(me, CREW), lax.rem(me, CREW)
    chip, core = lax.div(post, CORES), lax.rem(post, CORES)
    rows, width = hbm.latent.shape
    blocks = rows // TILE
    row_share = hbm.shift_weight.shape[0]
    chunks = hbm.shift_weight.shape[1] // LANES
    reducers, share = reduction(chunks, crews)
    first_reducer = (crews - reducers) // 2
    owner = core == CORES - 1
    middle_crew = (crew >= first_reducer) & (crew < first_reducer + reducers)
    reducer = owner & middle_crew
    ctx_rows = vm.context.shape[0]
    ctx_group = lax.rem(tp, GROUPS)

    def place(flat):
        return (lax.div(flat, jnp.int32(tp_count)), lax.rem(flat, jnp.int32(tp_count)))

    def remote(src, dst, send, recv, flat):
        return pltpu.make_async_remote_copy(
            src_ref=src,
            dst_ref=dst,
            send_sem=send,
            recv_sem=recv,
            device_id=place(flat),
            device_id_type=MESH,
        )

    def others(body, total):
        def step(i, carry):
            body(i)
            return carry

        lax.fori_loop(1, total, step, 0)

    def mate(i):
        return lax.rem(post + i, CREW)

    def mates(body):
        for i in range(1, CREW):
            body(mate(i))

    def owners(body):
        for i in range(OWNERS):
            at = lax.rem(chip + i, OWNERS)
            if i == 0:
                pl.when(jnp.logical_not(owner))(functools.partial(body, at))
            else:
                body(at)

    def owner_of(at):
        return at * CORES + CORES - 1

    ctx_at = pl.multiple_of((tp // GROUPS) * ctx_rows, SUB)
    hbm.context = hbm.context.at[pl.ds(ctx_at, ctx_rows)]
    loads = {
        name: pltpu.make_async_copy(getattr(hbm, name), getattr(vm, name), sem.load.at[i])
        for i, name in enumerate(FIRST + LATER)
    }
    for name in FIRST:
        loads[name].start()

    barrier = pltpu.get_barrier_semaphore()

    def greet(flat):
        pl.semaphore_signal(barrier, inc=1, device_id=place(flat), device_id_type=MESH)

    for r in range(reducers):
        for q in range(OWNERS):
            flat = (first_reducer + r) * CREW + owner_of(q)

            @pl.when(flat != me)
            def _():
                greet(flat)

    @pl.when(reducer)
    def _():
        for c in range(crews):
            for k in range(CORES):
                if k < CORES - 1 or not first_reducer <= c < first_reducer + reducers:
                    greet(c * CREW + chip * CORES + k)

    loads["latent_condition"].wait()
    loads["context_condition"].wait()
    vm.cond[0:1, :] = vm.latent_condition[...].astype(f32).reshape(1, width)
    vm.cond[1:2, :] = vm.context_condition[...].astype(f32).reshape(1, width)
    mine = pl.ds(pl.multiple_of(sp * row_share, LANES), row_share)
    pick = iota((STRIP, row_share), 0) == 0
    raw = jnp.where(pick, vm.cond[0:1, mine], vm.cond[1:2, mine])
    cond = (raw / (1.0 + jnp.exp(-raw))).astype(bf16)
    for which, name in enumerate(("shift_weight", "scale_weight", "gate_weight")):
        loads[name].wait()
        part = dot(cond, getattr(vm, name)[...])
        for c in range(chunks):
            at = slice(c * LANES, (c + 1) * LANES)
            r, row = c // share, c % share
            if which == 2:
                vm.gate_part[r, row] = part[0:1, at]
            else:
                vm.part[r, row * 4 + which : row * 4 + which + 1, :] = part[0:1, at]
                vm.part[r, row * 4 + 2 + which : row * 4 + 3 + which, :] = part[1:2, at]
    for name in LATER:
        loads[name].start()
    @pl.when(reducer)
    def _():
        pl.semaphore_wait(barrier, count - 1)

    @pl.when(jnp.logical_not(reducer))
    def _():
        pl.semaphore_wait(barrier, reducers)

    home_core = (CORES - 1, 0)

    def to_reducer(r, c, k, which):
        part, parts = ((vm.part, vm.parts), (vm.gate_part, vm.gate_parts))[which]
        return remote(
            part.at[r],
            parts.at[c, k],
            sem.part_send.at[which, r],
            sem.part_recv.at[which, c, k],
            (first_reducer + r) * CREW + chip * CORES + home_core[which],
        )

    def elsewhere(r, which):
        return jnp.logical_not((core == home_core[which]) & (crew == first_reducer + r))

    def send_parts(which):
        for r in range(reducers):

            @pl.when(elsewhere(r, which))
            def _():
                to_reducer(r, crew, core, which).start()

    send_parts(0)

    loads["context"].wait()
    xc = vm.context[...].astype(f32)
    vm.ctx_scaled[...] = xc * rms_factor(xc)
    loads["latent"].wait()

    def scale_strip(i, carry):
        at = pl.ds(pl.multiple_of(i * TILE, TILE), TILE)
        x = vm.latent[at, :].astype(f32)
        vm.scaled[at, :] = x * rms_factor(x)
        return carry

    lax.fori_loop(0, rows // TILE, scale_strip, 0)
    loads["down_weight"].wait()
    vm.down[...] = vm.down_weight[...].T

    reduced = reducers * OWNERS

    def spread(flat, slot, step=0):
        return remote(
            vm.total, vm.totals.at[slot], sem.total_send.at[step], sem.total_recv.at[slot], flat
        )

    def gate_spread(flat, slot, step=0):
        return remote(
            vm.gate_total,
            vm.gate_totals.at[slot],
            sem.gate_send.at[step],
            sem.gate_recv.at[slot],
            flat,
        )

    def reduce_here(which, mine, held, total, totals, copy):
        for r in range(reducers):
            home = first_reducer + r

            @pl.when((core == home_core[which]) & (crew == home))
            def _():
                slot = r * OWNERS + chip
                for k in range(CORES):
                    out = None
                    for c in range(crews):
                        if c == home and k == home_core[which]:
                            term = mine[r]
                        else:
                            to_reducer(r, c, k, which).wait_recv()
                            term = held[c, k]
                        out = term if out is None else out + term
                    total[k] = out
                    totals[slot, k] = out
                for c in sorted(range(crews), key=lambda c: -abs(c - home)):

                    def send(i, carry):
                        copy(c * CREW + mate(i), slot, c * CREW + i).start()
                        return carry

                    lax.fori_loop(0 if c != home else 1, CREW, send, 0)

    def arrivals(which, copy):
        for i in range(reduced):
            flat = (first_reducer + i // OWNERS) * CREW + i % OWNERS * CORES + home_core[which]

            @pl.when(flat != me)
            def _():
                copy(me, i).wait_recv()

    def sent(which, copy):
        for r in range(reducers):
            home = first_reducer + r

            @pl.when((core == home_core[which]) & (crew == home))
            def _():
                for step in range(count):
                    if step != home * CREW:
                        copy(me, 0, step).wait_send()

    reduce_here(0, vm.part, vm.parts, vm.total, vm.totals, spread)
    loads_needed = ("norm_gain", "decay_bias", "post_gain", "up_weight", "key_weight")
    for name in loads_needed + ("value_weight",):
        loads[name].wait()
    arrivals(0, spread)
    def summed(totals, r, t):
        out = None
        for p in range(t, CREW, tp_count):
            term = totals[r * OWNERS + p // CORES, p % CORES]
            out = term if out is None else out + term
        return out

    for r in range(reducers):
        for t in range(tp_count):
            tile = summed(vm.totals, r, t)
            for s in range(share):
                at = (t * chunks + r * share + s) * LANES
                vm.mods[0:4, at : at + LANES] = tile[s * 4 : s * 4 + 4]

    gain = vm.norm_gain[...] * (1.0 + vm.mods[3:4, :])
    ctx_normed = (vm.ctx_scaled[...] * gain + vm.mods[2:3, :]).astype(bf16)
    head_k = iota((DV, 2 * LANES), 1) % LANES // DK
    key_at = pl.ds(pl.multiple_of(ctx_group * LANES, LANES), LANES)
    val_at = pl.ds(pl.multiple_of(ctx_group * GV, GV), GV)
    low = dot(ctx_normed, vm.down[...]).astype(bf16)
    log_rows = log_decays(dot(low, vm.up_weight[:, key_at]) + vm.decay_bias[:, key_at])
    keys = dot(ctx_normed, vm.key_weight[:, key_at]).astype(bf16).astype(f32)
    values = dot(ctx_normed, vm.value_weight[:, val_at]).astype(bf16)
    inclusive = running_sum(lower_ones(ctx_rows), log_rows)
    closing = inclusive[ctx_rows - 1 : ctx_rows, :]
    both = jnp.concatenate(
        [keys * jnp.exp(closing - inclusive), keys * jnp.exp(inclusive - log_rows)], axis=1
    ).astype(bf16)
    state = per_head(dot_tn(values, both), head_k)
    for j in range(OWNERS):
        at = slice(j * UNIT, (j + 1) * UNIT)
        vm.ctx_out[j] = jnp.concatenate([state[at, :LANES], state[at, LANES:]], axis=0).astype(bf16)
    vm.ctx_log[...] = closing

    def ctx_copies(o, p):
        flat = crew * CREW + owner_of(o)
        return (
            remote(vm.ctx_out.at[o], vm.ctx_in.at[p], sem.ctx_send.at[o], sem.ctx_recv.at[p], flat),
            remote(vm.ctx_log, vm.ctx_logs.at[p], sem.ctx_log_send.at[o], sem.ctx_log_recv.at[p], flat),
        )

    def ctx_start(o):
        for copy in ctx_copies(o, post):
            copy.start()

    owners(ctx_start)

    gain = vm.norm_gain[...] * (1.0 + vm.mods[1:2, :])
    shift = vm.mods[0:1, :]
    for i in range(rows // STRIP):
        at = slice(i * STRIP, (i + 1) * STRIP)
        vm.normed[at, :] = (vm.scaled[at, :] * gain + shift).astype(bf16)

    def project(weight, out):
        for n in range(0, weight.shape[1], COLS):
            at = slice(n, n + COLS)
            out[:, at] = dot(vm.normed[...], weight[:, at]).astype(bf16)

    def project_tile(weight, out, n):
        at = slice(n, min(n + COLS, weight.shape[1]))
        out[:, at] = dot(vm.normed[...], weight[:, at]).astype(bf16)

    tiles = [(vm.key_weight, vm.key, n) for n in range(0, vm.key_weight.shape[1], COLS)]
    tiles += [(vm.value_weight, vm.value, n) for n in range(0, vm.value_weight.shape[1], COLS)]
    low = dot(vm.normed[...], vm.down[...]).astype(bf16)
    project_tile(*tiles.pop(0))
    lower = lower_ones(TILE)
    offset = None
    for b in range(blocks):
        at = slice(b * TILE, (b + 1) * TILE)
        log_rows = log_decays(dot(low[at], vm.up_weight[...]) + vm.decay_bias[...])
        inclusive = running_sum(lower, log_rows)
        end = inclusive[TILE - 1 : TILE, :]
        vm.inclusive[at, :] = inclusive
        vm.before[at, :] = inclusive - log_rows
        vm.closing[b : b + 1, :] = end
        vm.offset[b : b + 1, :] = jnp.zeros_like(end) if offset is None else offset
        offset = end if offset is None else offset + end
        if tiles:
            project_tile(*tiles.pop(0))
    vm.offset[blocks : blocks + 1, :] = offset
    for g in range(GROUPS):
        vm.log_out[g : g + 1, :] = offset[:, g * LANES : (g + 1) * LANES]
    while tiles:
        project_tile(*tiles.pop(0))

    send_parts(1)

    def log_copy(o, p):
        return remote(
            vm.log_out, vm.logs.at[p], sem.log_send.at[o], sem.log_recv.at[p], crew * CREW + owner_of(o)
        )

    def early_copies(o, p):
        return (*ctx_copies(o, p), log_copy(o, p))

    owners(lambda o: log_copy(o, post).start())

    @pl.when(owner)
    def _():
        vm.ctx_in[post] = vm.ctx_out[chip]
        vm.ctx_logs[post] = vm.ctx_log[...]
        vm.logs[post] = vm.log_out[...]

    every = pl.ds(0, GROUPS)

    def seg_copy(o, p, g):
        return remote(
            vm.seg_out.at[o, g],
            vm.seg_in.at[p, g],
            sem.seg_send.at[o],
            sem.seg_recv.at[p],
            crew * CREW + owner_of(o),
        )

    for g in range(GROUPS):
        lanes = slice(g * LANES, (g + 1) * LANES)
        v_lanes = slice(g * GV, (g + 1) * GV)
        whole = vm.offset[blocks : blocks + 1, lanes]
        both = []
        for b in range(blocks):
            at = slice(b * TILE, (b + 1) * TILE)
            keys = vm.key[at, lanes].astype(f32)
            start, closing = vm.offset[b : b + 1, lanes], vm.closing[b : b + 1, lanes]
            ahead = keys * jnp.exp(closing - vm.inclusive[at, lanes])
            behind = keys * jnp.exp(vm.before[at, lanes])
            vm.k_block[g, at, :] = jnp.concatenate([ahead, behind], axis=1).astype(bf16)
            both.append(
                jnp.concatenate(
                    [ahead * jnp.exp((whole - start) - closing), behind * jnp.exp(start)], axis=1
                ).astype(bf16)
            )
        state = per_head(dot_tn(vm.value[:, v_lanes], jnp.concatenate(both, axis=0)), head_k)
        for j in range(OWNERS):
            at = slice(j * UNIT, (j + 1) * UNIT)
            vm.seg_out[j, g] = jnp.concatenate([state[at, :LANES], state[at, LANES:]], axis=0).astype(bf16)
        owners(lambda o: seg_copy(o, post, g).start())

    @pl.when(owner)
    def _():
        vm.seg_in[post] = vm.seg_out[chip]

    head_k1 = iota((TILE, LANES), 1) // DK
    head_v = iota((TILE, GV), 1) // DV
    t_index = iota((TILE, GROUP * TILE), 0)
    s_index = iota((TILE, GROUP * TILE), 1) % TILE

    def inside(g):
        lanes = slice(g * LANES, (g + 1) * LANES)
        v_lanes = slice(g * GV, (g + 1) * GV)
        whole = vm.offset[blocks : blocks + 1, lanes]
        for b in range(blocks):
            at = slice(b * TILE, (b + 1) * TILE)
            inclusive, before = vm.inclusive[at, lanes], vm.before[at, lanes]
            start = vm.offset[b : b + 1, lanes]
            closing = inclusive[TILE - 1 : TILE, :]
            middle = inclusive[TILE // 2 - 1 : TILE // 2, :]
            queries = vm.query[at, lanes].astype(f32) * DK ** (-0.5)
            keys = vm.key[at, lanes].astype(f32)
            scores = []
            for q_log, k_log in (
                (inclusive - middle, middle - inclusive),
                (middle - before, before - middle),
            ):
                k_stack = stacked((keys * jnp.exp(k_log)).astype(bf16), head_k1)
                scores.append(dot_nt((queries * jnp.exp(q_log)).astype(bf16), k_stack))
            both = jnp.where(t_index >= s_index, scores[0], 0.0) + jnp.where(
                t_index <= s_index, scores[1], 0.0
            )
            v_stack = stacked(vm.value[at, v_lanes], head_v)
            vm.within[at, v_lanes] = dot(both.astype(bf16), v_stack)
            ahead = queries * jnp.exp(inclusive)
            behind = queries * jnp.exp(closing - before)
            vm.q_block[g, at, :] = jnp.concatenate([ahead, behind], axis=1).astype(bf16)
            vm.q_whole[g, at, :] = jnp.concatenate(
                [ahead * jnp.exp(start), behind * jnp.exp((whole - start) - closing)], axis=1
            ).astype(bf16)

    def between(g):
        lanes = slice(g * LANES, (g + 1) * LANES)
        v_lanes = slice(g * GV, (g + 1) * GV)
        decays = [jnp.exp(vm.closing[b : b + 1, lanes]) for b in range(blocks)]
        left = []
        for b in range(blocks):
            at = slice(b * TILE, (b + 1) * TILE)
            left.append(per_head(dot_tn(vm.value[at, v_lanes], vm.k_block[g, at, :]), head_k))
        forward = [jnp.zeros((DV, LANES), f32)]
        backward = [jnp.zeros((DV, LANES), f32)]
        for b in range(blocks - 1):
            forward.append(decays[b] * forward[b] + left[b][:, :LANES])
            back = blocks - 1 - b
            backward.insert(0, decays[back] * backward[0] + left[back][:, LANES:])
        for b in range(blocks):
            at = slice(b * TILE, (b + 1) * TILE)
            states = jnp.concatenate([forward[b], backward[b]], axis=1)
            across = dot_nt(vm.q_block[g, at, :], stacked(states, head_k).astype(bf16))
            vm.within[at, v_lanes] = vm.within[at, v_lanes] + across

    loads["query_weight"].wait()
    project(vm.query_weight, vm.query)
    inside(0)

    def ctx_crew_copies(c, slot):
        flat = c * CREW + post
        return (
            remote(
                vm.ctx_crews_out,
                vm.ctx_crews.at[slot],
                sem.ctx_crew_send.at[c],
                sem.ctx_crew_recv.at[slot],
                flat,
            ),
            remote(
                vm.crew_log, vm.crew_logs.at[slot], sem.crew_log_send.at[c], sem.crew_log_recv.at[slot], flat
            ),
        )

    @pl.when(owner)
    def _():
        def early_in(p):
            for copy in early_copies(0, p):
                copy.wait_recv()

        mates(early_in)
        vm.decay[...] = jnp.exp(vm.logs[...])
        crew_log = vm.logs[0]
        for p in range(1, CREW):
            crew_log = crew_log + vm.logs[p]
        vm.crew_log[0, :GROUPS] = crew_log
        for g in range(GROUPS):
            posts = list(range(g, CREW, GROUPS))
            logs = [vm.ctx_logs[p] for p in posts]
            tiles = [vm.ctx_in[p].astype(f32) for p in posts]
            forward, backward, log_sum = tiles[0][:UNIT], tiles[-1][UNIT:], logs[0]
            for i in range(1, len(posts)):
                forward = jnp.exp(logs[i]) * forward + tiles[i][:UNIT]
                backward = jnp.exp(logs[-1 - i]) * backward + tiles[-1 - i][UNIT:]
                log_sum = log_sum + logs[i]
            vm.ctx_crews_out[g] = jnp.concatenate([forward, backward], axis=0).astype(bf16)
            vm.crew_log[1, g : g + 1, :] = log_sum

        def ctx_crew_start(i):
            for copy in ctx_crew_copies(lax.rem(crew + i, crews), crew):
                copy.start()

        others(ctx_crew_start, crews)
        vm.ctx_crews[crew] = vm.ctx_crews_out[...]
        vm.crew_logs[crew] = vm.crew_log[...]

    inside(1)

    reduce_here(1, vm.gate_part, vm.gate_parts, vm.gate_total, vm.gate_totals, gate_spread)

    def crew_copy(c, slot, side):
        return remote(
            vm.crew_out.at[side],
            vm.crew_in.at[slot],
            sem.crew_send.at[c],
            sem.crew_recv.at[slot],
            c * CREW + post,
        )

    def post_decay(p, g):
        return vm.decay[p, g : g + 1, :]

    @pl.when(owner)
    def _():
        mates(lambda p: seg_copy(0, p, every).wait_recv())
        for g in range(GROUPS):
            at = slice(g * UNIT, (g + 1) * UNIT)
            forward = vm.seg_in[0, g, :UNIT].astype(f32)
            for p in range(1, CREW):
                forward = post_decay(p, g) * forward + vm.seg_in[p, g, :UNIT].astype(f32)
            backward = vm.seg_in[CREW - 1, g, UNIT:].astype(f32)
            for p in range(CREW - 2, -1, -1):
                backward = post_decay(p, g) * backward + vm.seg_in[p, g, UNIT:].astype(f32)
            vm.crew_out[0, at, :] = forward.astype(bf16)
            vm.crew_out[1, at, :] = backward.astype(bf16)

        def crew_start(i):
            ahead, behind = crews - i, i - 1

            @pl.when(ahead > crew)
            def _():
                crew_copy(ahead, crew, 0).start()

            @pl.when(behind < crew)
            def _():
                crew_copy(behind, crew, 1).start()

        others(crew_start, crews)

    for g in range(2, GROUPS):
        inside(g)
    for g in range(GROUPS - 2):
        between(g)

    half = GROUPS // 2

    def enter_copy(p, o, h):
        part = pl.ds(h * half, half)
        return remote(
            vm.enter_out.at[p, part],
            vm.enter_in.at[o, part],
            sem.enter_send.at[h, p],
            sem.enter_recv.at[h, o],
            crew * CREW + p,
        )

    @pl.when(owner)
    def _():
        def ctx_arrived(i):
            c = lax.rem(crew + i, crews)
            for copy in ctx_crew_copies(c, c):
                copy.wait_recv()

        others(ctx_arrived, crews)
        vm.crew_decay[...] = jnp.exp(vm.crew_logs[...])
        zero = jnp.zeros((UNIT, LANES), f32)
        forward, backward = [zero] * GROUPS, [zero] * GROUPS
        for a in range(crews):
            z = crews - 1 - a
            for g in range(GROUPS):
                forward[g] = (
                    vm.crew_decay[a, 1, g : g + 1, :] * forward[g]
                    + vm.ctx_crews[a, g, :UNIT].astype(f32)
                )
                backward[g] = (
                    vm.crew_decay[z, 1, g : g + 1, :] * backward[g]
                    + vm.ctx_crews[z, g, UNIT:].astype(f32)
                )

        def step_states(c, states):
            left = vm.crew_in[c].astype(f32)
            return tuple(
                vm.crew_decay[c, 0, g : g + 1, :] * states[g] + left[g * UNIT : (g + 1) * UNIT]
                for g in range(GROUPS)
            )

        def from_before(c, states):
            crew_copy(c, c, 0).wait_recv()
            return step_states(c, states)

        def from_after(i, states):
            c = crews - 1 - i
            crew_copy(c, c, 1).wait_recv()
            return step_states(c, states)

        forward = lax.fori_loop(0, crew, from_before, tuple(forward))
        backward = lax.fori_loop(0, crews - 1 - crew, from_after, tuple(backward))
        for g in range(GROUPS):
            state = forward[g]
            for p in range(CREW):
                vm.enter_out[p, g, :UNIT] = state.astype(bf16)
                if p < CREW - 1:
                    state = post_decay(p, g) * state + vm.seg_in[p, g, :UNIT].astype(f32)
            state = backward[g]
            for p in range(CREW - 1, -1, -1):
                vm.enter_out[p, g, UNIT:] = state.astype(bf16)
                if p > 0:
                    state = post_decay(p, g) * state + vm.seg_in[p, g, UNIT:].astype(f32)
            if g % half == half - 1:
                mates(lambda p: enter_copy(p, chip, g // half).start())
        vm.enter_in[chip] = vm.enter_out[post]

    loads["outgate_weight"].wait()
    for n in range(0, vm.outgate_weight.shape[1], COLS):
        at = slice(n, n + COLS)
        gate = dot(vm.normed[...], vm.outgate_weight[:, at]).astype(bf16).astype(f32)
        vm.silu[:, at] = gate / (1.0 + jnp.exp(-gate))
    for g in range(GROUPS - 2, GROUPS):
        between(g)
    head_mean = jnp.where(iota((GV, GV), 0) // DV == iota((GV, GV), 1) // DV, 1.0 / DV, 0.0).astype(bf16)

    arrivals(1, gate_spread)
    for r in range(reducers):
        for t in range(tp_count):
            tile = summed(vm.gate_totals, r, t)
            for s in range(share):
                at = (t * chunks + r * share + s) * LANES
                vm.mods[4:5, at : at + LANES] = tile[s]
    loads["out_weight"].wait()

    for which in range(2):
        for r in range(reducers):

            @pl.when(elsewhere(r, which))
            def _():
                to_reducer(r, crew, core, which).wait_send()

    sent(0, spread)
    sent(1, gate_spread)

    def to_owner_sent(o):
        for copy in early_copies(o, post):
            copy.wait_send()
        seg_copy(o, post, every).wait_send()

    owners(to_owner_sent)

    @pl.when(owner)
    def _():
        def crew_sent(i):
            c = lax.rem(crew + i, crews)
            for copy in ctx_crew_copies(c, crew):
                copy.wait_send()
            crew_copy(c, crew, 0).wait_send()

        others(crew_sent, crews)

    def finish(g):
        v_lanes = slice(g * GV, (g + 1) * GV)
        states = jnp.concatenate(
            [
                jnp.concatenate([vm.enter_in[o, g, :UNIT] for o in range(OWNERS)], axis=0),
                jnp.concatenate([vm.enter_in[o, g, UNIT:] for o in range(OWNERS)], axis=0),
            ],
            axis=1,
        )
        across = dot_nt(vm.q_whole[g], stacked(states, head_k))
        mixed = vm.within[:, v_lanes] + across
        mean = dot((mixed * mixed).astype(bf16), head_mean)
        vm.gated[:, v_lanes] = (mixed * lax.rsqrt(mean + epsilon) * vm.silu[:, v_lanes]).astype(bf16)

    depth = half * GV
    owners(lambda o: enter_copy(post, o, 0).wait_recv())
    for g in range(half):
        finish(g)
    for n in range(0, width, COLS):
        at = slice(n, n + COLS)
        vm.branch_part[:, at] = dot(vm.gated[:, :depth], vm.out_weight[:depth, at])
    owners(lambda o: enter_copy(post, o, 1).wait_recv())
    for g in range(half, GROUPS):
        finish(g)

    square = jnp.zeros((rows, LANES), f32)
    for n in range(0, width, COLS):
        at = slice(n, n + COLS)
        branch = (vm.branch_part[:, at] + dot(vm.gated[:, depth:], vm.out_weight[depth:, at])).astype(bf16)
        vm.branch[:, at] = branch
        branch = branch.astype(f32)
        branch = branch * branch
        for s in range(0, COLS, LANES):
            square = square + branch[:, s : s + LANES]
    factor = lax.rsqrt(jnp.sum(square, axis=1, keepdims=True) / width + epsilon)
    gain = vm.mods[4:5, :] * vm.post_gain[...]
    for i in range(rows // STRIP):
        at = slice(i * STRIP, (i + 1) * STRIP)
        hbm.out[at, :] = (
            vm.latent[at, :].astype(f32) + gain * (vm.branch[at, :].astype(f32) * factor[at])
        ).astype(bf16)

    @pl.when(owner)
    def _():
        for h in range(2):
            mates(lambda p: enter_copy(p, chip, h).wait_send())


def shards(*operands):
    values = dict(zip(NAMES, operands))
    values["down_weight"] = values["down_weight"].T
    latent, context = values["latent"], values["context"]
    sp_count, tp_count = lax.axis_size("sp"), lax.axis_size("tp")
    count = sp_count * tp_count
    crews = count // CREW
    rows, width = latent.shape
    args, specs = [], []
    for name, value in values.items():
        vector = value.ndim == 1
        args.append(value.reshape(1, -1) if vector and value.dtype == f32 else value)
        specs.append(pl.BlockSpec(memory_space=pltpu.HBM))
    ctx_rows = context.shape[0] * GROUPS // tp_count
    chunks = values["shift_weight"].shape[1] // LANES
    reducers, share = reduction(chunks, crews)
    part_rows = -(-4 * share // SUB) * SUB
    keyw, valw = values["key_weight"].shape[1], values["value_weight"].shape[1]
    blocks = rows // TILE
    unit = (2 * UNIT, LANES)
    buffers = dict(
        context=pltpu.VMEM((ctx_rows, width), bf16),
        cond=pltpu.VMEM((SUB, width), f32),
        part=pltpu.VMEM((reducers, part_rows, LANES), f32),
        parts=pltpu.VMEM((crews, CORES, part_rows, LANES), f32),
        total=pltpu.VMEM((CORES, part_rows, LANES), f32),
        totals=pltpu.VMEM((reducers * OWNERS, CORES, part_rows, LANES), f32),
        gate_part=pltpu.VMEM((reducers, share, 1, LANES), f32),
        gate_parts=pltpu.VMEM((crews, CORES, share, 1, LANES), f32),
        gate_total=pltpu.VMEM((CORES, share, 1, LANES), f32),
        gate_totals=pltpu.VMEM((reducers * OWNERS, CORES, share, 1, LANES), f32),
        mods=pltpu.VMEM((SUB, width), f32),
        scaled=pltpu.VMEM((rows, width), f32),
        down=pltpu.VMEM((width, values["down_weight"].shape[0]), bf16),
        ctx_scaled=pltpu.VMEM((ctx_rows, width), f32),
        normed=pltpu.VMEM((rows, width), bf16),
        ctx_out=pltpu.VMEM((OWNERS, *unit), bf16),
        ctx_in=pltpu.VMEM((CREW, *unit), bf16),
        ctx_log=pltpu.VMEM((1, LANES), f32),
        ctx_logs=pltpu.VMEM((CREW, 1, LANES), f32),
        ctx_crews_out=pltpu.VMEM((GROUPS, *unit), bf16),
        ctx_crews=pltpu.VMEM((crews, GROUPS, *unit), bf16),
        key=pltpu.VMEM((rows, keyw), bf16),
        query=pltpu.VMEM((rows, keyw), bf16),
        value=pltpu.VMEM((rows, valw), bf16),
        silu=pltpu.VMEM((rows, valw), f32),
        gated=pltpu.VMEM((rows, valw), bf16),
        inclusive=pltpu.VMEM((rows, keyw), f32),
        before=pltpu.VMEM((rows, keyw), f32),
        closing=pltpu.VMEM((blocks, keyw), f32),
        offset=pltpu.VMEM((blocks + 1, keyw), f32),
        log_out=pltpu.VMEM((GROUPS, LANES), f32),
        logs=pltpu.VMEM((CREW, GROUPS, LANES), f32),
        decay=pltpu.VMEM((CREW, GROUPS, LANES), f32),
        crew_decay=pltpu.VMEM((crews, 2, SUB, LANES), f32),
        seg_out=pltpu.VMEM((OWNERS, GROUPS, *unit), bf16),
        seg_in=pltpu.VMEM((CREW, GROUPS, *unit), bf16),
        crew_out=pltpu.VMEM((2, GROUPS * UNIT, LANES), bf16),
        crew_in=pltpu.VMEM((crews, GROUPS * UNIT, LANES), bf16),
        crew_log=pltpu.VMEM((2, SUB, LANES), f32),
        crew_logs=pltpu.VMEM((crews, 2, SUB, LANES), f32),
        enter_out=pltpu.VMEM((CREW, GROUPS, *unit), bf16),
        enter_in=pltpu.VMEM((OWNERS, GROUPS, *unit), bf16),
        k_block=pltpu.VMEM((GROUPS, rows, 2 * LANES), bf16),
        q_block=pltpu.VMEM((GROUPS, rows, 2 * LANES), bf16),
        q_whole=pltpu.VMEM((GROUPS, rows, 2 * LANES), bf16),
        within=pltpu.VMEM((rows, valw), f32),
        branch_part=pltpu.VMEM((rows, width), f32),
        branch=pltpu.VMEM((rows, width), bf16),
    )
    for name, value in zip(NAMES, args):
        if name not in buffers:
            buffers[name] = pltpu.VMEM(value.shape, value.dtype)
    dma = pltpu.SemaphoreType.DMA
    semaphores = dict(
        load=dma((len(NAMES),)),
        part_send=dma((2, reducers)),
        part_recv=dma((2, crews, CORES)),
        total_send=dma((count,)),
        total_recv=dma((reducers * OWNERS,)),
        gate_send=dma((count,)),
        gate_recv=dma((reducers * OWNERS,)),
        ctx_send=dma((OWNERS,)),
        ctx_recv=dma((CREW,)),
        ctx_log_send=dma((OWNERS,)),
        ctx_log_recv=dma((CREW,)),
        log_send=dma((OWNERS,)),
        log_recv=dma((CREW,)),
        seg_send=dma((OWNERS,)),
        seg_recv=dma((CREW,)),
        ctx_crew_send=dma((crews,)),
        ctx_crew_recv=dma((crews,)),
        crew_log_send=dma((crews,)),
        crew_log_recv=dma((crews,)),
        crew_send=dma((crews,)),
        crew_recv=dma((crews,)),
        enter_send=dma((2, CREW)),
        enter_recv=dma((2, OWNERS)),
    )
    return pl.pallas_call(
        functools.partial(block_kernel, sp_count, tp_count),
        out_shape=pltpu.VMEM((rows, width), bf16),
        in_specs=specs,
        out_specs=pl.BlockSpec(memory_space=pltpu.VMEM),
        scratch_shapes=[buffers, semaphores],
        compiler_params=pltpu.CompilerParams(
            collective_id=0, has_side_effects=True, vmem_limit_bytes=VMEM_LIMIT
        ),
        name="block",
    )(*args)


def solution(mesh):
    placed = (
        P(("sp", "tp"), None),
        P("sp", None),
        P(),
        P(),
        P("sp", "tp"),
        P("sp", "tp"),
        P("sp", "tp"),
        P(),
        P(),
        P(),
        P(),
        P(),
        P(),
        P(),
        P(),
        P(),
        P(),
    )
    return jax.shard_map(
        shards, mesh=mesh, in_specs=placed, out_specs=P(("sp", "tp"), None), check_vma=False
    )
```

```python
import functools
from types import SimpleNamespace

import jax
import jax.numpy as jnp
from jax import lax
from jax.experimental import pallas as pl
from jax.experimental.pallas import tpu as pltpu
from jax.sharding import PartitionSpec as P

HEADS = 16
DK = 32
DV = 64
LANES = 128
SUB = 8
GROUP = LANES // DK
GV = GROUP * DV
GROUPS = HEADS // GROUP
CREW = DV // SUB
CORES = 2
OWNERS = CREW // CORES
UNIT = DV // OWNERS
MESH = pl.DeviceIdType.MESH
TILE = 64
COLS = 256
STRIP = 16
VMEM_LIMIT = 60 * 1024 * 1024

NAMES = (
    "latent",
    "context",
    "latent_condition",
    "context_condition",
    "shift_weight",
    "scale_weight",
    "gate_weight",
    "norm_gain",
    "query_weight",
    "key_weight",
    "value_weight",
    "outgate_weight",
    "down_weight",
    "up_weight",
    "decay_bias",
    "out_weight",
    "post_gain",
)
FIRST = (
    "latent_condition",
    "context_condition",
    "shift_weight",
    "scale_weight",
    "gate_weight",
)
LATER = (
    "context",
    "latent",
    "down_weight",
    "norm_gain",
    "decay_bias",
    "post_gain",
    "up_weight",
    "key_weight",
    "value_weight",
    "query_weight",
    "outgate_weight",
    "out_weight",
)

epsilon = 1e-06
decay_temper = 16.0
f32 = jnp.float32
bf16 = jnp.bfloat16


def dot(a, b):
    return jnp.dot(a, b, preferred_element_type=f32)


def dot_nt(a, b):
    return lax.dot_general(a, b, (((1,), (1,)), ((), ())), preferred_element_type=f32)


def dot_tn(a, b):
    return lax.dot_general(a, b, (((0,), (0,)), ((), ())), preferred_element_type=f32)


def iota(shape, axis):
    return lax.broadcasted_iota(jnp.int32, shape, axis)


def lower_ones(rows):
    return jnp.where(iota((rows, rows), 0) >= iota((rows, rows), 1), 1.0, 0.0).astype(bf16)


def running_sum(lower, log_rows):
    high = log_rows.astype(bf16)
    rest = log_rows - high.astype(f32)
    return dot(lower, high) + dot(lower, rest.astype(bf16))


def log_decays(values):
    return (jnp.minimum(values, 0.0) - jnp.log(1.0 + jnp.exp(-jnp.abs(values)))) * (1.0 / decay_temper)


def rms_factor(values):
    return lax.rsqrt(jnp.mean(values * values, axis=-1, keepdims=True) + epsilon)


def per_head(full, head):
    out = full[(GROUP - 1) * DV :]
    for h in range(GROUP - 2, -1, -1):
        out = jnp.where(head == h, full[h * DV : (h + 1) * DV], out)
    return out


def stacked(values, head):
    zero = jnp.zeros_like(values)
    return jnp.concatenate([jnp.where(head == h, values, zero) for h in range(GROUP)], axis=0)


def reduction(chunks, crews):
    reducers = min(2, chunks, crews)
    return reducers, chunks // reducers


def block_kernel(sp_count, tp_count, *refs):
    hbm = SimpleNamespace(**dict(zip((*NAMES, "out"), refs)))
    vm = SimpleNamespace(**refs[-2])
    sem = SimpleNamespace(**refs[-1])

    count = sp_count * tp_count
    crews = count // CREW
    sp, tp = lax.axis_index("sp"), lax.axis_index("tp")
    me = sp * tp_count + tp
    crew, post = lax.div(me, CREW), lax.rem(me, CREW)
    chip, core = lax.div(post, CORES), lax.rem(post, CORES)
    rows, width = hbm.latent.shape
    blocks = rows // TILE
    row_share = hbm.shift_weight.shape[0]
    chunks = hbm.shift_weight.shape[1] // LANES
    reducers, share = reduction(chunks, crews)
    first_reducer = (crews - reducers) // 2
    owner = core == CORES - 1
    middle_crew = (crew >= first_reducer) & (crew < first_reducer + reducers)
    reducer = owner & middle_crew
    ctx_rows = vm.context.shape[0]
    ctx_group = lax.rem(tp, GROUPS)

    def place(flat):
        return (lax.div(flat, jnp.int32(tp_count)), lax.rem(flat, jnp.int32(tp_count)))

    def remote(src, dst, send, recv, flat):
        return pltpu.make_async_remote_copy(
            src_ref=src,
            dst_ref=dst,
            send_sem=send,
            recv_sem=recv,
            device_id=place(flat),
            device_id_type=MESH,
        )

    def others(body, total):
        def step(i, carry):
            body(i)
            return carry

        lax.fori_loop(1, total, step, 0)

    def mate(i):
        return lax.rem(post + i, CREW)

    def mates(body):
        for i in range(1, CREW):
            body(mate(i))

    def owners(body):
        for i in range(OWNERS):
            at = lax.rem(chip + i, OWNERS)
            if i == 0:
                pl.when(jnp.logical_not(owner))(functools.partial(body, at))
            else:
                body(at)

    def owner_of(at):
        return at * CORES + CORES - 1

    ctx_at = pl.multiple_of((tp // GROUPS) * ctx_rows, SUB)
    hbm.context = hbm.context.at[pl.ds(ctx_at, ctx_rows)]
    loads = {
        name: pltpu.make_async_copy(getattr(hbm, name), getattr(vm, name), sem.load.at[i])
        for i, name in enumerate(FIRST + LATER)
    }
    for name in FIRST:
        loads[name].start()

    barrier = pltpu.get_barrier_semaphore()

    def greet(flat):
        pl.semaphore_signal(barrier, inc=1, device_id=place(flat), device_id_type=MESH)

    for r in range(reducers):
        for q in range(OWNERS):
            flat = (first_reducer + r) * CREW + owner_of(q)

            @pl.when(flat != me)
            def _():
                greet(flat)

    @pl.when(reducer)
    def _():
        for c in range(crews):
            for k in range(CORES):
                if k < CORES - 1 or not first_reducer <= c < first_reducer + reducers:
                    greet(c * CREW + chip * CORES + k)

    loads["latent_condition"].wait()
    loads["context_condition"].wait()
    vm.cond[0:1, :] = vm.latent_condition[...].astype(f32).reshape(1, width)
    vm.cond[1:2, :] = vm.context_condition[...].astype(f32).reshape(1, width)
    mine = pl.ds(pl.multiple_of(sp * row_share, LANES), row_share)
    pick = iota((STRIP, row_share), 0) == 0
    raw = jnp.where(pick, vm.cond[0:1, mine], vm.cond[1:2, mine])
    cond = (raw / (1.0 + jnp.exp(-raw))).astype(bf16)
    loads["shift_weight"].wait()
    loads["scale_weight"].wait()
    for which, weight in enumerate((vm.shift_weight, vm.scale_weight)):
        part = dot(cond, weight[...])
        for c in range(chunks):
            at = slice(c * LANES, (c + 1) * LANES)
            r, row = c // share, c % share * 4 + which
            vm.part[r, row : row + 1, :] = part[0:1, at]
            vm.part[r, row + 2 : row + 3, :] = part[1:2, at]
    for name in LATER:
        loads[name].start()
    @pl.when(jnp.logical_not(reducer))
    def _():
        pl.semaphore_wait(barrier, reducers)

    home_core = (CORES - 1, 0)

    def to_reducer(r, c, k, which):
        part, parts = ((vm.part, vm.parts), (vm.gate_part, vm.gate_parts))[which]
        return remote(
            part.at[r],
            parts.at[c, k],
            sem.part_send.at[which, r],
            sem.part_recv.at[which, c, k],
            (first_reducer + r) * CREW + chip * CORES + home_core[which],
        )

    def elsewhere(r, which):
        return jnp.logical_not((core == home_core[which]) & (crew == first_reducer + r))

    def send_parts(which):
        for r in range(reducers):

            @pl.when(elsewhere(r, which))
            def _():
                to_reducer(r, crew, core, which).start()

    def early_part(r):
        return to_reducer(r, crew, 0, 0)

    for r in range(reducers):

        @pl.when(jnp.logical_not(elsewhere(r, 0)))
        def _():
            early_part(r).wait_recv()

    send_parts(0)
    loads["gate_weight"].wait()
    part = dot(cond, vm.gate_weight[...])
    for c in range(chunks):
        vm.gate_part[c // share, c % share] = part[0:1, c * LANES : (c + 1) * LANES]

    loads["context"].wait()
    xc = vm.context[...].astype(f32)
    vm.ctx_scaled[...] = xc * rms_factor(xc)
    loads["latent"].wait()

    def scale_strip(i, carry):
        at = pl.ds(pl.multiple_of(i * TILE, TILE), TILE)
        x = vm.latent[at, :].astype(f32)
        vm.scaled[at, :] = x * rms_factor(x)
        return carry

    lax.fori_loop(0, rows // TILE, scale_strip, 0)
    loads["down_weight"].wait()
    vm.down[...] = vm.down_weight[...].T

    reduced = reducers * OWNERS

    def spread(flat, slot, step=0):
        return remote(
            vm.total, vm.totals.at[slot], sem.total_send.at[step], sem.total_recv.at[slot], flat
        )

    def gate_spread(flat, slot, step=0):
        return remote(
            vm.gate_total,
            vm.gate_totals.at[slot],
            sem.gate_send.at[step],
            sem.gate_recv.at[slot],
            flat,
        )

    def reduce_here(which, mine, held, total, totals, copy):
        for r in range(reducers):
            home = first_reducer + r

            @pl.when((core == home_core[which]) & (crew == home))
            def _():
                slot = r * OWNERS + chip
                for k in range(CORES):
                    out = None
                    for c in range(crews):
                        if c == home and k == home_core[which]:
                            term = mine[r]
                        else:
                            if which == 1 or c != home or k != 0:
                                to_reducer(r, c, k, which).wait_recv()
                            term = held[c, k]
                        out = term if out is None else out + term
                    total[k] = out
                    totals[slot, k] = out
                for c in sorted(range(crews), key=lambda c: -abs(c - home)):

                    def send(i, carry):
                        copy(c * CREW + mate(i), slot, c * CREW + i).start()
                        return carry

                    lax.fori_loop(0 if c != home else 1, CREW, send, 0)

    def arrivals(which, copy):
        for i in range(reduced):
            flat = (first_reducer + i // OWNERS) * CREW + i % OWNERS * CORES + home_core[which]

            @pl.when(flat != me)
            def _():
                copy(me, i).wait_recv()

    def sent(which, copy):
        for r in range(reducers):
            home = first_reducer + r

            @pl.when((core == home_core[which]) & (crew == home))
            def _():
                for step in range(count):
                    if step != home * CREW:
                        copy(me, 0, step).wait_send()

    @pl.when(reducer)
    def _():
        pl.semaphore_wait(barrier, count - 1)

    reduce_here(0, vm.part, vm.parts, vm.total, vm.totals, spread)
    loads_needed = ("norm_gain", "decay_bias", "post_gain", "up_weight", "key_weight")
    for name in loads_needed + ("value_weight",):
        loads[name].wait()
    arrivals(0, spread)
    def summed(totals, r, t):
        out = None
        for p in range(t, CREW, tp_count):
            term = totals[r * OWNERS + p // CORES, p % CORES]
            out = term if out is None else out + term
        return out

    for r in range(reducers):
        for t in range(tp_count):
            tile = summed(vm.totals, r, t)
            for s in range(share):
                at = (t * chunks + r * share + s) * LANES
                vm.mods[0:4, at : at + LANES] = tile[s * 4 : s * 4 + 4]

    gain = vm.norm_gain[...] * (1.0 + vm.mods[3:4, :])
    ctx_normed = (vm.ctx_scaled[...] * gain + vm.mods[2:3, :]).astype(bf16)
    head_k = iota((DV, 2 * LANES), 1) % LANES // DK
    key_at = pl.ds(pl.multiple_of(ctx_group * LANES, LANES), LANES)
    val_at = pl.ds(pl.multiple_of(ctx_group * GV, GV), GV)
    low = dot(ctx_normed, vm.down[...]).astype(bf16)
    log_rows = log_decays(dot(low, vm.up_weight[:, key_at]) + vm.decay_bias[:, key_at])
    keys = dot(ctx_normed, vm.key_weight[:, key_at]).astype(bf16).astype(f32)
    values = dot(ctx_normed, vm.value_weight[:, val_at]).astype(bf16)
    inclusive = running_sum(lower_ones(ctx_rows), log_rows)
    closing = inclusive[ctx_rows - 1 : ctx_rows, :]
    both = jnp.concatenate(
        [keys * jnp.exp(closing - inclusive), keys * jnp.exp(inclusive - log_rows)], axis=1
    ).astype(bf16)
    state = per_head(dot_tn(values, both), head_k)
    for j in range(OWNERS):
        at = slice(j * UNIT, (j + 1) * UNIT)
        vm.ctx_out[j] = jnp.concatenate([state[at, :LANES], state[at, LANES:]], axis=0).astype(bf16)
    vm.ctx_log[...] = closing

    def ctx_copies(o, p):
        flat = crew * CREW + owner_of(o)
        return (
            remote(vm.ctx_out.at[o], vm.ctx_in.at[p], sem.ctx_send.at[o], sem.ctx_recv.at[p], flat),
            remote(vm.ctx_log, vm.ctx_logs.at[p], sem.ctx_log_send.at[o], sem.ctx_log_recv.at[p], flat),
        )

    def ctx_start(o):
        for copy in ctx_copies(o, post):
            copy.start()

    owners(ctx_start)

    gain = vm.norm_gain[...] * (1.0 + vm.mods[1:2, :])
    shift = vm.mods[0:1, :]
    for i in range(rows // STRIP):
        at = slice(i * STRIP, (i + 1) * STRIP)
        vm.normed[at, :] = (vm.scaled[at, :] * gain + shift).astype(bf16)

    def project(weight, out):
        for n in range(0, weight.shape[1], COLS):
            at = slice(n, n + COLS)
            out[:, at] = dot(vm.normed[...], weight[:, at]).astype(bf16)

    def project_tile(weight, out, n):
        at = slice(n, min(n + COLS, weight.shape[1]))
        out[:, at] = dot(vm.normed[...], weight[:, at]).astype(bf16)

    tiles = [(vm.key_weight, vm.key, n) for n in range(0, vm.key_weight.shape[1], COLS)]
    tiles += [(vm.value_weight, vm.value, n) for n in range(0, vm.value_weight.shape[1], COLS)]
    low = dot(vm.normed[...], vm.down[...]).astype(bf16)
    project_tile(*tiles.pop(0))
    lower = lower_ones(TILE)
    offset = None
    for b in range(blocks):
        at = slice(b * TILE, (b + 1) * TILE)
        log_rows = log_decays(dot(low[at], vm.up_weight[...]) + vm.decay_bias[...])
        inclusive = running_sum(lower, log_rows)
        end = inclusive[TILE - 1 : TILE, :]
        vm.inclusive[at, :] = inclusive
        vm.before[at, :] = inclusive - log_rows
        vm.closing[b : b + 1, :] = end
        vm.offset[b : b + 1, :] = jnp.zeros_like(end) if offset is None else offset
        offset = end if offset is None else offset + end
        if tiles:
            project_tile(*tiles.pop(0))
    vm.offset[blocks : blocks + 1, :] = offset
    for g in range(GROUPS):
        vm.log_out[g : g + 1, :] = offset[:, g * LANES : (g + 1) * LANES]
    while tiles:
        project_tile(*tiles.pop(0))

    send_parts(1)

    def log_copy(o, p):
        return remote(
            vm.log_out, vm.logs.at[p], sem.log_send.at[o], sem.log_recv.at[p], crew * CREW + owner_of(o)
        )

    def early_copies(o, p):
        return (*ctx_copies(o, p), log_copy(o, p))

    owners(lambda o: log_copy(o, post).start())

    @pl.when(owner)
    def _():
        vm.ctx_in[post] = vm.ctx_out[chip]
        vm.ctx_logs[post] = vm.ctx_log[...]
        vm.logs[post] = vm.log_out[...]

    every = pl.ds(0, GROUPS)

    def seg_copy(o, p, g):
        return remote(
            vm.seg_out.at[o, g],
            vm.seg_in.at[p, g],
            sem.seg_send.at[o],
            sem.seg_recv.at[p],
            crew * CREW + owner_of(o),
        )

    for g in range(GROUPS):
        lanes = slice(g * LANES, (g + 1) * LANES)
        v_lanes = slice(g * GV, (g + 1) * GV)
        whole = vm.offset[blocks : blocks + 1, lanes]
        both = []
        for b in range(blocks):
            at = slice(b * TILE, (b + 1) * TILE)
            keys = vm.key[at, lanes].astype(f32)
            start, closing = vm.offset[b : b + 1, lanes], vm.closing[b : b + 1, lanes]
            ahead = keys * jnp.exp(closing - vm.inclusive[at, lanes])
            behind = keys * jnp.exp(vm.before[at, lanes])
            vm.k_block[g, at, :] = jnp.concatenate([ahead, behind], axis=1).astype(bf16)
            both.append(
                jnp.concatenate(
                    [ahead * jnp.exp((whole - start) - closing), behind * jnp.exp(start)], axis=1
                ).astype(bf16)
            )
        state = per_head(dot_tn(vm.value[:, v_lanes], jnp.concatenate(both, axis=0)), head_k)
        for j in range(OWNERS):
            at = slice(j * UNIT, (j + 1) * UNIT)
            vm.seg_out[j, g] = jnp.concatenate([state[at, :LANES], state[at, LANES:]], axis=0).astype(bf16)
        owners(lambda o: seg_copy(o, post, g).start())

    @pl.when(owner)
    def _():
        vm.seg_in[post] = vm.seg_out[chip]

    def ctx_crew_copies(c, slot):
        flat = c * CREW + post
        return (
            remote(
                vm.ctx_crews_out,
                vm.ctx_crews.at[slot],
                sem.ctx_crew_send.at[c],
                sem.ctx_crew_recv.at[slot],
                flat,
            ),
            remote(
                vm.ctx_crews_log,
                vm.ctx_crews_logs.at[slot],
                sem.ctx_crew_log_send.at[c],
                sem.ctx_crew_log_recv.at[slot],
                flat,
            ),
        )

    @pl.when(owner)
    def _():
        def ctx_arrived(p):
            for copy in ctx_copies(0, p):
                copy.wait_recv()

        mates(ctx_arrived)
        for g in range(GROUPS):
            posts = list(range(g, CREW, GROUPS))
            logs = [vm.ctx_logs[p] for p in posts]
            tiles = [vm.ctx_in[p].astype(f32) for p in posts]
            forward, backward, log_sum = tiles[0][:UNIT], tiles[-1][UNIT:], logs[0]
            for i in range(1, len(posts)):
                forward = jnp.exp(logs[i]) * forward + tiles[i][:UNIT]
                backward = jnp.exp(logs[-1 - i]) * backward + tiles[-1 - i][UNIT:]
                log_sum = log_sum + logs[i]
            vm.ctx_crews_out[g] = jnp.concatenate([forward, backward], axis=0).astype(bf16)
            vm.ctx_crews_log[g : g + 1, :] = log_sum

        def ctx_crew_start(i):
            for copy in ctx_crew_copies(lax.rem(crew + i, crews), crew):
                copy.start()

        others(ctx_crew_start, crews)
        vm.ctx_crews[crew] = vm.ctx_crews_out[...]
        vm.ctx_crews_logs[crew] = vm.ctx_crews_log[...]

    head_k1 = iota((TILE, LANES), 1) // DK
    head_v = iota((TILE, GV), 1) // DV
    t_index = iota((TILE, GROUP * TILE), 0)
    s_index = iota((TILE, GROUP * TILE), 1) % TILE

    def inside(g):
        lanes = slice(g * LANES, (g + 1) * LANES)
        v_lanes = slice(g * GV, (g + 1) * GV)
        whole = vm.offset[blocks : blocks + 1, lanes]
        for b in range(blocks):
            at = slice(b * TILE, (b + 1) * TILE)
            inclusive, before = vm.inclusive[at, lanes], vm.before[at, lanes]
            start = vm.offset[b : b + 1, lanes]
            closing = inclusive[TILE - 1 : TILE, :]
            middle = inclusive[TILE // 2 - 1 : TILE // 2, :]
            queries = vm.query[at, lanes].astype(f32) * DK ** (-0.5)
            keys = vm.key[at, lanes].astype(f32)
            scores = []
            for q_log, k_log in (
                (inclusive - middle, middle - inclusive),
                (middle - before, before - middle),
            ):
                k_stack = stacked((keys * jnp.exp(k_log)).astype(bf16), head_k1)
                scores.append(dot_nt((queries * jnp.exp(q_log)).astype(bf16), k_stack))
            both = jnp.where(t_index >= s_index, scores[0], 0.0) + jnp.where(
                t_index <= s_index, scores[1], 0.0
            )
            v_stack = stacked(vm.value[at, v_lanes], head_v)
            vm.within[at, v_lanes] = dot(both.astype(bf16), v_stack)
            ahead = queries * jnp.exp(inclusive)
            behind = queries * jnp.exp(closing - before)
            vm.q_block[g, at, :] = jnp.concatenate([ahead, behind], axis=1).astype(bf16)
            vm.q_whole[g, at, :] = jnp.concatenate(
                [ahead * jnp.exp(start), behind * jnp.exp((whole - start) - closing)], axis=1
            ).astype(bf16)

    def between(g):
        lanes = slice(g * LANES, (g + 1) * LANES)
        v_lanes = slice(g * GV, (g + 1) * GV)
        decays = [jnp.exp(vm.closing[b : b + 1, lanes]) for b in range(blocks)]
        left = []
        for b in range(blocks):
            at = slice(b * TILE, (b + 1) * TILE)
            left.append(per_head(dot_tn(vm.value[at, v_lanes], vm.k_block[g, at, :]), head_k))
        forward = [jnp.zeros((DV, LANES), f32)]
        backward = [jnp.zeros((DV, LANES), f32)]
        for b in range(blocks - 1):
            forward.append(decays[b] * forward[b] + left[b][:, :LANES])
            back = blocks - 1 - b
            backward.insert(0, decays[back] * backward[0] + left[back][:, LANES:])
        for b in range(blocks):
            at = slice(b * TILE, (b + 1) * TILE)
            states = jnp.concatenate([forward[b], backward[b]], axis=1)
            across = dot_nt(vm.q_block[g, at, :], stacked(states, head_k).astype(bf16))
            vm.within[at, v_lanes] = vm.within[at, v_lanes] + across

    loads["query_weight"].wait()
    project(vm.query_weight, vm.query)
    inside(0)

    def crew_log_copy(c, slot):
        return remote(
            vm.crew_log,
            vm.crew_logs.at[slot],
            sem.crew_log_send.at[c],
            sem.crew_log_recv.at[slot],
            c * CREW + post,
        )

    @pl.when(owner)
    def _():
        mates(lambda p: log_copy(0, p).wait_recv())
        vm.decay[...] = jnp.exp(vm.logs[...])
        crew_log = vm.logs[0]
        for p in range(1, CREW):
            crew_log = crew_log + vm.logs[p]
        vm.crew_log[...] = crew_log
        others(lambda i: crew_log_copy(lax.rem(crew + i, crews), crew).start(), crews)

    inside(1)

    reduce_here(1, vm.gate_part, vm.gate_parts, vm.gate_total, vm.gate_totals, gate_spread)

    def crew_copy(c, slot, side):
        return remote(
            vm.crew_out.at[side],
            vm.crew_in.at[slot],
            sem.crew_send.at[c],
            sem.crew_recv.at[slot],
            c * CREW + post,
        )

    def post_decay(p, g):
        return vm.decay[p, g : g + 1, :]

    @pl.when(owner)
    def _():
        mates(lambda p: seg_copy(0, p, every).wait_recv())
        for g in range(GROUPS):
            at = slice(g * UNIT, (g + 1) * UNIT)
            forward = vm.seg_in[0, g, :UNIT].astype(f32)
            for p in range(1, CREW):
                forward = post_decay(p, g) * forward + vm.seg_in[p, g, :UNIT].astype(f32)
            backward = vm.seg_in[CREW - 1, g, UNIT:].astype(f32)
            for p in range(CREW - 2, -1, -1):
                backward = post_decay(p, g) * backward + vm.seg_in[p, g, UNIT:].astype(f32)
            vm.crew_out[0, at, :] = forward.astype(bf16)
            vm.crew_out[1, at, :] = backward.astype(bf16)

        def crew_start(i):
            ahead, behind = crews - i, i - 1

            @pl.when(ahead > crew)
            def _():
                crew_copy(ahead, crew, 0).start()

            @pl.when(behind < crew)
            def _():
                crew_copy(behind, crew, 1).start()

        others(crew_start, crews)

    for g in range(2, GROUPS):
        inside(g)
    for g in range(GROUPS - 2):
        between(g)

    half = GROUPS // 2

    def enter_copy(p, o, h):
        part = pl.ds(h * half, half)
        return remote(
            vm.enter_out.at[p, part],
            vm.enter_in.at[o, part],
            sem.enter_send.at[h, p],
            sem.enter_recv.at[h, o],
            crew * CREW + p,
        )

    @pl.when(owner)
    def _():
        def ctx_arrived(i):
            c = lax.rem(crew + i, crews)
            for copy in (*ctx_crew_copies(c, c), crew_log_copy(c, c)):
                copy.wait_recv()

        others(ctx_arrived, crews)
        vm.crew_decay[...] = jnp.exp(vm.crew_logs[...])
        vm.ctx_decay[...] = jnp.exp(vm.ctx_crews_logs[...])
        zero = jnp.zeros((UNIT, LANES), f32)
        forward, backward = [zero] * GROUPS, [zero] * GROUPS
        for a in range(crews):
            z = crews - 1 - a
            for g in range(GROUPS):
                forward[g] = (
                    vm.ctx_decay[a, g : g + 1, :] * forward[g]
                    + vm.ctx_crews[a, g, :UNIT].astype(f32)
                )
                backward[g] = (
                    vm.ctx_decay[z, g : g + 1, :] * backward[g]
                    + vm.ctx_crews[z, g, UNIT:].astype(f32)
                )

        def step_states(c, states):
            left = vm.crew_in[c].astype(f32)
            return tuple(
                vm.crew_decay[c, g : g + 1, :] * states[g] + left[g * UNIT : (g + 1) * UNIT]
                for g in range(GROUPS)
            )

        def from_before(c, states):
            crew_copy(c, c, 0).wait_recv()
            return step_states(c, states)

        def from_after(i, states):
            c = crews - 1 - i
            crew_copy(c, c, 1).wait_recv()
            return step_states(c, states)

        forward = lax.fori_loop(0, crew, from_before, tuple(forward))
        backward = lax.fori_loop(0, crews - 1 - crew, from_after, tuple(backward))
        for g in range(GROUPS):
            state = forward[g]
            for p in range(CREW):
                vm.enter_out[p, g, :UNIT] = state.astype(bf16)
                if p < CREW - 1:
                    state = post_decay(p, g) * state + vm.seg_in[p, g, :UNIT].astype(f32)
            state = backward[g]
            for p in range(CREW - 1, -1, -1):
                vm.enter_out[p, g, UNIT:] = state.astype(bf16)
                if p > 0:
                    state = post_decay(p, g) * state + vm.seg_in[p, g, UNIT:].astype(f32)
            if g % half == half - 1:
                mates(lambda p: enter_copy(p, chip, g // half).start())
        vm.enter_in[chip] = vm.enter_out[post]

    loads["outgate_weight"].wait()
    for n in range(0, vm.outgate_weight.shape[1], COLS):
        at = slice(n, n + COLS)
        gate = dot(vm.normed[...], vm.outgate_weight[:, at]).astype(bf16).astype(f32)
        vm.silu[:, at] = gate / (1.0 + jnp.exp(-gate))
    for g in range(GROUPS - 2, GROUPS):
        between(g)
    head_mean = jnp.where(iota((GV, GV), 0) // DV == iota((GV, GV), 1) // DV, 1.0 / DV, 0.0).astype(bf16)

    arrivals(1, gate_spread)
    for r in range(reducers):
        for t in range(tp_count):
            tile = summed(vm.gate_totals, r, t)
            for s in range(share):
                at = (t * chunks + r * share + s) * LANES
                vm.mods[4:5, at : at + LANES] = tile[s]
    loads["out_weight"].wait()

    for which in range(2):
        for r in range(reducers):

            @pl.when(elsewhere(r, which))
            def _():
                to_reducer(r, crew, core, which).wait_send()

    sent(0, spread)
    sent(1, gate_spread)

    def to_owner_sent(o):
        for copy in early_copies(o, post):
            copy.wait_send()
        seg_copy(o, post, every).wait_send()

    owners(to_owner_sent)

    @pl.when(owner)
    def _():
        def crew_sent(i):
            c = lax.rem(crew + i, crews)
            for copy in (*ctx_crew_copies(c, crew), crew_log_copy(c, crew)):
                copy.wait_send()
            crew_copy(c, crew, 0).wait_send()

        others(crew_sent, crews)

    def finish(g):
        v_lanes = slice(g * GV, (g + 1) * GV)
        states = jnp.concatenate(
            [
                jnp.concatenate([vm.enter_in[o, g, :UNIT] for o in range(OWNERS)], axis=0),
                jnp.concatenate([vm.enter_in[o, g, UNIT:] for o in range(OWNERS)], axis=0),
            ],
            axis=1,
        )
        across = dot_nt(vm.q_whole[g], stacked(states, head_k))
        mixed = vm.within[:, v_lanes] + across
        mean = dot((mixed * mixed).astype(bf16), head_mean)
        vm.gated[:, v_lanes] = (mixed * lax.rsqrt(mean + epsilon) * vm.silu[:, v_lanes]).astype(bf16)

    depth = half * GV
    owners(lambda o: enter_copy(post, o, 0).wait_recv())
    for g in range(half):
        finish(g)
    for n in range(0, width, COLS):
        at = slice(n, n + COLS)
        vm.branch_part[:, at] = dot(vm.gated[:, :depth], vm.out_weight[:depth, at])
    owners(lambda o: enter_copy(post, o, 1).wait_recv())
    for g in range(half, GROUPS):
        finish(g)

    square = jnp.zeros((rows, LANES), f32)
    for n in range(0, width, COLS):
        at = slice(n, n + COLS)
        branch = (vm.branch_part[:, at] + dot(vm.gated[:, depth:], vm.out_weight[depth:, at])).astype(bf16)
        vm.branch[:, at] = branch
        branch = branch.astype(f32)
        branch = branch * branch
        for s in range(0, COLS, LANES):
            square = square + branch[:, s : s + LANES]
    factor = lax.rsqrt(jnp.sum(square, axis=1, keepdims=True) / width + epsilon)
    gain = vm.mods[4:5, :] * vm.post_gain[...]
    for i in range(rows // STRIP):
        at = slice(i * STRIP, (i + 1) * STRIP)
        hbm.out[at, :] = (
            vm.latent[at, :].astype(f32) + gain * (vm.branch[at, :].astype(f32) * factor[at])
        ).astype(bf16)

    @pl.when(owner)
    def _():
        for h in range(2):
            mates(lambda p: enter_copy(p, chip, h).wait_send())


def shards(*operands):
    values = dict(zip(NAMES, operands))
    values["down_weight"] = values["down_weight"].T
    latent, context = values["latent"], values["context"]
    sp_count, tp_count = lax.axis_size("sp"), lax.axis_size("tp")
    count = sp_count * tp_count
    crews = count // CREW
    rows, width = latent.shape
    args, specs = [], []
    for name, value in values.items():
        vector = value.ndim == 1
        args.append(value.reshape(1, -1) if vector and value.dtype == f32 else value)
        specs.append(pl.BlockSpec(memory_space=pltpu.HBM))
    ctx_rows = context.shape[0] * GROUPS // tp_count
    chunks = values["shift_weight"].shape[1] // LANES
    reducers, share = reduction(chunks, crews)
    part_rows = -(-4 * share // SUB) * SUB
    keyw, valw = values["key_weight"].shape[1], values["value_weight"].shape[1]
    blocks = rows // TILE
    unit = (2 * UNIT, LANES)
    buffers = dict(
        context=pltpu.VMEM((ctx_rows, width), bf16),
        cond=pltpu.VMEM((SUB, width), f32),
        part=pltpu.VMEM((reducers, part_rows, LANES), f32),
        parts=pltpu.VMEM((crews, CORES, part_rows, LANES), f32),
        total=pltpu.VMEM((CORES, part_rows, LANES), f32),
        totals=pltpu.VMEM((reducers * OWNERS, CORES, part_rows, LANES), f32),
        gate_part=pltpu.VMEM((reducers, share, 1, LANES), f32),
        gate_parts=pltpu.VMEM((crews, CORES, share, 1, LANES), f32),
        gate_total=pltpu.VMEM((CORES, share, 1, LANES), f32),
        gate_totals=pltpu.VMEM((reducers * OWNERS, CORES, share, 1, LANES), f32),
        mods=pltpu.VMEM((SUB, width), f32),
        scaled=pltpu.VMEM((rows, width), f32),
        down=pltpu.VMEM((width, values["down_weight"].shape[0]), bf16),
        ctx_scaled=pltpu.VMEM((ctx_rows, width), f32),
        normed=pltpu.VMEM((rows, width), bf16),
        ctx_out=pltpu.VMEM((OWNERS, *unit), bf16),
        ctx_in=pltpu.VMEM((CREW, *unit), bf16),
        ctx_log=pltpu.VMEM((1, LANES), f32),
        ctx_logs=pltpu.VMEM((CREW, 1, LANES), f32),
        ctx_crews_out=pltpu.VMEM((GROUPS, *unit), bf16),
        ctx_crews=pltpu.VMEM((crews, GROUPS, *unit), bf16),
        key=pltpu.VMEM((rows, keyw), bf16),
        query=pltpu.VMEM((rows, keyw), bf16),
        value=pltpu.VMEM((rows, valw), bf16),
        silu=pltpu.VMEM((rows, valw), f32),
        gated=pltpu.VMEM((rows, valw), bf16),
        inclusive=pltpu.VMEM((rows, keyw), f32),
        before=pltpu.VMEM((rows, keyw), f32),
        closing=pltpu.VMEM((blocks, keyw), f32),
        offset=pltpu.VMEM((blocks + 1, keyw), f32),
        log_out=pltpu.VMEM((GROUPS, LANES), f32),
        logs=pltpu.VMEM((CREW, GROUPS, LANES), f32),
        decay=pltpu.VMEM((CREW, GROUPS, LANES), f32),
        crew_decay=pltpu.VMEM((crews, GROUPS, LANES), f32),
        ctx_decay=pltpu.VMEM((crews, GROUPS, LANES), f32),
        ctx_crews_log=pltpu.VMEM((GROUPS, LANES), f32),
        ctx_crews_logs=pltpu.VMEM((crews, GROUPS, LANES), f32),
        seg_out=pltpu.VMEM((OWNERS, GROUPS, *unit), bf16),
        seg_in=pltpu.VMEM((CREW, GROUPS, *unit), bf16),
        crew_out=pltpu.VMEM((2, GROUPS * UNIT, LANES), bf16),
        crew_in=pltpu.VMEM((crews, GROUPS * UNIT, LANES), bf16),
        crew_log=pltpu.VMEM((GROUPS, LANES), f32),
        crew_logs=pltpu.VMEM((crews, GROUPS, LANES), f32),
        enter_out=pltpu.VMEM((CREW, GROUPS, *unit), bf16),
        enter_in=pltpu.VMEM((OWNERS, GROUPS, *unit), bf16),
        k_block=pltpu.VMEM((GROUPS, rows, 2 * LANES), bf16),
        q_block=pltpu.VMEM((GROUPS, rows, 2 * LANES), bf16),
        q_whole=pltpu.VMEM((GROUPS, rows, 2 * LANES), bf16),
        within=pltpu.VMEM((rows, valw), f32),
        branch_part=pltpu.VMEM((rows, width), f32),
        branch=pltpu.VMEM((rows, width), bf16),
    )
    for name, value in zip(NAMES, args):
        if name not in buffers:
            buffers[name] = pltpu.VMEM(value.shape, value.dtype)
    dma = pltpu.SemaphoreType.DMA
    semaphores = dict(
        load=dma((len(NAMES),)),
        part_send=dma((2, reducers)),
        part_recv=dma((2, crews, CORES)),
        total_send=dma((count,)),
        total_recv=dma((reducers * OWNERS,)),
        gate_send=dma((count,)),
        gate_recv=dma((reducers * OWNERS,)),
        ctx_send=dma((OWNERS,)),
        ctx_recv=dma((CREW,)),
        ctx_log_send=dma((OWNERS,)),
        ctx_log_recv=dma((CREW,)),
        log_send=dma((OWNERS,)),
        log_recv=dma((CREW,)),
        seg_send=dma((OWNERS,)),
        seg_recv=dma((CREW,)),
        ctx_crew_send=dma((crews,)),
        ctx_crew_recv=dma((crews,)),
        ctx_crew_log_send=dma((crews,)),
        ctx_crew_log_recv=dma((crews,)),
        crew_log_send=dma((crews,)),
        crew_log_recv=dma((crews,)),
        crew_send=dma((crews,)),
        crew_recv=dma((crews,)),
        enter_send=dma((2, CREW)),
        enter_recv=dma((2, OWNERS)),
    )
    return pl.pallas_call(
        functools.partial(block_kernel, sp_count, tp_count),
        out_shape=pltpu.VMEM((rows, width), bf16),
        in_specs=specs,
        out_specs=pl.BlockSpec(memory_space=pltpu.VMEM),
        scratch_shapes=[buffers, semaphores],
        compiler_params=pltpu.CompilerParams(
            collective_id=0, has_side_effects=True, vmem_limit_bytes=VMEM_LIMIT
        ),
        name="block",
    )(*args)


def solution(mesh):
    placed = (
        P(("sp", "tp"), None),
        P("sp", None),
        P(),
        P(),
        P("sp", "tp"),
        P("sp", "tp"),
        P("sp", "tp"),
        P(),
        P(),
        P(),
        P(),
        P(),
        P(),
        P(),
        P(),
        P(),
        P(),
    )
    return jax.shard_map(
        shards, mesh=mesh, in_specs=placed, out_specs=P(("sp", "tp"), None), check_vma=False
    )
```

```python
import functools
from types import SimpleNamespace

import jax
import jax.numpy as jnp
from jax import lax
from jax.experimental import pallas as pl
from jax.experimental.pallas import tpu as pltpu
from jax.sharding import PartitionSpec as P

HEADS = 16
DK = 32
DV = 64
LANES = 128
SUB = 8
GROUP = LANES // DK
GV = GROUP * DV
GROUPS = HEADS // GROUP
CREW = DV // SUB
CORES = 2
OWNERS = CREW // CORES
UNIT = DV // OWNERS
MESH = pl.DeviceIdType.MESH
TILE = 64
COLS = 256
STRIP = 16
VMEM_LIMIT = 60 * 1024 * 1024

NAMES = (
    "latent",
    "context",
    "latent_condition",
    "context_condition",
    "shift_weight",
    "scale_weight",
    "gate_weight",
    "norm_gain",
    "query_weight",
    "key_weight",
    "value_weight",
    "outgate_weight",
    "down_weight",
    "up_weight",
    "decay_bias",
    "out_weight",
    "post_gain",
)
FIRST = (
    "latent_condition",
    "context_condition",
    "shift_weight",
    "scale_weight",
    "gate_weight",
)
LATER = (
    "context",
    "latent",
    "down_weight",
    "norm_gain",
    "decay_bias",
    "post_gain",
    "up_weight",
    "key_weight",
    "value_weight",
    "query_weight",
    "outgate_weight",
    "out_weight",
)

epsilon = 1e-06
decay_temper = 16.0
f32 = jnp.float32
bf16 = jnp.bfloat16


def dot(a, b):
    return jnp.dot(a, b, preferred_element_type=f32)


def dot_nt(a, b):
    return lax.dot_general(a, b, (((1,), (1,)), ((), ())), preferred_element_type=f32)


def dot_tn(a, b):
    return lax.dot_general(a, b, (((0,), (0,)), ((), ())), preferred_element_type=f32)


def iota(shape, axis):
    return lax.broadcasted_iota(jnp.int32, shape, axis)


def lower_ones(rows):
    return jnp.where(iota((rows, rows), 0) >= iota((rows, rows), 1), 1.0, 0.0).astype(bf16)


def running_sum(lower, log_rows):
    high = log_rows.astype(bf16)
    rest = log_rows - high.astype(f32)
    return dot(lower, high) + dot(lower, rest.astype(bf16))


def log_decays(values):
    return (jnp.minimum(values, 0.0) - jnp.log(1.0 + jnp.exp(-jnp.abs(values)))) * (1.0 / decay_temper)


def rms_factor(values):
    return lax.rsqrt(jnp.mean(values * values, axis=-1, keepdims=True) + epsilon)


def per_head(full, head):
    out = full[(GROUP - 1) * DV :]
    for h in range(GROUP - 2, -1, -1):
        out = jnp.where(head == h, full[h * DV : (h + 1) * DV], out)
    return out


def stacked(values, head):
    zero = jnp.zeros_like(values)
    return jnp.concatenate([jnp.where(head == h, values, zero) for h in range(GROUP)], axis=0)


def reduction(chunks, crews):
    reducers = min(2, chunks, crews)
    return reducers, chunks // reducers


def block_kernel(sp_count, tp_count, *refs):
    hbm = SimpleNamespace(**dict(zip((*NAMES, "out"), refs)))
    vm = SimpleNamespace(**refs[-2])
    sem = SimpleNamespace(**refs[-1])

    count = sp_count * tp_count
    crews = count // CREW
    sp, tp = lax.axis_index("sp"), lax.axis_index("tp")
    me = sp * tp_count + tp
    crew, post = lax.div(me, CREW), lax.rem(me, CREW)
    chip, core = lax.div(post, CORES), lax.rem(post, CORES)
    rows, width = hbm.latent.shape
    blocks = rows // TILE
    row_share = hbm.shift_weight.shape[0]
    chunks = hbm.shift_weight.shape[1] // LANES
    reducers, share = reduction(chunks, crews)
    first_reducer = (crews - reducers) // 2
    owner = core == CORES - 1
    middle_crew = (crew >= first_reducer) & (crew < first_reducer + reducers)
    reducer = owner & middle_crew
    ctx_rows = vm.context.shape[0]
    ctx_group = lax.rem(tp, GROUPS)

    def place(flat):
        return (lax.div(flat, jnp.int32(tp_count)), lax.rem(flat, jnp.int32(tp_count)))

    def remote(src, dst, send, recv, flat):
        return pltpu.make_async_remote_copy(
            src_ref=src,
            dst_ref=dst,
            send_sem=send,
            recv_sem=recv,
            device_id=place(flat),
            device_id_type=MESH,
        )

    def others(body, total):
        def step(i, carry):
            body(i)
            return carry

        lax.fori_loop(1, total, step, 0)

    def mate(i):
        return lax.rem(post + i, CREW)

    def mates(body):
        for i in range(1, CREW):
            body(mate(i))

    def owners(body):
        for i in range(OWNERS):
            at = lax.rem(chip + i, OWNERS)
            if i == 0:
                pl.when(jnp.logical_not(owner))(functools.partial(body, at))
            else:
                body(at)

    def landed(ref, semaphore):
        remote(ref, ref, semaphore, semaphore, me).wait_recv()

    def gone(ref, semaphore):
        remote(ref, ref, semaphore, semaphore, me).wait_send()

    def by_role(body):
        pl.when(owner)(functools.partial(body, OWNERS - 1))
        pl.when(jnp.logical_not(owner))(functools.partial(body, OWNERS))

    def owner_of(at):
        return at * CORES + CORES - 1

    ctx_at = pl.multiple_of((tp // GROUPS) * ctx_rows, SUB)
    hbm.context = hbm.context.at[pl.ds(ctx_at, ctx_rows)]
    loads = {
        name: pltpu.make_async_copy(getattr(hbm, name), getattr(vm, name), sem.load.at[i])
        for i, name in enumerate(FIRST + LATER)
    }
    for name in FIRST:
        loads[name].start()

    barrier = pltpu.get_barrier_semaphore()

    def greet(flat):
        pl.semaphore_signal(barrier, inc=1, device_id=place(flat), device_id_type=MESH)

    for r in range(reducers):
        for q in range(OWNERS):
            flat = (first_reducer + r) * CREW + owner_of(q)

            @pl.when(flat != me)
            def _():
                greet(flat)

    @pl.when(reducer)
    def _():
        for c in range(crews):
            for k in range(CORES):
                if k < CORES - 1 or not first_reducer <= c < first_reducer + reducers:
                    greet(c * CREW + chip * CORES + k)

    loads["latent_condition"].wait()
    loads["context_condition"].wait()
    vm.cond[0:1, :] = vm.latent_condition[...].astype(f32).reshape(1, width)
    vm.cond[1:2, :] = vm.context_condition[...].astype(f32).reshape(1, width)
    mine = pl.ds(pl.multiple_of(sp * row_share, LANES), row_share)
    pick = iota((STRIP, row_share), 0) == 0
    raw = jnp.where(pick, vm.cond[0:1, mine], vm.cond[1:2, mine])
    cond = (raw / (1.0 + jnp.exp(-raw))).astype(bf16)
    loads["shift_weight"].wait()
    loads["scale_weight"].wait()
    for which, weight in enumerate((vm.shift_weight, vm.scale_weight)):
        part = dot(cond, weight[...])
        for c in range(chunks):
            at = slice(c * LANES, (c + 1) * LANES)
            r, row = c // share, c % share * 4 + which
            vm.part[r, row : row + 1, :] = part[0:1, at]
            vm.part[r, row + 2 : row + 3, :] = part[1:2, at]
    for name in LATER:
        loads[name].start()
    @pl.when(jnp.logical_not(reducer))
    def _():
        pl.semaphore_wait(barrier, reducers)

    home_core = (CORES - 1, 0)

    def to_reducer(r, c, k, which):
        part, parts = ((vm.part, vm.parts), (vm.gate_part, vm.gate_parts))[which]
        return remote(
            part.at[r],
            parts.at[c, k],
            sem.part_send.at[which, r],
            sem.part_recv.at[which, c, k],
            (first_reducer + r) * CREW + chip * CORES + home_core[which],
        )

    def elsewhere(r, which):
        return jnp.logical_not((core == home_core[which]) & (crew == first_reducer + r))

    def send_parts(which):
        for r in range(reducers):

            @pl.when(elsewhere(r, which))
            def _():
                to_reducer(r, crew, core, which).start()

    def early_part(r):
        return to_reducer(r, crew, 0, 0)

    for r in range(reducers):

        @pl.when(jnp.logical_not(elsewhere(r, 0)))
        def _():
            early_part(r).wait_recv()

    send_parts(0)
    loads["gate_weight"].wait()
    part = dot(cond, vm.gate_weight[...])
    for c in range(chunks):
        vm.gate_part[c // share, c % share] = part[0:1, c * LANES : (c + 1) * LANES]

    loads["context"].wait()
    xc = vm.context[...].astype(f32)
    vm.ctx_scaled[...] = xc * rms_factor(xc)
    loads["latent"].wait()

    def scale_strip(i, carry):
        at = pl.ds(pl.multiple_of(i * TILE, TILE), TILE)
        x = vm.latent[at, :].astype(f32)
        vm.scaled[at, :] = x * rms_factor(x)
        return carry

    lax.fori_loop(0, rows // TILE, scale_strip, 0)
    loads["down_weight"].wait()
    vm.down[...] = vm.down_weight[...].T

    reduced = reducers * OWNERS

    def spread(flat, slot):
        return remote(vm.total, vm.totals.at[slot], sem.total_send.at[0], sem.total_recv.at[0], flat)

    def gate_spread(flat, slot):
        return remote(
            vm.gate_total, vm.gate_totals.at[slot], sem.gate_send.at[0], sem.gate_recv.at[0], flat
        )

    def reduce_here(which, mine, held, total, totals, copy):
        for r in range(reducers):
            home = first_reducer + r

            @pl.when((core == home_core[which]) & (crew == home))
            def _():
                slot = r * OWNERS + chip
                for k in range(CORES):
                    out = None
                    for c in range(crews):
                        if c == home and k == home_core[which]:
                            term = mine[r]
                        else:
                            if which == 1 or c != home or k != 0:
                                to_reducer(r, c, k, which).wait_recv()
                            term = held[c, k]
                        out = term if out is None else out + term
                    total[k] = out
                    totals[slot, k] = out
                for c in sorted(range(crews), key=lambda c: -abs(c - home)):

                    def send(i, carry):
                        copy(c * CREW + mate(i), slot).start()
                        return carry

                    lax.fori_loop(0 if c != home else 1, CREW, send, 0)

    def reduces(which):
        return (core == home_core[which]) & middle_crew

    def arrivals(which, totals, semaphore):
        @pl.when(reduces(which))
        def _():
            landed(totals.at[pl.ds(0, reduced - 1)], semaphore)

        @pl.when(jnp.logical_not(reduces(which)))
        def _():
            landed(totals, semaphore)

    def sent(which, credit, semaphore):
        @pl.when(reduces(which))
        def _():
            gone(credit, semaphore)

    @pl.when(reducer)
    def _():
        pl.semaphore_wait(barrier, count - 1)

    reduce_here(0, vm.part, vm.parts, vm.total, vm.totals, spread)
    loads_needed = ("norm_gain", "decay_bias", "post_gain", "up_weight", "key_weight")
    for name in loads_needed + ("value_weight",):
        loads[name].wait()
    arrivals(0, vm.totals, sem.total_recv.at[0])
    def summed(totals, r, t):
        out = None
        for p in range(t, CREW, tp_count):
            term = totals[r * OWNERS + p // CORES, p % CORES]
            out = term if out is None else out + term
        return out

    for r in range(reducers):
        for t in range(tp_count):
            tile = summed(vm.totals, r, t)
            for s in range(share):
                at = (t * chunks + r * share + s) * LANES
                vm.mods[0:4, at : at + LANES] = tile[s * 4 : s * 4 + 4]

    gain = vm.norm_gain[...] * (1.0 + vm.mods[3:4, :])
    ctx_normed = (vm.ctx_scaled[...] * gain + vm.mods[2:3, :]).astype(bf16)
    head_k = iota((DV, 2 * LANES), 1) % LANES // DK
    key_at = pl.ds(pl.multiple_of(ctx_group * LANES, LANES), LANES)
    val_at = pl.ds(pl.multiple_of(ctx_group * GV, GV), GV)
    low = dot(ctx_normed, vm.down[...]).astype(bf16)
    log_rows = log_decays(dot(low, vm.up_weight[:, key_at]) + vm.decay_bias[:, key_at])
    keys = dot(ctx_normed, vm.key_weight[:, key_at]).astype(bf16).astype(f32)
    values = dot(ctx_normed, vm.value_weight[:, val_at]).astype(bf16)
    inclusive = running_sum(lower_ones(ctx_rows), log_rows)
    closing = inclusive[ctx_rows - 1 : ctx_rows, :]
    both = jnp.concatenate(
        [keys * jnp.exp(closing - inclusive), keys * jnp.exp(inclusive - log_rows)], axis=1
    ).astype(bf16)
    state = per_head(dot_tn(values, both), head_k)
    for j in range(OWNERS):
        at = slice(j * UNIT, (j + 1) * UNIT)
        vm.ctx_out[j] = jnp.concatenate([state[at, :LANES], state[at, LANES:]], axis=0).astype(bf16)
    vm.ctx_log[...] = closing

    def ctx_copies(o, p):
        flat = crew * CREW + owner_of(o)
        return (
            remote(vm.ctx_out.at[o], vm.ctx_in.at[p], sem.ctx_send.at[0], sem.ctx_recv.at[0], flat),
            remote(vm.ctx_log, vm.ctx_logs.at[p], sem.ctx_log_send.at[0], sem.ctx_log_recv.at[0], flat),
        )

    def ctx_start(o):
        for copy in ctx_copies(o, post):
            copy.start()

    owners(ctx_start)

    gain = vm.norm_gain[...] * (1.0 + vm.mods[1:2, :])
    shift = vm.mods[0:1, :]
    for i in range(rows // STRIP):
        at = slice(i * STRIP, (i + 1) * STRIP)
        vm.normed[at, :] = (vm.scaled[at, :] * gain + shift).astype(bf16)

    def project(weight, out):
        for n in range(0, weight.shape[1], COLS):
            at = slice(n, n + COLS)
            out[:, at] = dot(vm.normed[...], weight[:, at]).astype(bf16)

    def project_tile(weight, out, n):
        at = slice(n, min(n + COLS, weight.shape[1]))
        out[:, at] = dot(vm.normed[...], weight[:, at]).astype(bf16)

    tiles = [(vm.key_weight, vm.key, n) for n in range(0, vm.key_weight.shape[1], COLS)]
    tiles += [(vm.value_weight, vm.value, n) for n in range(0, vm.value_weight.shape[1], COLS)]
    low = dot(vm.normed[...], vm.down[...]).astype(bf16)
    project_tile(*tiles.pop(0))
    lower = lower_ones(TILE)
    offset = None
    for b in range(blocks):
        at = slice(b * TILE, (b + 1) * TILE)
        log_rows = log_decays(dot(low[at], vm.up_weight[...]) + vm.decay_bias[...])
        inclusive = running_sum(lower, log_rows)
        end = inclusive[TILE - 1 : TILE, :]
        vm.inclusive[at, :] = inclusive
        vm.before[at, :] = inclusive - log_rows
        vm.closing[b : b + 1, :] = end
        vm.offset[b : b + 1, :] = jnp.zeros_like(end) if offset is None else offset
        offset = end if offset is None else offset + end
        if tiles:
            project_tile(*tiles.pop(0))
    vm.offset[blocks : blocks + 1, :] = offset
    for g in range(GROUPS):
        vm.log_out[g : g + 1, :] = offset[:, g * LANES : (g + 1) * LANES]
    while tiles:
        project_tile(*tiles.pop(0))

    send_parts(1)

    def log_copy(o, p):
        return remote(
            vm.log_out, vm.logs.at[p], sem.log_send.at[0], sem.log_recv.at[0], crew * CREW + owner_of(o)
        )

    def early_copies(o, p):
        return (*ctx_copies(o, p), log_copy(o, p))

    owners(lambda o: log_copy(o, post).start())

    @pl.when(owner)
    def _():
        vm.ctx_in[post] = vm.ctx_out[chip]
        vm.ctx_logs[post] = vm.ctx_log[...]
        vm.logs[post] = vm.log_out[...]

    def seg_copy(o, p, g):
        return remote(
            vm.seg_out.at[o, g],
            vm.seg_in.at[p, g],
            sem.seg_send.at[0],
            sem.seg_recv.at[0],
            crew * CREW + owner_of(o),
        )

    for g in range(GROUPS):
        lanes = slice(g * LANES, (g + 1) * LANES)
        v_lanes = slice(g * GV, (g + 1) * GV)
        whole = vm.offset[blocks : blocks + 1, lanes]
        both = []
        for b in range(blocks):
            at = slice(b * TILE, (b + 1) * TILE)
            keys = vm.key[at, lanes].astype(f32)
            start, closing = vm.offset[b : b + 1, lanes], vm.closing[b : b + 1, lanes]
            ahead = keys * jnp.exp(closing - vm.inclusive[at, lanes])
            behind = keys * jnp.exp(vm.before[at, lanes])
            vm.k_block[g, at, :] = jnp.concatenate([ahead, behind], axis=1).astype(bf16)
            both.append(
                jnp.concatenate(
                    [ahead * jnp.exp((whole - start) - closing), behind * jnp.exp(start)], axis=1
                ).astype(bf16)
            )
        state = per_head(dot_tn(vm.value[:, v_lanes], jnp.concatenate(both, axis=0)), head_k)
        for j in range(OWNERS):
            at = slice(j * UNIT, (j + 1) * UNIT)
            vm.seg_out[j, g] = jnp.concatenate([state[at, :LANES], state[at, LANES:]], axis=0).astype(bf16)
        owners(lambda o: seg_copy(o, post, g).start())

    @pl.when(owner)
    def _():
        vm.seg_in[post] = vm.seg_out[chip]

    def ctx_crew_copies(c, slot):
        flat = c * CREW + post
        return (
            remote(
                vm.ctx_crews_out,
                vm.ctx_crews.at[slot],
                sem.ctx_crew_send.at[0],
                sem.ctx_crew_recv.at[0],
                flat,
            ),
            remote(
                vm.ctx_crews_log,
                vm.ctx_crews_logs.at[slot],
                sem.ctx_crew_log_send.at[0],
                sem.ctx_crew_log_recv.at[0],
                flat,
            ),
        )

    @pl.when(owner)
    def _():
        landed(vm.ctx_in.at[pl.ds(0, CREW - 1)], sem.ctx_recv.at[0])
        landed(vm.ctx_logs.at[pl.ds(0, CREW - 1)], sem.ctx_log_recv.at[0])
        for g in range(GROUPS):
            posts = list(range(g, CREW, GROUPS))
            logs = [vm.ctx_logs[p] for p in posts]
            tiles = [vm.ctx_in[p].astype(f32) for p in posts]
            forward, backward, log_sum = tiles[0][:UNIT], tiles[-1][UNIT:], logs[0]
            for i in range(1, len(posts)):
                forward = jnp.exp(logs[i]) * forward + tiles[i][:UNIT]
                backward = jnp.exp(logs[-1 - i]) * backward + tiles[-1 - i][UNIT:]
                log_sum = log_sum + logs[i]
            vm.ctx_crews_out[g] = jnp.concatenate([forward, backward], axis=0).astype(bf16)
            vm.ctx_crews_log[g : g + 1, :] = log_sum

        def ctx_crew_start(i):
            for copy in ctx_crew_copies(lax.rem(crew + i, crews), crew):
                copy.start()

        others(ctx_crew_start, crews)
        vm.ctx_crews[crew] = vm.ctx_crews_out[...]
        vm.ctx_crews_logs[crew] = vm.ctx_crews_log[...]

    head_k1 = iota((TILE, LANES), 1) // DK
    head_v = iota((TILE, GV), 1) // DV
    t_index = iota((TILE, GROUP * TILE), 0)
    s_index = iota((TILE, GROUP * TILE), 1) % TILE

    def inside(g):
        lanes = slice(g * LANES, (g + 1) * LANES)
        v_lanes = slice(g * GV, (g + 1) * GV)
        whole = vm.offset[blocks : blocks + 1, lanes]
        for b in range(blocks):
            at = slice(b * TILE, (b + 1) * TILE)
            inclusive, before = vm.inclusive[at, lanes], vm.before[at, lanes]
            start = vm.offset[b : b + 1, lanes]
            closing = inclusive[TILE - 1 : TILE, :]
            middle = inclusive[TILE // 2 - 1 : TILE // 2, :]
            queries = vm.query[at, lanes].astype(f32) * DK ** (-0.5)
            keys = vm.key[at, lanes].astype(f32)
            scores = []
            for q_log, k_log in (
                (inclusive - middle, middle - inclusive),
                (middle - before, before - middle),
            ):
                k_stack = stacked((keys * jnp.exp(k_log)).astype(bf16), head_k1)
                scores.append(dot_nt((queries * jnp.exp(q_log)).astype(bf16), k_stack))
            both = jnp.where(t_index >= s_index, scores[0], 0.0) + jnp.where(
                t_index <= s_index, scores[1], 0.0
            )
            v_stack = stacked(vm.value[at, v_lanes], head_v)
            vm.within[at, v_lanes] = dot(both.astype(bf16), v_stack)
            ahead = queries * jnp.exp(inclusive)
            behind = queries * jnp.exp(closing - before)
            vm.q_block[g, at, :] = jnp.concatenate([ahead, behind], axis=1).astype(bf16)
            vm.q_whole[g, at, :] = jnp.concatenate(
                [ahead * jnp.exp(start), behind * jnp.exp((whole - start) - closing)], axis=1
            ).astype(bf16)

    def between(g):
        lanes = slice(g * LANES, (g + 1) * LANES)
        v_lanes = slice(g * GV, (g + 1) * GV)
        decays = [jnp.exp(vm.closing[b : b + 1, lanes]) for b in range(blocks)]
        left = []
        for b in range(blocks):
            at = slice(b * TILE, (b + 1) * TILE)
            left.append(per_head(dot_tn(vm.value[at, v_lanes], vm.k_block[g, at, :]), head_k))
        forward = [jnp.zeros((DV, LANES), f32)]
        backward = [jnp.zeros((DV, LANES), f32)]
        for b in range(blocks - 1):
            forward.append(decays[b] * forward[b] + left[b][:, :LANES])
            back = blocks - 1 - b
            backward.insert(0, decays[back] * backward[0] + left[back][:, LANES:])
        for b in range(blocks):
            at = slice(b * TILE, (b + 1) * TILE)
            states = jnp.concatenate([forward[b], backward[b]], axis=1)
            across = dot_nt(vm.q_block[g, at, :], stacked(states, head_k).astype(bf16))
            vm.within[at, v_lanes] = vm.within[at, v_lanes] + across

    loads["query_weight"].wait()
    project(vm.query_weight, vm.query)
    inside(0)

    def crew_log_copy(c, slot):
        return remote(
            vm.crew_log,
            vm.crew_logs.at[slot],
            sem.crew_log_send.at[0],
            sem.crew_log_recv.at[0],
            c * CREW + post,
        )

    @pl.when(owner)
    def _():
        landed(vm.logs.at[pl.ds(0, CREW - 1)], sem.log_recv.at[0])
        vm.decay[...] = jnp.exp(vm.logs[...])
        crew_log = vm.logs[0]
        for p in range(1, CREW):
            crew_log = crew_log + vm.logs[p]
        vm.crew_log[...] = crew_log
        others(lambda i: crew_log_copy(lax.rem(crew + i, crews), crew).start(), crews)

    inside(1)

    reduce_here(1, vm.gate_part, vm.gate_parts, vm.gate_total, vm.gate_totals, gate_spread)

    def crew_copy(c, slot, side):
        return remote(
            vm.crew_out.at[side],
            vm.crew_in.at[slot],
            sem.crew_send.at[0],
            sem.crew_recv.at[0],
            c * CREW + post,
        )

    def post_decay(p, g):
        return vm.decay[p, g : g + 1, :]

    @pl.when(owner)
    def _():
        landed(vm.seg_in.at[pl.ds(0, CREW - 1)], sem.seg_recv.at[0])
        for g in range(GROUPS):
            at = slice(g * UNIT, (g + 1) * UNIT)
            forward = vm.seg_in[0, g, :UNIT].astype(f32)
            for p in range(1, CREW):
                forward = post_decay(p, g) * forward + vm.seg_in[p, g, :UNIT].astype(f32)
            backward = vm.seg_in[CREW - 1, g, UNIT:].astype(f32)
            for p in range(CREW - 2, -1, -1):
                backward = post_decay(p, g) * backward + vm.seg_in[p, g, UNIT:].astype(f32)
            vm.crew_out[0, at, :] = forward.astype(bf16)
            vm.crew_out[1, at, :] = backward.astype(bf16)

        def crew_start(i):
            ahead, behind = crews - i, i - 1

            @pl.when(ahead > crew)
            def _():
                crew_copy(ahead, crew, 0).start()

            @pl.when(behind < crew)
            def _():
                crew_copy(behind, crew, 1).start()

        others(crew_start, crews)

    for g in range(2, GROUPS):
        inside(g)
    for g in range(GROUPS - 2):
        between(g)

    half = GROUPS // 2

    def enter_copy(p, o, h):
        part = pl.ds(h * half, half)
        return remote(
            vm.enter_out.at[p, part],
            vm.enter_in.at[o, part],
            sem.enter_send.at[0],
            sem.enter_recv.at[h],
            crew * CREW + p,
        )

    @pl.when(owner)
    def _():
        away = pl.ds(0, crews - 1)
        landed(vm.ctx_crews.at[away], sem.ctx_crew_recv.at[0])
        landed(vm.ctx_crews_logs.at[away], sem.ctx_crew_log_recv.at[0])
        landed(vm.crew_logs.at[away], sem.crew_log_recv.at[0])
        vm.crew_decay[...] = jnp.exp(vm.crew_logs[...])
        vm.ctx_decay[...] = jnp.exp(vm.ctx_crews_logs[...])
        zero = jnp.zeros((UNIT, LANES), f32)
        forward, backward = [zero] * GROUPS, [zero] * GROUPS
        for a in range(crews):
            z = crews - 1 - a
            for g in range(GROUPS):
                forward[g] = (
                    vm.ctx_decay[a, g : g + 1, :] * forward[g]
                    + vm.ctx_crews[a, g, :UNIT].astype(f32)
                )
                backward[g] = (
                    vm.ctx_decay[z, g : g + 1, :] * backward[g]
                    + vm.ctx_crews[z, g, UNIT:].astype(f32)
                )

        def step_states(c, states):
            left = vm.crew_in[c].astype(f32)
            return tuple(
                vm.crew_decay[c, g : g + 1, :] * states[g] + left[g * UNIT : (g + 1) * UNIT]
                for g in range(GROUPS)
            )

        def from_after(i, states):
            return step_states(crews - 1 - i, states)

        landed(vm.crew_in.at[away], sem.crew_recv.at[0])
        forward = lax.fori_loop(0, crew, step_states, tuple(forward))
        backward = lax.fori_loop(0, crews - 1 - crew, from_after, tuple(backward))
        for g in range(GROUPS):
            state = forward[g]
            for p in range(CREW):
                vm.enter_out[p, g, :UNIT] = state.astype(bf16)
                if p < CREW - 1:
                    state = post_decay(p, g) * state + vm.seg_in[p, g, :UNIT].astype(f32)
            state = backward[g]
            for p in range(CREW - 1, -1, -1):
                vm.enter_out[p, g, UNIT:] = state.astype(bf16)
                if p > 0:
                    state = post_decay(p, g) * state + vm.seg_in[p, g, UNIT:].astype(f32)
            if g % half == half - 1:
                mates(lambda p: enter_copy(p, chip, g // half).start())
        vm.enter_in[chip] = vm.enter_out[post]

    loads["outgate_weight"].wait()
    for n in range(0, vm.outgate_weight.shape[1], COLS):
        at = slice(n, n + COLS)
        gate = dot(vm.normed[...], vm.outgate_weight[:, at]).astype(bf16).astype(f32)
        vm.silu[:, at] = gate / (1.0 + jnp.exp(-gate))
    for g in range(GROUPS - 2, GROUPS):
        between(g)
    head_mean = jnp.where(iota((GV, GV), 0) // DV == iota((GV, GV), 1) // DV, 1.0 / DV, 0.0).astype(bf16)

    arrivals(1, vm.gate_totals, sem.gate_recv.at[0])
    for r in range(reducers):
        for t in range(tp_count):
            tile = summed(vm.gate_totals, r, t)
            for s in range(share):
                at = (t * chunks + r * share + s) * LANES
                vm.mods[4:5, at : at + LANES] = tile[s]
    loads["out_weight"].wait()

    for which in range(2):
        for r in range(reducers):

            @pl.when(elsewhere(r, which))
            def _():
                to_reducer(r, crew, core, which).wait_send()

    sent(0, vm.credit, sem.total_send.at[0])
    sent(1, vm.gate_credit, sem.gate_send.at[0])

    def to_owners_sent(n):
        gone(vm.ctx_out.at[pl.ds(0, n)], sem.ctx_send.at[0])
        gone(vm.ctx_logs.at[pl.ds(0, n)], sem.ctx_log_send.at[0])
        gone(vm.logs.at[pl.ds(0, n)], sem.log_send.at[0])
        gone(vm.seg_out.at[pl.ds(0, n)], sem.seg_send.at[0])

    by_role(to_owners_sent)

    @pl.when(owner)
    def _():
        away = pl.ds(0, crews - 1)
        gone(vm.ctx_crews.at[away], sem.ctx_crew_send.at[0])
        gone(vm.ctx_crews_logs.at[away], sem.ctx_crew_log_send.at[0])
        gone(vm.crew_logs.at[away], sem.crew_log_send.at[0])
        gone(vm.crew_in.at[away], sem.crew_send.at[0])

    def finish(g):
        v_lanes = slice(g * GV, (g + 1) * GV)
        states = jnp.concatenate(
            [
                jnp.concatenate([vm.enter_in[o, g, :UNIT] for o in range(OWNERS)], axis=0),
                jnp.concatenate([vm.enter_in[o, g, UNIT:] for o in range(OWNERS)], axis=0),
            ],
            axis=1,
        )
        across = dot_nt(vm.q_whole[g], stacked(states, head_k))
        mixed = vm.within[:, v_lanes] + across
        mean = dot((mixed * mixed).astype(bf16), head_mean)
        vm.gated[:, v_lanes] = (mixed * lax.rsqrt(mean + epsilon) * vm.silu[:, v_lanes]).astype(bf16)

    def entered(h):
        part = pl.ds(h * half, half)
        by_role(lambda n: landed(vm.enter_in.at[pl.ds(0, n), part], sem.enter_recv.at[h]))

    depth = half * GV
    entered(0)
    for g in range(half):
        finish(g)
    for n in range(0, width, COLS):
        at = slice(n, n + COLS)
        vm.branch_part[:, at] = dot(vm.gated[:, :depth], vm.out_weight[:depth, at])
    entered(1)
    for g in range(half, GROUPS):
        finish(g)

    square = jnp.zeros((rows, LANES), f32)
    for n in range(0, width, COLS):
        at = slice(n, n + COLS)
        branch = (vm.branch_part[:, at] + dot(vm.gated[:, depth:], vm.out_weight[depth:, at])).astype(bf16)
        vm.branch[:, at] = branch
        branch = branch.astype(f32)
        branch = branch * branch
        for s in range(0, COLS, LANES):
            square = square + branch[:, s : s + LANES]
    factor = lax.rsqrt(jnp.sum(square, axis=1, keepdims=True) / width + epsilon)
    gain = vm.mods[4:5, :] * vm.post_gain[...]
    for i in range(rows // STRIP):
        at = slice(i * STRIP, (i + 1) * STRIP)
        hbm.out[at, :] = (
            vm.latent[at, :].astype(f32) + gain * (vm.branch[at, :].astype(f32) * factor[at])
        ).astype(bf16)

    @pl.when(owner)
    def _():
        gone(vm.enter_out.at[pl.ds(0, CREW - 1)], sem.enter_send.at[0])


def shards(*operands):
    values = dict(zip(NAMES, operands))
    values["down_weight"] = values["down_weight"].T
    latent, context = values["latent"], values["context"]
    sp_count, tp_count = lax.axis_size("sp"), lax.axis_size("tp")
    count = sp_count * tp_count
    crews = count // CREW
    rows, width = latent.shape
    args, specs = [], []
    for name, value in values.items():
        vector = value.ndim == 1
        args.append(value.reshape(1, -1) if vector and value.dtype == f32 else value)
        specs.append(pl.BlockSpec(memory_space=pltpu.HBM))
    ctx_rows = context.shape[0] * GROUPS // tp_count
    chunks = values["shift_weight"].shape[1] // LANES
    reducers, share = reduction(chunks, crews)
    part_rows = -(-4 * share // SUB) * SUB
    keyw, valw = values["key_weight"].shape[1], values["value_weight"].shape[1]
    blocks = rows // TILE
    unit = (2 * UNIT, LANES)
    buffers = dict(
        context=pltpu.VMEM((ctx_rows, width), bf16),
        credit=pltpu.VMEM((count - 1, CORES, part_rows, LANES), f32),
        gate_credit=pltpu.VMEM((count - 1, CORES, share, 1, LANES), f32),
        cond=pltpu.VMEM((SUB, width), f32),
        part=pltpu.VMEM((reducers, part_rows, LANES), f32),
        parts=pltpu.VMEM((crews, CORES, part_rows, LANES), f32),
        total=pltpu.VMEM((CORES, part_rows, LANES), f32),
        totals=pltpu.VMEM((reducers * OWNERS, CORES, part_rows, LANES), f32),
        gate_part=pltpu.VMEM((reducers, share, 1, LANES), f32),
        gate_parts=pltpu.VMEM((crews, CORES, share, 1, LANES), f32),
        gate_total=pltpu.VMEM((CORES, share, 1, LANES), f32),
        gate_totals=pltpu.VMEM((reducers * OWNERS, CORES, share, 1, LANES), f32),
        mods=pltpu.VMEM((SUB, width), f32),
        scaled=pltpu.VMEM((rows, width), f32),
        down=pltpu.VMEM((width, values["down_weight"].shape[0]), bf16),
        ctx_scaled=pltpu.VMEM((ctx_rows, width), f32),
        normed=pltpu.VMEM((rows, width), bf16),
        ctx_out=pltpu.VMEM((OWNERS, *unit), bf16),
        ctx_in=pltpu.VMEM((CREW, *unit), bf16),
        ctx_log=pltpu.VMEM((1, LANES), f32),
        ctx_logs=pltpu.VMEM((CREW, 1, LANES), f32),
        ctx_crews_out=pltpu.VMEM((GROUPS, *unit), bf16),
        ctx_crews=pltpu.VMEM((crews, GROUPS, *unit), bf16),
        key=pltpu.VMEM((rows, keyw), bf16),
        query=pltpu.VMEM((rows, keyw), bf16),
        value=pltpu.VMEM((rows, valw), bf16),
        silu=pltpu.VMEM((rows, valw), f32),
        gated=pltpu.VMEM((rows, valw), bf16),
        inclusive=pltpu.VMEM((rows, keyw), f32),
        before=pltpu.VMEM((rows, keyw), f32),
        closing=pltpu.VMEM((blocks, keyw), f32),
        offset=pltpu.VMEM((blocks + 1, keyw), f32),
        log_out=pltpu.VMEM((GROUPS, LANES), f32),
        logs=pltpu.VMEM((CREW, GROUPS, LANES), f32),
        decay=pltpu.VMEM((CREW, GROUPS, LANES), f32),
        crew_decay=pltpu.VMEM((crews, GROUPS, LANES), f32),
        ctx_decay=pltpu.VMEM((crews, GROUPS, LANES), f32),
        ctx_crews_log=pltpu.VMEM((GROUPS, LANES), f32),
        ctx_crews_logs=pltpu.VMEM((crews, GROUPS, LANES), f32),
        seg_out=pltpu.VMEM((OWNERS, GROUPS, *unit), bf16),
        seg_in=pltpu.VMEM((CREW, GROUPS, *unit), bf16),
        crew_out=pltpu.VMEM((2, GROUPS * UNIT, LANES), bf16),
        crew_in=pltpu.VMEM((crews, GROUPS * UNIT, LANES), bf16),
        crew_log=pltpu.VMEM((GROUPS, LANES), f32),
        crew_logs=pltpu.VMEM((crews, GROUPS, LANES), f32),
        enter_out=pltpu.VMEM((CREW, GROUPS, *unit), bf16),
        enter_in=pltpu.VMEM((OWNERS, GROUPS, *unit), bf16),
        k_block=pltpu.VMEM((GROUPS, rows, 2 * LANES), bf16),
        q_block=pltpu.VMEM((GROUPS, rows, 2 * LANES), bf16),
        q_whole=pltpu.VMEM((GROUPS, rows, 2 * LANES), bf16),
        within=pltpu.VMEM((rows, valw), f32),
        branch_part=pltpu.VMEM((rows, width), f32),
        branch=pltpu.VMEM((rows, width), bf16),
    )
    for name, value in zip(NAMES, args):
        if name not in buffers:
            buffers[name] = pltpu.VMEM(value.shape, value.dtype)
    dma = pltpu.SemaphoreType.DMA
    semaphores = dict(
        load=dma((len(NAMES),)),
        part_send=dma((2, reducers)),
        part_recv=dma((2, crews, CORES)),
        total_send=dma((1,)),
        total_recv=dma((1,)),
        gate_send=dma((1,)),
        gate_recv=dma((1,)),
        ctx_send=dma((1,)),
        ctx_recv=dma((1,)),
        ctx_log_send=dma((1,)),
        ctx_log_recv=dma((1,)),
        log_send=dma((1,)),
        log_recv=dma((1,)),
        seg_send=dma((1,)),
        seg_recv=dma((1,)),
        ctx_crew_send=dma((1,)),
        ctx_crew_recv=dma((1,)),
        ctx_crew_log_send=dma((1,)),
        ctx_crew_log_recv=dma((1,)),
        crew_log_send=dma((1,)),
        crew_log_recv=dma((1,)),
        crew_send=dma((1,)),
        crew_recv=dma((1,)),
        enter_send=dma((1,)),
        enter_recv=dma((2,)),
    )
    return pl.pallas_call(
        functools.partial(block_kernel, sp_count, tp_count),
        out_shape=pltpu.VMEM((rows, width), bf16),
        in_specs=specs,
        out_specs=pl.BlockSpec(memory_space=pltpu.VMEM),
        scratch_shapes=[buffers, semaphores],
        compiler_params=pltpu.CompilerParams(
            collective_id=0, has_side_effects=True, vmem_limit_bytes=VMEM_LIMIT
        ),
        name="block",
    )(*args)


def solution(mesh):
    placed = (
        P(("sp", "tp"), None),
        P("sp", None),
        P(),
        P(),
        P("sp", "tp"),
        P("sp", "tp"),
        P("sp", "tp"),
        P(),
        P(),
        P(),
        P(),
        P(),
        P(),
        P(),
        P(),
        P(),
        P(),
    )
    return jax.shard_map(
        shards, mesh=mesh, in_specs=placed, out_specs=P(("sp", "tp"), None), check_vma=False
    )
```

```python
import functools
from types import SimpleNamespace

import jax
import jax.numpy as jnp
from jax import lax
from jax.experimental import pallas as pl
from jax.experimental.pallas import tpu as pltpu
from jax.sharding import PartitionSpec as P

HEADS = 16
DK = 32
DV = 64
LANES = 128
SUB = 8
GROUP = LANES // DK
GV = GROUP * DV
GROUPS = HEADS // GROUP
CREW = DV // SUB
CORES = 2
OWNERS = CREW // CORES
UNIT = DV // OWNERS
MESH = pl.DeviceIdType.MESH
TILE = 64
COLS = 256
STRIP = 16
VMEM_LIMIT = 60 * 1024 * 1024

NAMES = (
    "latent",
    "context",
    "latent_condition",
    "context_condition",
    "shift_weight",
    "scale_weight",
    "gate_weight",
    "norm_gain",
    "query_weight",
    "key_weight",
    "value_weight",
    "outgate_weight",
    "down_weight",
    "up_weight",
    "decay_bias",
    "out_weight",
    "post_gain",
)
FIRST = (
    "latent_condition",
    "context_condition",
    "shift_weight",
    "scale_weight",
    "gate_weight",
)
LATER = (
    "context",
    "latent",
    "down_weight",
    "norm_gain",
    "decay_bias",
    "post_gain",
    "up_weight",
    "key_weight",
    "value_weight",
    "query_weight",
    "outgate_weight",
    "out_weight",
)

epsilon = 1e-06
decay_temper = 16.0
f32 = jnp.float32
bf16 = jnp.bfloat16


def dot(a, b):
    return jnp.dot(a, b, preferred_element_type=f32)


def dot_nt(a, b):
    return lax.dot_general(a, b, (((1,), (1,)), ((), ())), preferred_element_type=f32)


def dot_tn(a, b):
    return lax.dot_general(a, b, (((0,), (0,)), ((), ())), preferred_element_type=f32)


def iota(shape, axis):
    return lax.broadcasted_iota(jnp.int32, shape, axis)


def lower_ones(rows):
    return jnp.where(iota((rows, rows), 0) >= iota((rows, rows), 1), 1.0, 0.0).astype(bf16)


def running_sum(lower, log_rows):
    high = log_rows.astype(bf16)
    rest = log_rows - high.astype(f32)
    return dot(lower, high) + dot(lower, rest.astype(bf16))


def log_decays(values):
    return (jnp.minimum(values, 0.0) - jnp.log(1.0 + jnp.exp(-jnp.abs(values)))) * (1.0 / decay_temper)


def rms_factor(values):
    return lax.rsqrt(jnp.mean(values * values, axis=-1, keepdims=True) + epsilon)


def per_head(full, head):
    out = full[(GROUP - 1) * DV :]
    for h in range(GROUP - 2, -1, -1):
        out = jnp.where(head == h, full[h * DV : (h + 1) * DV], out)
    return out


def stacked(values, head):
    zero = jnp.zeros_like(values)
    return jnp.concatenate([jnp.where(head == h, values, zero) for h in range(GROUP)], axis=0)


def reduction(chunks, crews):
    reducers = min(2, chunks, crews)
    return reducers, chunks // reducers


def block_kernel(sp_count, tp_count, *refs):
    hbm = SimpleNamespace(**dict(zip((*NAMES, "out"), refs)))
    vm = SimpleNamespace(**refs[-2])
    sem = SimpleNamespace(**refs[-1])

    count = sp_count * tp_count
    crews = count // CREW
    sp, tp = lax.axis_index("sp"), lax.axis_index("tp")
    me = sp * tp_count + tp
    crew, post = lax.div(me, CREW), lax.rem(me, CREW)
    chip, core = lax.div(post, CORES), lax.rem(post, CORES)
    rows, width = hbm.latent.shape
    blocks = rows // TILE
    row_share = hbm.shift_weight.shape[0]
    chunks = hbm.shift_weight.shape[1] // LANES
    reducers, share = reduction(chunks, crews)
    first_reducer = (crews - reducers) // 2
    owner = core == CORES - 1
    middle_crew = (crew >= first_reducer) & (crew < first_reducer + reducers)
    reducer = owner & middle_crew
    ctx_rows = vm.context.shape[0]
    ctx_group = lax.rem(tp, GROUPS)

    def place(flat):
        return (lax.div(flat, jnp.int32(tp_count)), lax.rem(flat, jnp.int32(tp_count)))

    def remote(src, dst, send, recv, flat):
        return pltpu.make_async_remote_copy(
            src_ref=src,
            dst_ref=dst,
            send_sem=send,
            recv_sem=recv,
            device_id=place(flat),
            device_id_type=MESH,
        )

    def others(body, total):
        def step(i, carry):
            body(i)
            return carry

        lax.fori_loop(1, total, step, 0)

    def mate(i):
        return lax.rem(post + i, CREW)

    def mates(body):
        for i in range(1, CREW):
            body(mate(i))

    def owners(body):
        for i in range(OWNERS):
            at = lax.rem(chip + i, OWNERS)
            if i == 0:
                pl.when(jnp.logical_not(owner))(functools.partial(body, at))
            else:
                body(at)

    def landed(ref, semaphore):
        remote(ref, ref, semaphore, semaphore, me).wait_recv()

    def gone(ref, semaphore):
        remote(ref, ref, semaphore, semaphore, me).wait_send()

    def by_role(body):
        pl.when(owner)(functools.partial(body, OWNERS - 1))
        pl.when(jnp.logical_not(owner))(functools.partial(body, OWNERS))

    def owner_of(at):
        return at * CORES + CORES - 1

    ctx_at = pl.multiple_of((tp // GROUPS) * ctx_rows, SUB)
    hbm.context = hbm.context.at[pl.ds(ctx_at, ctx_rows)]
    loads = {
        name: pltpu.make_async_copy(getattr(hbm, name), getattr(vm, name), sem.load.at[i])
        for i, name in enumerate(FIRST + LATER)
    }
    for name in FIRST:
        loads[name].start()

    barrier = pltpu.get_barrier_semaphore()

    def greet(flat):
        pl.semaphore_signal(barrier, inc=1, device_id=place(flat), device_id_type=MESH)

    for r in range(reducers):
        for q in range(OWNERS):
            flat = (first_reducer + r) * CREW + owner_of(q)

            @pl.when(flat != me)
            def _():
                greet(flat)

    @pl.when(reducer)
    def _():
        for c in range(crews):
            for k in range(CORES):
                if k < CORES - 1 or not first_reducer <= c < first_reducer + reducers:
                    greet(c * CREW + chip * CORES + k)

    loads["latent_condition"].wait()
    loads["context_condition"].wait()
    vm.cond[0:1, :] = vm.latent_condition[...].astype(f32).reshape(1, width)
    vm.cond[1:2, :] = vm.context_condition[...].astype(f32).reshape(1, width)
    mine = pl.ds(pl.multiple_of(sp * row_share, LANES), row_share)
    pick = iota((STRIP, row_share), 0) == 0
    raw = jnp.where(pick, vm.cond[0:1, mine], vm.cond[1:2, mine])
    cond = (raw / (1.0 + jnp.exp(-raw))).astype(bf16)
    loads["shift_weight"].wait()
    loads["scale_weight"].wait()
    for which, weight in enumerate((vm.shift_weight, vm.scale_weight)):
        part = dot(cond, weight[...])
        for c in range(chunks):
            at = slice(c * LANES, (c + 1) * LANES)
            r, row = c // share, c % share * 4 + which
            vm.part[r, row : row + 1, :] = part[0:1, at]
            vm.part[r, row + 2 : row + 3, :] = part[1:2, at]
    def load_later():
        for name in LATER:
            loads[name].start()

    pl.when(reducer)(load_later)
    @pl.when(jnp.logical_not(reducer))
    def _():
        pl.semaphore_wait(barrier, reducers)

    home_core = (CORES - 1, 0)

    def to_reducer(r, c, k, which):
        part, parts = ((vm.part, vm.parts), (vm.gate_part, vm.gate_parts))[which]
        return remote(
            part.at[r],
            parts.at[c, k],
            sem.part_send.at[which, r],
            sem.gate_part_recv.at[0] if which == 1 else sem.part_recv.at[c, k],
            (first_reducer + r) * CREW + chip * CORES + home_core[which],
        )

    def elsewhere(r, which):
        return jnp.logical_not((core == home_core[which]) & (crew == first_reducer + r))

    def send_parts(which):
        for r in range(reducers):

            @pl.when(elsewhere(r, which))
            def _():
                to_reducer(r, crew, core, which).start()

    def early_part(r):
        return to_reducer(r, crew, 0, 0)

    for r in range(reducers):

        @pl.when(jnp.logical_not(elsewhere(r, 0)))
        def _():
            early_part(r).wait_recv()

    send_parts(0)
    pl.when(jnp.logical_not(reducer))(load_later)
    loads["gate_weight"].wait()
    part = dot(cond, vm.gate_weight[...])
    for c in range(chunks):
        vm.gate_part[c // share, c % share] = part[0:1, c * LANES : (c + 1) * LANES]

    loads["context"].wait()
    xc = vm.context[...].astype(f32)
    vm.ctx_scaled[...] = xc * rms_factor(xc)
    loads["latent"].wait()

    def scale_strip(i, carry):
        at = pl.ds(pl.multiple_of(i * TILE, TILE), TILE)
        x = vm.latent[at, :].astype(f32)
        vm.scaled[at, :] = x * rms_factor(x)
        return carry

    lax.fori_loop(0, rows // TILE, scale_strip, 0)
    loads["down_weight"].wait()
    vm.down[...] = vm.down_weight[...].T

    reduced = reducers * OWNERS

    def spread(flat, slot):
        return remote(vm.total, vm.totals.at[slot], sem.total_send.at[0], sem.total_recv.at[0], flat)

    def gate_spread(flat, slot):
        return remote(
            vm.gate_total, vm.gate_totals.at[slot], sem.gate_send.at[0], sem.gate_recv.at[0], flat
        )

    def reduce_here(which, mine, held, total, totals, copy):
        for r in range(reducers):
            home = first_reducer + r

            @pl.when((core == home_core[which]) & (crew == home))
            def _():
                slot = r * OWNERS + chip
                if which == 1:
                    landed(vm.gate_part_credit, sem.gate_part_recv.at[0])
                for k in range(CORES):
                    out = None
                    for c in range(crews):
                        if c == home and k == home_core[which]:
                            term = mine[r]
                        else:
                            if which == 0 and (c != home or k != 0):
                                to_reducer(r, c, k, which).wait_recv()
                            term = held[c, k]
                        out = term if out is None else out + term
                    total[k] = out
                    totals[slot, k] = out
                for c in sorted(range(crews), key=lambda c: -abs(c - home)):

                    def send(i, carry):
                        copy(c * CREW + mate(i), slot).start()
                        return carry

                    lax.fori_loop(0 if c != home else 1, CREW, send, 0)

    def reduces(which):
        return (core == home_core[which]) & middle_crew

    def arrivals(which, totals, semaphore):
        @pl.when(reduces(which))
        def _():
            landed(totals.at[pl.ds(0, reduced - 1)], semaphore)

        @pl.when(jnp.logical_not(reduces(which)))
        def _():
            landed(totals, semaphore)

    def sent(which, credit, semaphore):
        @pl.when(reduces(which))
        def _():
            gone(credit, semaphore)

    @pl.when(reducer)
    def _():
        pl.semaphore_wait(barrier, count - 1)

    reduce_here(0, vm.part, vm.parts, vm.total, vm.totals, spread)
    loads_needed = ("norm_gain", "decay_bias", "post_gain", "up_weight", "key_weight")
    for name in loads_needed + ("value_weight",):
        loads[name].wait()
    arrivals(0, vm.totals, sem.total_recv.at[0])
    def summed(totals, r, t):
        out = None
        for p in range(t, CREW, tp_count):
            term = totals[r * OWNERS + p // CORES, p % CORES]
            out = term if out is None else out + term
        return out

    for r in range(reducers):
        for t in range(tp_count):
            tile = summed(vm.totals, r, t)
            for s in range(share):
                at = (t * chunks + r * share + s) * LANES
                vm.mods[0:4, at : at + LANES] = tile[s * 4 : s * 4 + 4]

    gain = vm.norm_gain[...] * (1.0 + vm.mods[3:4, :])
    ctx_normed = (vm.ctx_scaled[...] * gain + vm.mods[2:3, :]).astype(bf16)
    head_k = iota((DV, 2 * LANES), 1) % LANES // DK
    key_at = pl.ds(pl.multiple_of(ctx_group * LANES, LANES), LANES)
    val_at = pl.ds(pl.multiple_of(ctx_group * GV, GV), GV)
    low = dot(ctx_normed, vm.down[...]).astype(bf16)
    log_rows = log_decays(dot(low, vm.up_weight[:, key_at]) + vm.decay_bias[:, key_at])
    keys = dot(ctx_normed, vm.key_weight[:, key_at]).astype(bf16).astype(f32)
    values = dot(ctx_normed, vm.value_weight[:, val_at]).astype(bf16)
    inclusive = running_sum(lower_ones(ctx_rows), log_rows)
    closing = inclusive[ctx_rows - 1 : ctx_rows, :]
    both = jnp.concatenate(
        [keys * jnp.exp(closing - inclusive), keys * jnp.exp(inclusive - log_rows)], axis=1
    ).astype(bf16)
    state = per_head(dot_tn(values, both), head_k)
    for j in range(OWNERS):
        at = slice(j * UNIT, (j + 1) * UNIT)
        vm.ctx_out[j] = jnp.concatenate([state[at, :LANES], state[at, LANES:]], axis=0).astype(bf16)
    vm.ctx_log[...] = closing

    def ctx_copies(o, p):
        flat = crew * CREW + owner_of(o)
        return (
            remote(vm.ctx_out.at[o], vm.ctx_in.at[p], sem.ctx_send.at[0], sem.ctx_recv.at[0], flat),
            remote(vm.ctx_log, vm.ctx_logs.at[p], sem.ctx_log_send.at[0], sem.ctx_log_recv.at[0], flat),
        )

    def ctx_start(o):
        for copy in ctx_copies(o, post):
            copy.start()

    owners(ctx_start)

    gain = vm.norm_gain[...] * (1.0 + vm.mods[1:2, :])
    shift = vm.mods[0:1, :]
    for i in range(rows // STRIP):
        at = slice(i * STRIP, (i + 1) * STRIP)
        vm.normed[at, :] = (vm.scaled[at, :] * gain + shift).astype(bf16)

    def project(weight, out):
        for n in range(0, weight.shape[1], COLS):
            at = slice(n, n + COLS)
            out[:, at] = dot(vm.normed[...], weight[:, at]).astype(bf16)

    def project_tile(weight, out, n):
        at = slice(n, min(n + COLS, weight.shape[1]))
        out[:, at] = dot(vm.normed[...], weight[:, at]).astype(bf16)

    tiles = [(vm.key_weight, vm.key, n) for n in range(0, vm.key_weight.shape[1], COLS)]
    tiles += [(vm.value_weight, vm.value, n) for n in range(0, vm.value_weight.shape[1], COLS)]
    low = dot(vm.normed[...], vm.down[...]).astype(bf16)
    project_tile(*tiles.pop(0))
    lower = lower_ones(TILE)
    offset = None
    for b in range(blocks):
        at = slice(b * TILE, (b + 1) * TILE)
        log_rows = log_decays(dot(low[at], vm.up_weight[...]) + vm.decay_bias[...])
        inclusive = running_sum(lower, log_rows)
        end = inclusive[TILE - 1 : TILE, :]
        vm.inclusive[at, :] = inclusive
        vm.before[at, :] = inclusive - log_rows
        vm.closing[b : b + 1, :] = end
        vm.offset[b : b + 1, :] = jnp.zeros_like(end) if offset is None else offset
        offset = end if offset is None else offset + end
        if tiles:
            project_tile(*tiles.pop(0))
    vm.offset[blocks : blocks + 1, :] = offset
    for g in range(GROUPS):
        vm.log_out[g : g + 1, :] = offset[:, g * LANES : (g + 1) * LANES]
    while tiles:
        project_tile(*tiles.pop(0))

    send_parts(1)

    def log_copy(o, p):
        return remote(
            vm.log_out, vm.logs.at[p], sem.log_send.at[0], sem.log_recv.at[0], crew * CREW + owner_of(o)
        )

    def early_copies(o, p):
        return (*ctx_copies(o, p), log_copy(o, p))

    owners(lambda o: log_copy(o, post).start())

    @pl.when(owner)
    def _():
        vm.ctx_in[post] = vm.ctx_out[chip]
        vm.ctx_logs[post] = vm.ctx_log[...]
        vm.logs[post] = vm.log_out[...]

    def seg_copy(o, p, g):
        return remote(
            vm.seg_out.at[o, g],
            vm.seg_in.at[p, g],
            sem.seg_send.at[0],
            sem.seg_recv.at[0],
            crew * CREW + owner_of(o),
        )

    for g in range(GROUPS):
        lanes = slice(g * LANES, (g + 1) * LANES)
        v_lanes = slice(g * GV, (g + 1) * GV)
        whole = vm.offset[blocks : blocks + 1, lanes]
        both = []
        for b in range(blocks):
            at = slice(b * TILE, (b + 1) * TILE)
            keys = vm.key[at, lanes].astype(f32)
            start, closing = vm.offset[b : b + 1, lanes], vm.closing[b : b + 1, lanes]
            ahead = keys * jnp.exp(closing - vm.inclusive[at, lanes])
            behind = keys * jnp.exp(vm.before[at, lanes])
            vm.k_block[g, at, :] = jnp.concatenate([ahead, behind], axis=1).astype(bf16)
            both.append(
                jnp.concatenate(
                    [ahead * jnp.exp((whole - start) - closing), behind * jnp.exp(start)], axis=1
                ).astype(bf16)
            )
        state = per_head(dot_tn(vm.value[:, v_lanes], jnp.concatenate(both, axis=0)), head_k)
        for j in range(OWNERS):
            at = slice(j * UNIT, (j + 1) * UNIT)
            vm.seg_out[j, g] = jnp.concatenate([state[at, :LANES], state[at, LANES:]], axis=0).astype(bf16)
        owners(lambda o: seg_copy(o, post, g).start())

    @pl.when(owner)
    def _():
        vm.seg_in[post] = vm.seg_out[chip]

    def ctx_crew_copies(c, slot):
        flat = c * CREW + post
        return (
            remote(
                vm.ctx_crews_out,
                vm.ctx_crews.at[slot],
                sem.ctx_crew_send.at[0],
                sem.ctx_crew_recv.at[0],
                flat,
            ),
            remote(
                vm.ctx_crews_log,
                vm.ctx_crews_logs.at[slot],
                sem.ctx_crew_log_send.at[0],
                sem.ctx_crew_log_recv.at[0],
                flat,
            ),
        )

    @pl.when(owner)
    def _():
        landed(vm.ctx_in.at[pl.ds(0, CREW - 1)], sem.ctx_recv.at[0])
        landed(vm.ctx_logs.at[pl.ds(0, CREW - 1)], sem.ctx_log_recv.at[0])
        for g in range(GROUPS):
            posts = list(range(g, CREW, GROUPS))
            logs = [vm.ctx_logs[p] for p in posts]
            tiles = [vm.ctx_in[p].astype(f32) for p in posts]
            forward, backward, log_sum = tiles[0][:UNIT], tiles[-1][UNIT:], logs[0]
            for i in range(1, len(posts)):
                forward = jnp.exp(logs[i]) * forward + tiles[i][:UNIT]
                backward = jnp.exp(logs[-1 - i]) * backward + tiles[-1 - i][UNIT:]
                log_sum = log_sum + logs[i]
            vm.ctx_crews_out[g] = jnp.concatenate([forward, backward], axis=0).astype(bf16)
            vm.ctx_crews_log[g : g + 1, :] = log_sum

        def ctx_crew_start(i):
            for copy in ctx_crew_copies(lax.rem(crew + i, crews), crew):
                copy.start()

        others(ctx_crew_start, crews)
        vm.ctx_crews[crew] = vm.ctx_crews_out[...]
        vm.ctx_crews_logs[crew] = vm.ctx_crews_log[...]

    head_k1 = iota((TILE, LANES), 1) // DK
    head_v = iota((TILE, GV), 1) // DV
    t_index = iota((TILE, GROUP * TILE), 0)
    s_index = iota((TILE, GROUP * TILE), 1) % TILE

    def inside(g):
        lanes = slice(g * LANES, (g + 1) * LANES)
        v_lanes = slice(g * GV, (g + 1) * GV)
        whole = vm.offset[blocks : blocks + 1, lanes]
        for b in range(blocks):
            at = slice(b * TILE, (b + 1) * TILE)
            inclusive, before = vm.inclusive[at, lanes], vm.before[at, lanes]
            start = vm.offset[b : b + 1, lanes]
            closing = inclusive[TILE - 1 : TILE, :]
            middle = inclusive[TILE // 2 - 1 : TILE // 2, :]
            queries = vm.query[at, lanes].astype(f32) * DK ** (-0.5)
            keys = vm.key[at, lanes].astype(f32)
            scores = []
            for q_log, k_log in (
                (inclusive - middle, middle - inclusive),
                (middle - before, before - middle),
            ):
                k_stack = stacked((keys * jnp.exp(k_log)).astype(bf16), head_k1)
                scores.append(dot_nt((queries * jnp.exp(q_log)).astype(bf16), k_stack))
            both = jnp.where(t_index >= s_index, scores[0], 0.0) + jnp.where(
                t_index <= s_index, scores[1], 0.0
            )
            v_stack = stacked(vm.value[at, v_lanes], head_v)
            vm.within[at, v_lanes] = dot(both.astype(bf16), v_stack)
            ahead = queries * jnp.exp(inclusive)
            behind = queries * jnp.exp(closing - before)
            vm.q_block[g, at, :] = jnp.concatenate([ahead, behind], axis=1).astype(bf16)
            vm.q_whole[g, at, :] = jnp.concatenate(
                [ahead * jnp.exp(start), behind * jnp.exp((whole - start) - closing)], axis=1
            ).astype(bf16)

    def between(g):
        lanes = slice(g * LANES, (g + 1) * LANES)
        v_lanes = slice(g * GV, (g + 1) * GV)
        decays = [jnp.exp(vm.closing[b : b + 1, lanes]) for b in range(blocks)]
        left = []
        for b in range(blocks):
            at = slice(b * TILE, (b + 1) * TILE)
            left.append(per_head(dot_tn(vm.value[at, v_lanes], vm.k_block[g, at, :]), head_k))
        forward = [jnp.zeros((DV, LANES), f32)]
        backward = [jnp.zeros((DV, LANES), f32)]
        for b in range(blocks - 1):
            forward.append(decays[b] * forward[b] + left[b][:, :LANES])
            back = blocks - 1 - b
            backward.insert(0, decays[back] * backward[0] + left[back][:, LANES:])
        for b in range(blocks):
            at = slice(b * TILE, (b + 1) * TILE)
            states = jnp.concatenate([forward[b], backward[b]], axis=1)
            across = dot_nt(vm.q_block[g, at, :], stacked(states, head_k).astype(bf16))
            vm.within[at, v_lanes] = vm.within[at, v_lanes] + across

    loads["query_weight"].wait()
    project(vm.query_weight, vm.query)
    inside(0)

    def crew_log_copy(c, slot):
        return remote(
            vm.crew_log,
            vm.crew_logs.at[slot],
            sem.crew_log_send.at[0],
            sem.crew_log_recv.at[0],
            c * CREW + post,
        )

    @pl.when(owner)
    def _():
        landed(vm.logs.at[pl.ds(0, CREW - 1)], sem.log_recv.at[0])
        vm.decay[...] = jnp.exp(vm.logs[...])
        crew_log = vm.logs[0]
        for p in range(1, CREW):
            crew_log = crew_log + vm.logs[p]
        vm.crew_log[...] = crew_log
        others(lambda i: crew_log_copy(lax.rem(crew + i, crews), crew).start(), crews)

    inside(1)

    reduce_here(1, vm.gate_part, vm.gate_parts, vm.gate_total, vm.gate_totals, gate_spread)

    def crew_copy(c, slot, side):
        return remote(
            vm.crew_out.at[side],
            vm.crew_in.at[slot],
            sem.crew_send.at[0],
            sem.crew_recv.at[0],
            c * CREW + post,
        )

    def post_decay(p, g):
        return vm.decay[p, g : g + 1, :]

    @pl.when(owner)
    def _():
        landed(vm.seg_in.at[pl.ds(0, CREW - 1)], sem.seg_recv.at[0])
        for g in range(GROUPS):
            at = slice(g * UNIT, (g + 1) * UNIT)
            forward = vm.seg_in[0, g, :UNIT].astype(f32)
            for p in range(1, CREW):
                forward = post_decay(p, g) * forward + vm.seg_in[p, g, :UNIT].astype(f32)
            backward = vm.seg_in[CREW - 1, g, UNIT:].astype(f32)
            for p in range(CREW - 2, -1, -1):
                backward = post_decay(p, g) * backward + vm.seg_in[p, g, UNIT:].astype(f32)
            vm.crew_out[0, at, :] = forward.astype(bf16)
            vm.crew_out[1, at, :] = backward.astype(bf16)

        def crew_start(i):
            ahead, behind = crews - i, i - 1

            @pl.when(ahead > crew)
            def _():
                crew_copy(ahead, crew, 0).start()

            @pl.when(behind < crew)
            def _():
                crew_copy(behind, crew, 1).start()

        others(crew_start, crews)

    for g in range(2, GROUPS):
        inside(g)
    for g in range(GROUPS - 2):
        between(g)

    half = GROUPS // 2

    def enter_copy(p, o, h):
        part = pl.ds(h * half, half)
        return remote(
            vm.enter_out.at[p, part],
            vm.enter_in.at[o, part],
            sem.enter_send.at[0],
            sem.enter_recv.at[h],
            crew * CREW + p,
        )

    @pl.when(owner)
    def _():
        away = pl.ds(0, crews - 1)
        landed(vm.ctx_crews.at[away], sem.ctx_crew_recv.at[0])
        landed(vm.ctx_crews_logs.at[away], sem.ctx_crew_log_recv.at[0])
        landed(vm.crew_logs.at[away], sem.crew_log_recv.at[0])
        vm.crew_decay[...] = jnp.exp(vm.crew_logs[...])
        vm.ctx_decay[...] = jnp.exp(vm.ctx_crews_logs[...])
        zero = jnp.zeros((UNIT, LANES), f32)
        forward, backward = [zero] * GROUPS, [zero] * GROUPS
        for a in range(crews):
            z = crews - 1 - a
            for g in range(GROUPS):
                forward[g] = (
                    vm.ctx_decay[a, g : g + 1, :] * forward[g]
                    + vm.ctx_crews[a, g, :UNIT].astype(f32)
                )
                backward[g] = (
                    vm.ctx_decay[z, g : g + 1, :] * backward[g]
                    + vm.ctx_crews[z, g, UNIT:].astype(f32)
                )

        def step_states(c, states):
            left = vm.crew_in[c].astype(f32)
            return tuple(
                vm.crew_decay[c, g : g + 1, :] * states[g] + left[g * UNIT : (g + 1) * UNIT]
                for g in range(GROUPS)
            )

        def from_after(i, states):
            return step_states(crews - 1 - i, states)

        landed(vm.crew_in.at[away], sem.crew_recv.at[0])
        forward = lax.fori_loop(0, crew, step_states, tuple(forward))
        backward = lax.fori_loop(0, crews - 1 - crew, from_after, tuple(backward))
        for g in range(GROUPS):
            state = forward[g]
            for p in range(CREW):
                vm.enter_out[p, g, :UNIT] = state.astype(bf16)
                if p < CREW - 1:
                    state = post_decay(p, g) * state + vm.seg_in[p, g, :UNIT].astype(f32)
            state = backward[g]
            for p in range(CREW - 1, -1, -1):
                vm.enter_out[p, g, UNIT:] = state.astype(bf16)
                if p > 0:
                    state = post_decay(p, g) * state + vm.seg_in[p, g, UNIT:].astype(f32)
            if g % half == half - 1:
                mates(lambda p: enter_copy(p, chip, g // half).start())
        vm.enter_in[chip] = vm.enter_out[post]

    loads["outgate_weight"].wait()
    for n in range(0, vm.outgate_weight.shape[1], COLS):
        at = slice(n, n + COLS)
        gate = dot(vm.normed[...], vm.outgate_weight[:, at]).astype(bf16).astype(f32)
        vm.silu[:, at] = gate / (1.0 + jnp.exp(-gate))
    for g in range(GROUPS - 2, GROUPS):
        between(g)
    head_mean = jnp.where(iota((GV, GV), 0) // DV == iota((GV, GV), 1) // DV, 1.0 / DV, 0.0).astype(bf16)

    arrivals(1, vm.gate_totals, sem.gate_recv.at[0])
    for r in range(reducers):
        for t in range(tp_count):
            tile = summed(vm.gate_totals, r, t)
            for s in range(share):
                at = (t * chunks + r * share + s) * LANES
                vm.mods[4:5, at : at + LANES] = tile[s]
    loads["out_weight"].wait()

    for which in range(2):
        for r in range(reducers):

            @pl.when(elsewhere(r, which))
            def _():
                to_reducer(r, crew, core, which).wait_send()

    sent(0, vm.credit, sem.total_send.at[0])
    sent(1, vm.gate_credit, sem.gate_send.at[0])

    def to_owners_sent(n):
        gone(vm.ctx_out.at[pl.ds(0, n)], sem.ctx_send.at[0])
        gone(vm.ctx_logs.at[pl.ds(0, n)], sem.ctx_log_send.at[0])
        gone(vm.logs.at[pl.ds(0, n)], sem.log_send.at[0])
        gone(vm.seg_out.at[pl.ds(0, n)], sem.seg_send.at[0])

    by_role(to_owners_sent)

    @pl.when(owner)
    def _():
        away = pl.ds(0, crews - 1)
        gone(vm.ctx_crews.at[away], sem.ctx_crew_send.at[0])
        gone(vm.ctx_crews_logs.at[away], sem.ctx_crew_log_send.at[0])
        gone(vm.crew_logs.at[away], sem.crew_log_send.at[0])
        gone(vm.crew_in.at[away], sem.crew_send.at[0])

    def finish(g):
        v_lanes = slice(g * GV, (g + 1) * GV)
        states = jnp.concatenate(
            [
                jnp.concatenate([vm.enter_in[o, g, :UNIT] for o in range(OWNERS)], axis=0),
                jnp.concatenate([vm.enter_in[o, g, UNIT:] for o in range(OWNERS)], axis=0),
            ],
            axis=1,
        )
        across = dot_nt(vm.q_whole[g], stacked(states, head_k))
        mixed = vm.within[:, v_lanes] + across
        mean = dot((mixed * mixed).astype(bf16), head_mean)
        vm.gated[:, v_lanes] = (mixed * lax.rsqrt(mean + epsilon) * vm.silu[:, v_lanes]).astype(bf16)

    def entered(h):
        part = pl.ds(h * half, half)
        by_role(lambda n: landed(vm.enter_in.at[pl.ds(0, n), part], sem.enter_recv.at[h]))

    depth = half * GV
    entered(0)
    for g in range(half):
        finish(g)
    for n in range(0, width, COLS):
        at = slice(n, n + COLS)
        vm.branch_part[:, at] = dot(vm.gated[:, :depth], vm.out_weight[:depth, at])
    entered(1)
    for g in range(half, GROUPS):
        finish(g)

    square = jnp.zeros((rows, LANES), f32)
    for n in range(0, width, COLS):
        at = slice(n, n + COLS)
        branch = (vm.branch_part[:, at] + dot(vm.gated[:, depth:], vm.out_weight[depth:, at])).astype(bf16)
        vm.branch[:, at] = branch
        branch = branch.astype(f32)
        branch = branch * branch
        for s in range(0, COLS, LANES):
            square = square + branch[:, s : s + LANES]
    factor = lax.rsqrt(jnp.sum(square, axis=1, keepdims=True) / width + epsilon)
    gain = vm.mods[4:5, :] * vm.post_gain[...]
    for i in range(rows // STRIP):
        at = slice(i * STRIP, (i + 1) * STRIP)
        hbm.out[at, :] = (
            vm.latent[at, :].astype(f32) + gain * (vm.branch[at, :].astype(f32) * factor[at])
        ).astype(bf16)

    @pl.when(owner)
    def _():
        gone(vm.enter_out.at[pl.ds(0, CREW - 1)], sem.enter_send.at[0])


def shards(*operands):
    values = dict(zip(NAMES, operands))
    values["down_weight"] = values["down_weight"].T
    latent, context = values["latent"], values["context"]
    sp_count, tp_count = lax.axis_size("sp"), lax.axis_size("tp")
    count = sp_count * tp_count
    crews = count // CREW
    rows, width = latent.shape
    args, specs = [], []
    for name, value in values.items():
        vector = value.ndim == 1
        args.append(value.reshape(1, -1) if vector and value.dtype == f32 else value)
        specs.append(pl.BlockSpec(memory_space=pltpu.HBM))
    ctx_rows = context.shape[0] * GROUPS // tp_count
    chunks = values["shift_weight"].shape[1] // LANES
    reducers, share = reduction(chunks, crews)
    part_rows = -(-4 * share // SUB) * SUB
    keyw, valw = values["key_weight"].shape[1], values["value_weight"].shape[1]
    blocks = rows // TILE
    unit = (2 * UNIT, LANES)
    buffers = dict(
        context=pltpu.VMEM((ctx_rows, width), bf16),
        credit=pltpu.VMEM((count - 1, CORES, part_rows, LANES), f32),
        gate_credit=pltpu.VMEM((count - 1, CORES, share, 1, LANES), f32),
        gate_part_credit=pltpu.VMEM((crews * CORES - 1, share, 1, LANES), f32),
        cond=pltpu.VMEM((SUB, width), f32),
        part=pltpu.VMEM((reducers, part_rows, LANES), f32),
        parts=pltpu.VMEM((crews, CORES, part_rows, LANES), f32),
        total=pltpu.VMEM((CORES, part_rows, LANES), f32),
        totals=pltpu.VMEM((reducers * OWNERS, CORES, part_rows, LANES), f32),
        gate_part=pltpu.VMEM((reducers, share, 1, LANES), f32),
        gate_parts=pltpu.VMEM((crews, CORES, share, 1, LANES), f32),
        gate_total=pltpu.VMEM((CORES, share, 1, LANES), f32),
        gate_totals=pltpu.VMEM((reducers * OWNERS, CORES, share, 1, LANES), f32),
        mods=pltpu.VMEM((SUB, width), f32),
        scaled=pltpu.VMEM((rows, width), f32),
        down=pltpu.VMEM((width, values["down_weight"].shape[0]), bf16),
        ctx_scaled=pltpu.VMEM((ctx_rows, width), f32),
        normed=pltpu.VMEM((rows, width), bf16),
        ctx_out=pltpu.VMEM((OWNERS, *unit), bf16),
        ctx_in=pltpu.VMEM((CREW, *unit), bf16),
        ctx_log=pltpu.VMEM((1, LANES), f32),
        ctx_logs=pltpu.VMEM((CREW, 1, LANES), f32),
        ctx_crews_out=pltpu.VMEM((GROUPS, *unit), bf16),
        ctx_crews=pltpu.VMEM((crews, GROUPS, *unit), bf16),
        key=pltpu.VMEM((rows, keyw), bf16),
        query=pltpu.VMEM((rows, keyw), bf16),
        value=pltpu.VMEM((rows, valw), bf16),
        silu=pltpu.VMEM((rows, valw), f32),
        gated=pltpu.VMEM((rows, valw), bf16),
        inclusive=pltpu.VMEM((rows, keyw), f32),
        before=pltpu.VMEM((rows, keyw), f32),
        closing=pltpu.VMEM((blocks, keyw), f32),
        offset=pltpu.VMEM((blocks + 1, keyw), f32),
        log_out=pltpu.VMEM((GROUPS, LANES), f32),
        logs=pltpu.VMEM((CREW, GROUPS, LANES), f32),
        decay=pltpu.VMEM((CREW, GROUPS, LANES), f32),
        crew_decay=pltpu.VMEM((crews, GROUPS, LANES), f32),
        ctx_decay=pltpu.VMEM((crews, GROUPS, LANES), f32),
        ctx_crews_log=pltpu.VMEM((GROUPS, LANES), f32),
        ctx_crews_logs=pltpu.VMEM((crews, GROUPS, LANES), f32),
        seg_out=pltpu.VMEM((OWNERS, GROUPS, *unit), bf16),
        seg_in=pltpu.VMEM((CREW, GROUPS, *unit), bf16),
        crew_out=pltpu.VMEM((2, GROUPS * UNIT, LANES), bf16),
        crew_in=pltpu.VMEM((crews, GROUPS * UNIT, LANES), bf16),
        crew_log=pltpu.VMEM((GROUPS, LANES), f32),
        crew_logs=pltpu.VMEM((crews, GROUPS, LANES), f32),
        enter_out=pltpu.VMEM((CREW, GROUPS, *unit), bf16),
        enter_in=pltpu.VMEM((OWNERS, GROUPS, *unit), bf16),
        k_block=pltpu.VMEM((GROUPS, rows, 2 * LANES), bf16),
        q_block=pltpu.VMEM((GROUPS, rows, 2 * LANES), bf16),
        q_whole=pltpu.VMEM((GROUPS, rows, 2 * LANES), bf16),
        within=pltpu.VMEM((rows, valw), f32),
        branch_part=pltpu.VMEM((rows, width), f32),
        branch=pltpu.VMEM((rows, width), bf16),
    )
    for name, value in zip(NAMES, args):
        if name not in buffers:
            buffers[name] = pltpu.VMEM(value.shape, value.dtype)
    dma = pltpu.SemaphoreType.DMA
    semaphores = dict(
        load=dma((len(NAMES),)),
        part_send=dma((2, reducers)),
        part_recv=dma((crews, CORES)),
        gate_part_recv=dma((1,)),
        total_send=dma((1,)),
        total_recv=dma((1,)),
        gate_send=dma((1,)),
        gate_recv=dma((1,)),
        ctx_send=dma((1,)),
        ctx_recv=dma((1,)),
        ctx_log_send=dma((1,)),
        ctx_log_recv=dma((1,)),
        log_send=dma((1,)),
        log_recv=dma((1,)),
        seg_send=dma((1,)),
        seg_recv=dma((1,)),
        ctx_crew_send=dma((1,)),
        ctx_crew_recv=dma((1,)),
        ctx_crew_log_send=dma((1,)),
        ctx_crew_log_recv=dma((1,)),
        crew_log_send=dma((1,)),
        crew_log_recv=dma((1,)),
        crew_send=dma((1,)),
        crew_recv=dma((1,)),
        enter_send=dma((1,)),
        enter_recv=dma((2,)),
    )
    return pl.pallas_call(
        functools.partial(block_kernel, sp_count, tp_count),
        out_shape=pltpu.VMEM((rows, width), bf16),
        in_specs=specs,
        out_specs=pl.BlockSpec(memory_space=pltpu.VMEM),
        scratch_shapes=[buffers, semaphores],
        compiler_params=pltpu.CompilerParams(
            collective_id=0, has_side_effects=True, vmem_limit_bytes=VMEM_LIMIT
        ),
        name="block",
    )(*args)


def solution(mesh):
    placed = (
        P(("sp", "tp"), None),
        P("sp", None),
        P(),
        P(),
        P("sp", "tp"),
        P("sp", "tp"),
        P("sp", "tp"),
        P(),
        P(),
        P(),
        P(),
        P(),
        P(),
        P(),
        P(),
        P(),
        P(),
    )
    return jax.shard_map(
        shards, mesh=mesh, in_specs=placed, out_specs=P(("sp", "tp"), None), check_vma=False
    )
```
